256 devices in a mesh: ep: 64 (over z, y, x_hi), tp: 4 (over x_lo, core).
Axes of the slice: x: 4 (x_hi: 2, x_lo: 2; x = x_hi * 2 + x_lo), y: 4, z: 8, core: 2. Of those that a mesh axis runs over, the one named last changes fastest.
Arguments:
- tokens: bfloat16 [6144, 2048], P('ep'), may hold values from -6 to 6
- norm_gain: bfloat16 [2048], replicated, may hold values from 0.099609375 to 1.8984375
- in_weight: bfloat16 [2048, 1024], P(None, 'tp'), may hold values from -0.125 to 0.125
- sequence_state_real: float32 [6144, 4096], P('ep', 'tp'), may hold values from -6 to 6
- sequence_state_imaginary: float32 [6144, 4096], P('ep', 'tp'), may hold values from -6 to 6
- eigen_decay_real: float32 [64, 64], P('tp'), may hold values from -1 to -0.2
- log_step: float32 [64], P('tp'), may hold values from -4.6 to 0
- input_matrix_real: float32 [64, 64, 16], P('tp'), may hold values from -1 to 1
- input_matrix_imaginary: float32 [64, 64, 16], P('tp'), may hold values from -1 to 1
- output_matrix_real: float32 [64, 16, 64], P('tp'), may hold values from -0.75 to 0.75
- output_matrix_imaginary: float32 [64, 16, 64], P('tp'), may hold values from -0.75 to 0.75
- channel_skip_scale: float32 [64, 16], P('tp'), may hold values from -4 to 4
- out_weight: bfloat16 [1024, 2048], P('tp'), may hold values from -0.25 to 0.25
- ffn_gain: bfloat16 [2048], replicated, may hold values from 0.099609375 to 1.8984375
- routes: int32 [6144, 2], P('ep'), may hold values from 0 to 63, all different within a row; in each aligned block of 96 rows (0 to 95, 96 to 191, ...) at most 6 rows name the same one
- group_weight: float32 [6144], P('ep'), may hold values from 0.3 to 1
- expert_logit: float32 [6144, 2], P('ep'), may hold values from -6 to 6
- expert_gate: bfloat16 [64, 2048, 512], P('ep', None, 'tp'), may hold values from -0.125 to 0.125
- expert_up: bfloat16 [64, 2048, 512], P('ep', None, 'tp'), may hold values from -0.125 to 0.125
- expert_down: bfloat16 [64, 512, 2048], P('ep', 'tp'), may hold values from -0.5 to 0.5
- dense_gate: bfloat16 [2048, 2048], P(None, 'tp'), may hold values from -0.125 to 0.125
- dense_up: bfloat16 [2048, 2048], P(None, 'tp'), may hold values from -0.125 to 0.125
- dense_down: bfloat16 [2048, 2048], P('tp'), may hold values from -0.25 to 0.25
- blend_weight: bfloat16 [2048], replicated, may hold values from -0.25 to 0.25
Outputs:
- new_tokens: bfloat16 [6144, 2048], P('ep', 'tp')
- new_state_real: float32 [6144, 4096], P('ep', 'tp')
- new_state_imag: float32 [6144, 4096], P('ep', 'tp')
The draws below stay inside these ranges and needn't reach their ends.
Inputs may be any that keep to these rules, and one draw needn't show every extreme that they name: `routes`: each row names 2 different experts. Among the rows of one index of ep (aligned blocks of 96 rows) no expert is named by more than 6 rows, and in some block one expert is named by exactly 6 rows.
All inputs are finite; a program needn't handle non-finite values.
Results may differ from the reference program's by a relative error of at most 0.014.
Values may be sent and summed in bfloat16 or wider, within the bound.
No kernel may reach another device: no remote copies, remote signals or barrier semaphores. Data moves between devices by JAX's collectives and lax.ppermute only.
A program may use at most 64 MiB of HBM per device.

```python
import math
import jax
import jax.numpy as jnp
import numpy as np
from jax import lax

D = 2048
SSMW = 1024
GROUP_CHANNELS = 16
GROUP_STATE_SIZE = 64
STATE_GROUPS = 64
FE = 512
DFF = 2048
TOPK = 2
EXPERTS = 64
SEQ_DEV = 96
SEQUENCE_COUNT = 6144
CAP = 6
N_EP = 64
N_TP = 4


def level_of(key, dims, pieces, smallest, high):
    def one(dim, blocks):
        draws = jax.random.uniform(jax.random.fold_in(jax.random.fold_in(key, 6), dim), (blocks,), jnp.float32, smallest / len(pieces), high / len(pieces))
        return jnp.repeat(jnp.exp(draws), dims[dim] // blocks).reshape((-1,) + (1,) * (len(dims) - dim - 1))

    factor_of = one(*pieces[0])
    for cut in pieces[1:]:
        factor_of = factor_of * one(*cut)
    return factor_of


def deal_out(key, own, number, rows, count, top, limit, lean):
    order = jax.random.permutation(key, count)
    packed, common = shares(count, rows * top, limit, lean, True), shares(count, rows * top, limit, lean, False)
    places = jnp.arange(count)

    def named(lengths, offset_by):
        used = int((lengths > 0).sum())
        fixed = max(1, used // 4)
        shifted = fixed + (places - fixed + offset_by * (used - fixed)) % max(1, count - fixed)
        return jnp.zeros((count,), jnp.int32).at[order[jnp.where(places < fixed, places, shifted)]].set(jnp.asarray(lengths, jnp.int32))

    lengths = jnp.where(number % 4 == 0, named(packed, number // 4), named(common, number - number // 4 - 1))
    mixed = jax.random.permutation(jax.random.fold_in(own, 3), count)
    giver, receiver = mixed[0:count // 2 * 2:2], mixed[1:count // 2 * 2:2]
    slack = jnp.minimum(lengths[giver] - 1, limit - lengths[receiver]) // 2
    slack = jnp.where((giver == order[0]) | (receiver == order[0]) | (lengths[receiver] == 0), 0, jnp.maximum(slack, 0))
    shifted = jax.random.randint(jax.random.fold_in(own, 4), (count // 2,), 0, 1 << 20) % (slack + 1)
    lengths = lengths.at[giver].add(-shifted).at[receiver].add(shifted)
    items = jnp.searchsorted(jnp.cumsum(lengths), jnp.arange(rows * top), side="right").astype(jnp.int32)
    listing = items.reshape(top, rows).T
    listing = listing[jax.random.permutation(jax.random.fold_in(own, 1), rows)]
    offset_by = jax.random.randint(jax.random.fold_in(own, 2), (rows, 1), 0, top)
    return jnp.take_along_axis(listing, (jnp.arange(top)[None, :] + offset_by) % top, axis=1)


def shares(number_of, total, reach, slope, full):
    portions = [(1 << 20) // math.isqrt(rank ** slope) + 1 for rank in range(1, number_of + 1)]
    largest = reach if full else min(reach, max(-(-total // number_of), total * portions[0] // sum(portions)))
    least = 1 if total - largest >= number_of - 1 else 0
    holding, surplus = [largest] + [least] * (number_of - 1), total - largest - least * (number_of - 1)
    while surplus > 0:
        free = [i for i in range(1, number_of) if holding[i] < largest] or [i for i in range(1, number_of) if holding[i] < reach]
        mass, budget = sum([portions[i] for i in free]), surplus
        for i in free:
            addition = min(reach - holding[i], max(1, budget * portions[i] // mass), surplus)
            holding[i] = holding[i] + addition
            surplus = surplus - addition
    return np.array(holding)


def normal_values(key, shape, width, limit, pieces=(), held_as=jnp.bfloat16):
    array = jax.random.normal(key, shape, jnp.float32) * width
    if len(pieces) > 0:
        array = level_of(key, shape, pieces, -0.22, 0.18) * array
    return jnp.clip(array, min=-limit, max=limit).astype(held_as)


def setup_inputs(seed: int = 0) -> dict:
    seeds = jax.random.split(jax.random.key(seed), 25)
    tokens = normal_values(seeds[0], (SEQUENCE_COUNT, D), 1.0, 6.0, ((0, 64),))
    norm_gain = jnp.clip(1.0 + 0.18 * jax.random.normal(seeds[1], (D,), jnp.float32), 0.099609375, 1.8984375).astype(jnp.bfloat16)
    in_weight = normal_values(seeds[2], (D, SSMW), D ** -0.5, 0.125, ((1, 4),))
    sequence_state_real = normal_values(seeds[3], (SEQUENCE_COUNT, STATE_GROUPS * GROUP_STATE_SIZE), 1.0, 6.0, ((0, 64), (1, 4)), jnp.float32)
    sequence_state_imaginary = normal_values(seeds[4], (SEQUENCE_COUNT, STATE_GROUPS * GROUP_STATE_SIZE), 1.0, 6.0, ((0, 64), (1, 4)), jnp.float32)
    eigen_decay_real = jnp.clip(-1.0 + 0.8 * jax.random.uniform(seeds[5], (STATE_GROUPS, GROUP_STATE_SIZE), jnp.float32) ** level_of(seeds[5], (STATE_GROUPS, GROUP_STATE_SIZE), ((0, 4),), -0.2, 0.2), -1.0, -0.2)
    log_step = jnp.clip(-4.6 + 4.6 * jax.random.uniform(seeds[6], (STATE_GROUPS,), jnp.float32) ** level_of(seeds[6], (STATE_GROUPS,), ((0, 4),), -0.2, 0.2), -4.6, 0.0)
    input_matrix_real = normal_values(seeds[7], (STATE_GROUPS, GROUP_STATE_SIZE, GROUP_CHANNELS), (2 * GROUP_CHANNELS) ** -0.5, 1.0, ((0, 4),), jnp.float32)
    input_matrix_imaginary = normal_values(seeds[8], (STATE_GROUPS, GROUP_STATE_SIZE, GROUP_CHANNELS), (2 * GROUP_CHANNELS) ** -0.5, 1.0, ((0, 4),), jnp.float32)
    output_matrix_real = normal_values(seeds[9], (STATE_GROUPS, GROUP_CHANNELS, GROUP_STATE_SIZE), GROUP_STATE_SIZE ** -0.5, 0.75, ((0, 4),), jnp.float32)
    output_matrix_imaginary = normal_values(seeds[10], (STATE_GROUPS, GROUP_CHANNELS, GROUP_STATE_SIZE), GROUP_STATE_SIZE ** -0.5, 0.75, ((0, 4),), jnp.float32)
    channel_skip_scale = normal_values(seeds[11], (STATE_GROUPS, GROUP_CHANNELS), 1.0, 4.0, ((0, 4),), jnp.float32)
    out_weight = normal_values(seeds[12], (SSMW, D), (SSMW // 2) ** -0.5, 0.25, ((0, 4),))
    ffn_gain = jnp.clip(1.0 + 0.18 * jax.random.normal(seeds[13], (D,), jnp.float32), 0.099609375, 1.8984375).astype(jnp.bfloat16)
    routes_keys = jax.random.split(jax.random.fold_in(seeds[14], 1), SEQUENCE_COUNT // SEQ_DEV)
    routes_turns = jax.random.permutation(jax.random.fold_in(seeds[14], 3), SEQUENCE_COUNT // SEQ_DEV)
    routes = jax.vmap(lambda own, number: deal_out(jax.random.fold_in(seeds[14], 2), own, number, SEQ_DEV, EXPERTS, TOPK, CAP, 2))(routes_keys, routes_turns).reshape((SEQUENCE_COUNT, TOPK))
    group_weight = jnp.clip(0.3 + 0.7 * jax.random.uniform(seeds[15], (SEQUENCE_COUNT,), jnp.float32) ** level_of(seeds[15], (SEQUENCE_COUNT,), ((0, 64),), -0.2, 0.2), 0.3, 1.0)
    expert_logit = normal_values(seeds[16], (SEQUENCE_COUNT, TOPK), 1.5, 6.0, ((0, 64),), jnp.float32)
    expert_gate = normal_values(seeds[17], (EXPERTS, D, FE), D ** -0.5, 0.125, ((0, 64), (2, 4)))
    expert_up = normal_values(seeds[18], (EXPERTS, D, FE), D ** -0.5, 0.125, ((0, 64), (2, 4)))
    expert_down = normal_values(seeds[19], (EXPERTS, FE, D), (FE // 4) ** -0.5, 0.5, ((0, 64), (1, 4)))
    dense_gate = normal_values(seeds[20], (D, DFF), D ** -0.5, 0.125, ((1, 4),))
    dense_up = normal_values(seeds[21], (D, DFF), D ** -0.5, 0.125, ((1, 4),))
    dense_down = normal_values(seeds[22], (DFF, D), (DFF // 4) ** -0.5, 0.25, ((0, 4),))
    blend_weight = normal_values(seeds[23], (D,), (D // 4) ** -0.5, 0.25)
    return {"tokens": tokens, "norm_gain": norm_gain, "in_weight": in_weight, "sequence_state_real": sequence_state_real, "sequence_state_imaginary": sequence_state_imaginary, "eigen_decay_real": eigen_decay_real, "log_step": log_step, "input_matrix_real": input_matrix_real, "input_matrix_imaginary": input_matrix_imaginary, "output_matrix_real": output_matrix_real, "output_matrix_imaginary": output_matrix_imaginary, "channel_skip_scale": channel_skip_scale, "out_weight": out_weight, "ffn_gain": ffn_gain, "routes": routes, "group_weight": group_weight, "expert_logit": expert_logit, "expert_gate": expert_gate, "expert_up": expert_up, "expert_down": expert_down, "dense_gate": dense_gate, "dense_up": dense_up, "dense_down": dense_down, "blend_weight": blend_weight}


EPS = 1e-06

def rounded(values):
    return lax.optimization_barrier(values.astype(jnp.bfloat16)).astype(jnp.float32)

def norm_rows(values, gain):
    scale = lax.rsqrt(lax.optimization_barrier(jnp.mean(values * values, axis=-1, keepdims=True)) + EPS)
    return values * scale * gain.astype(jnp.float32)

def discretize(eigen_decay_real, log_step, input_matrix_real, input_matrix_imaginary):
    step = jnp.exp(log_step)[:, None]
    freq = math.pi * jnp.arange(eigen_decay_real.shape[1], dtype=jnp.float32)[None, :]
    magnitude = jnp.exp(eigen_decay_real * step)
    turned = freq * step
    lam_re = magnitude * jnp.cos(turned)
    lam_im = magnitude * jnp.sin(turned)
    denom = eigen_decay_real * eigen_decay_real + freq * freq
    fac_re = ((lam_re - 1.0) * eigen_decay_real + lam_im * freq) / denom
    fac_im = (lam_im * eigen_decay_real - (lam_re - 1.0) * freq) / denom
    bb_re = fac_re[..., None] * input_matrix_real - fac_im[..., None] * input_matrix_imaginary
    bb_im = fac_re[..., None] * input_matrix_imaginary + fac_im[..., None] * input_matrix_real
    return (lam_re, lam_im, bb_re, bb_im)

def state_update(drive, sequence_state_real, sequence_state_imaginary, eigen_decay_real, log_step, input_matrix_real, input_matrix_imaginary, output_matrix_real, output_matrix_imaginary, channel_skip_scale):
    highest_precision = lax.Precision.HIGHEST
    count = drive.shape[0]
    groups, entries = eigen_decay_real.shape
    chans = input_matrix_real.shape[2]
    lam_re, lam_im, bb_re, bb_im = discretize(eigen_decay_real, log_step, input_matrix_real, input_matrix_imaginary)
    layer_inputs = drive.astype(jnp.float32).reshape(count, groups, chans)
    push_re = jnp.einsum('gph,bgh->bgp', bb_re, layer_inputs, precision=highest_precision)
    push_im = jnp.einsum('gph,bgh->bgp', bb_im, layer_inputs, precision=highest_precision)
    old_re = sequence_state_real.reshape(count, groups, entries)
    old_im = sequence_state_imaginary.reshape(count, groups, entries)
    fresh_real = lam_re * old_re - lam_im * old_im + push_re
    fresh_imaginary = lam_re * old_im + lam_im * old_re + push_im
    mixer_result = jnp.einsum('uvy,ouy->ouv', output_matrix_real, fresh_real, precision=highest_precision) - jnp.einsum('uvy,ouy->ouv', output_matrix_imaginary, fresh_imaginary, precision=highest_precision) + channel_skip_scale * layer_inputs
    act = jax.nn.gelu(mixer_result).reshape(count, groups * chans).astype(jnp.bfloat16)
    return (act, fresh_real.reshape(count, groups * entries), fresh_imaginary.reshape(count, groups * entries))

def reference(tokens, norm_gain, in_weight, sequence_state_real, sequence_state_imaginary, eigen_decay_real, log_step, input_matrix_real, input_matrix_imaginary, output_matrix_real, output_matrix_imaginary, channel_skip_scale, out_weight, ffn_gain, routes, group_weight, expert_logit, expert_gate, expert_up, expert_down, dense_gate, dense_up, dense_down, blend_weight):
    f32 = jnp.float32
    bf16 = jnp.bfloat16
    resid0 = tokens.astype(f32)
    normed = norm_rows(resid0, norm_gain).astype(bf16)
    drive = jnp.dot(normed, in_weight, preferred_element_type=f32).astype(bf16)
    act, fresh_real, fresh_imaginary = state_update(drive, sequence_state_real, sequence_state_imaginary, eigen_decay_real, log_step, input_matrix_real, input_matrix_imaginary, output_matrix_real, output_matrix_imaginary, channel_skip_scale)
    block = SSMW // N_TP
    mix = jnp.zeros((SEQUENCE_COUNT, D), f32)
    for part in range(N_TP):
        mix = mix + rounded(jnp.dot(act[:, part * block:(part + 1) * block], out_weight[part * block:(part + 1) * block], preferred_element_type=f32))
    resid = resid0 + mix
    normed2 = norm_rows(resid, ffn_gain).astype(bf16)
    expo = jnp.exp(expert_logit)
    route_w = group_weight[:, None] * expo / lax.optimization_barrier(jnp.sum(expo, axis=-1, keepdims=True))
    onehot = (routes[:, :, None] == jnp.arange(EXPERTS, dtype=jnp.int32)).astype(jnp.int32)
    onehot = onehot.reshape(N_EP, SEQ_DEV * TOPK, EXPERTS)
    before = jnp.cumsum(onehot, axis=1) - onehot
    place = lax.optimization_barrier(jnp.sum(before * onehot, axis=-1)).reshape(SEQUENCE_COUNT, TOPK)
    source = (jnp.arange(SEQUENCE_COUNT, dtype=jnp.int32) // SEQ_DEV)[:, None]
    row_slot = (source * CAP + place).astype(jnp.int32)
    spread = jnp.broadcast_to(normed2[:, None, :], (SEQUENCE_COUNT, TOPK, D))
    buffer = jnp.zeros((EXPERTS, N_EP * CAP, D), bf16).at[routes, row_slot].set(spread)
    width_block = FE // N_TP

    def one_expert(operands):
        rows, w_gate, w_up, w_down = operands
        gate_pre = jnp.dot(rows, w_gate, preferred_element_type=f32)
        up_pre = jnp.dot(rows, w_up, preferred_element_type=f32)
        hidden = (jax.nn.silu(gate_pre) * up_pre).astype(bf16)
        total = jnp.zeros((rows.shape[0], D), f32)
        for part in range(N_TP):
            total = total + rounded(jnp.dot(hidden[:, part * width_block:(part + 1) * width_block], w_down[part * width_block:(part + 1) * width_block], preferred_element_type=f32))
        return total.astype(bf16)
    results = lax.map(one_expert, (buffer, expert_gate, expert_up, expert_down))
    picked = results[routes, row_slot].astype(f32)
    moe = lax.optimization_barrier(jnp.sum(route_w[:, :, None] * picked, axis=1))
    pre_gate = jnp.dot(normed2, dense_gate, preferred_element_type=f32)
    pre_up = jnp.dot(normed2, dense_up, preferred_element_type=f32)
    dense_hidden = (jax.nn.silu(pre_gate) * pre_up).astype(bf16)
    dense_block = DFF // N_TP
    dense_out = jnp.zeros((SEQUENCE_COUNT, D), f32)
    for part in range(N_TP):
        dense_out = dense_out + rounded(jnp.dot(dense_hidden[:, part * dense_block:(part + 1) * dense_block], dense_down[part * dense_block:(part + 1) * dense_block], preferred_element_type=f32))
    blend = jax.nn.sigmoid(jnp.dot(normed2, blend_weight, preferred_element_type=f32))
    new_tokens = (resid + moe + blend[:, None] * dense_out).astype(bf16)
    return (new_tokens, fresh_real, fresh_imaginary)
```

```python
import functools
import math

import jax
import jax.numpy as jnp
from jax import lax
from jax.experimental import pallas as pl
from jax.experimental.pallas import tpu as pltpu
from jax.sharding import PartitionSpec as P

EPS = 1e-06
F32 = jnp.float32
BF16 = jnp.bfloat16
HIGHEST = lax.Precision.HIGHEST
VMEM = pl.BlockSpec(memory_space=pltpu.VMEM)
SMEM = pl.BlockSpec(memory_space=pltpu.SMEM)
ANY = pl.BlockSpec(memory_space=pl.ANY)


def iota(shape, dim):
    return lax.broadcasted_iota(jnp.int32, shape, dim)


def nt_dot(a, b, precision=None):
    return lax.dot_general(
        a, b, (((1,), (1,)), ((), ())), precision=precision, preferred_element_type=F32
    )


def dot(a, b, precision=None):
    return jnp.dot(a, b, precision=precision, preferred_element_type=F32)


def cols_of(index, size):
    return pl.ds(pl.multiple_of(index * size, size), size)


def exchanged(value, mask):
    return lax.ppermute(value, "tp", [(i, i ^ mask) for i in range(4)])


def spread_blocks(small, channels):
    rows, entries = small.shape
    groups = rows // channels
    width = groups * entries
    tiler = (iota((entries, width), 1) % entries == iota((entries, width), 0)).astype(BF16)
    tiled = dot(small.astype(BF16), tiler)
    mine = iota((rows, width), 0) // channels == iota((rows, width), 1) // entries
    return jnp.where(mine, tiled, 0.0).astype(BF16)


def row_of(small):
    groups, n = small.shape
    width = groups * n
    tiler = (iota((n, width), 1) % n == iota((n, width), 0)).astype(F32)
    tiled = dot(small, tiler, HIGHEST)
    mine = iota((groups, width), 0) == iota((groups, width), 1) // n
    return jnp.sum(jnp.where(mine, tiled, 0.0), axis=0, keepdims=True)


def state_kernel(
    log_step, tokens, gain, in_weight, old_re, old_im, decay, b_re, b_im, c_re, c_im, skip,
    out_weight, gate, up, down,
    new_re, new_im, p0, p1, p2, p3, gu0, gu1, gu2, gu3, d0, d1, d2, d3, sems,
):
    t = lax.axis_index("tp")
    copies = []
    hid = gate.shape[1]
    for m, (gu, d) in enumerate(((gu0, d0), (gu1, d1), (gu2, d2), (gu3, d3))):
        part = cols_of(t ^ m, gu.shape[0])
        out = cols_of(t ^ m, d.shape[1])
        pairs = (
            (gate.at[part, :], gu.at[:, pl.ds(0, hid)]),
            (up.at[part, :], gu.at[:, pl.ds(hid, hid)]),
            (down.at[:, out], d),
        )
        for src, dst in pairs:
            copies.append(pltpu.make_async_copy(src, dst, sems.at[len(copies)]))
    for copy in copies:
        copy.start()
    groups, entries = decay.shape
    channels = skip.shape[1]
    x = tokens[...].astype(F32)
    scale = lax.rsqrt(jnp.mean(x * x, axis=-1, keepdims=True) + EPS)
    normed = (x * scale * gain[...].astype(F32)).astype(BF16)
    drive = dot(normed, in_weight[...]).astype(BF16)
    width = groups * entries
    of_group = iota((1, width), 1) // entries
    logs = jnp.zeros((1, width), F32)
    for g in range(groups):
        logs = jnp.where(of_group == g, log_step[g], logs)
    step = jnp.exp(logs)
    eigen = row_of(decay[...])
    freq = math.pi * (iota((1, width), 1) % entries).astype(F32)
    magnitude = jnp.exp(eigen * step)
    turned = freq * step
    lam_re = magnitude * jnp.cos(turned)
    lam_im = magnitude * jnp.sin(turned)
    denom = eigen * eigen + freq * freq
    fac_re = ((lam_re - 1.0) * eigen + lam_im * freq) / denom
    fac_im = (lam_im * eigen - (lam_re - 1.0) * freq) / denom
    in_re = dot(drive, spread_blocks(b_re[...], channels))
    in_im = dot(drive, spread_blocks(b_im[...], channels))
    was_re, was_im = old_re[...], old_im[...]
    fresh_re = lam_re * was_re - lam_im * was_im + (fac_re * in_re - fac_im * in_im)
    fresh_im = lam_re * was_im + lam_im * was_re + (fac_re * in_im + fac_im * in_re)
    new_re[...] = fresh_re
    new_im[...] = fresh_im
    mixed = (
        nt_dot(fresh_re.astype(BF16), spread_blocks(c_re[...], channels))
        - nt_dot(fresh_im.astype(BF16), spread_blocks(c_im[...], channels))
        + row_of(skip[...]) * drive.astype(F32)
    )
    act = jax.nn.gelu(mixed).astype(BF16)
    for m, p in enumerate((p0, p1, p2, p3)):
        p[...] = dot(act, out_weight[:, cols_of(t ^ m, p.shape[1])]).astype(BF16)
    for copy in copies:
        copy.wait()


def route_kernel(capacity, routes, group_weight, logits, z, w0, w1, share0, share1, padded):
    rows = routes.shape[1]
    lanes = padded.shape[1]
    slots = z.shape[0]
    blocks = z.shape[1] // lanes
    experts = slots // (capacity * blocks)
    padded[...] = jnp.full(padded.shape, -1, jnp.int32)
    padded[0:2, 0:rows] = routes[...]
    named = [padded[k : k + 1, :] for k in range(2)]
    hot = [(iota((experts, lanes), 0) == r).astype(F32) for r in named]
    earlier = (iota((lanes, lanes), 0) < iota((lanes, lanes), 1)).astype(BF16)
    before = dot((hot[0] + hot[1]).astype(BF16), earlier)
    eye = iota((lanes, lanes), 0) == iota((lanes, lanes), 1)
    place = [jnp.sum(before * h, axis=0, keepdims=True).astype(jnp.int32) for h in hot]
    slot = [
        jnp.where(r >= 0, r * (capacity * blocks) + p, -slots) for r, p in zip(named, place)
    ]
    for c in range(blocks):
        at = iota((slots, lanes), 0) - capacity * c
        z[:, c * lanes : (c + 1) * lanes] = (
            jnp.logical_or(at == slot[0], at == slot[1]).astype(F32).astype(BF16)
        )
    for k, w in enumerate((w0, w1)):
        column = jnp.sum(jnp.where(eye, slot[k], 0), axis=1, keepdims=True)[0:rows]
        for c in range(blocks):
            at = iota((rows, slots), 1) - capacity * c
            w[c * rows : (c + 1) * rows, :] = (at == column).astype(F32).astype(BF16)
    expo = jnp.exp(logits[...])
    share = group_weight[...] * expo / (expo[0:1] + expo[1:2])
    small_eye = iota((rows, rows), 0) == iota((rows, rows), 1)
    for k, out in enumerate((share0, share1)):
        column = jnp.sum(jnp.where(small_eye, share[k : k + 1], 0.0), axis=1, keepdims=True)
        out[...] = jnp.broadcast_to(column, out.shape)


def pack_kernel(tokens, p0, p1, p2, p3, z, resid, resid16, packed):
    t = lax.axis_index("tp")
    quarter = p0.shape[1]
    total = tokens[:, cols_of(t, quarter)].astype(F32) + (
        (p0[...].astype(F32) + p1[...].astype(F32)) + (p2[...].astype(F32) + p3[...].astype(F32))
    )
    resid[...] = total
    short = total.astype(BF16)
    resid16[...] = short
    rows = short.shape[0]
    lanes = packed.shape[1]
    gap = jnp.zeros((lanes - rows, lanes), BF16)
    pieces = []
    for c in range(quarter // lanes):
        pieces += [short[:, c * lanes : (c + 1) * lanes], gap]
    packed[...] = dot(z[...], jnp.concatenate(pieces, axis=0)).astype(BF16)


def dense_kernel(
    gains, a0, a1, a2, a3, gate, up, down, blend_weight, p0, p1, p2, p3, blend, full
):
    t = lax.axis_index("tp")
    quarter = a0.shape[1]
    for m, a in enumerate((a0, a1, a2, a3)):
        full[:, cols_of(t ^ m, quarter)] = a[...]
    x = full[...].astype(F32)
    scale = lax.rsqrt(jnp.mean(x * x, axis=-1, keepdims=True) + EPS)
    normed = (x * scale * gains[...].astype(F32)).astype(BF16)
    pre_gate = dot(normed, gate[...])
    pre_up = dot(normed, up[...])
    hidden = (jax.nn.silu(pre_gate) * pre_up).astype(BF16)
    for m, p in enumerate((p0, p1, p2, p3)):
        p[...] = dot(hidden, down[:, cols_of(t ^ m, quarter)]).astype(BF16)
    score = jnp.sum(
        normed.astype(F32) * blend_weight[...].astype(F32), axis=-1, keepdims=True
    )
    blend[...] = jnp.broadcast_to(jax.nn.sigmoid(score), blend.shape)


def enter_kernel(capacity, arrived, gains, gu0, gu1, gu2, gu3, keep, send, squares, wide, rows):
    t = lax.axis_index("tp")
    lanes = arrived.shape[1]
    quarter = rows.shape[1]
    blocks = quarter // lanes
    sources = arrived.shape[0] // (capacity * blocks)
    wide[...] = arrived[...].astype(F32)
    gain = gains[:, cols_of(t, quarter)].astype(F32)
    sums = []
    for s in range(capacity):
        total = jnp.zeros((sources, lanes), F32)
        for c in range(blocks):
            x = wide[pl.ds(c * capacity + s, sources, stride=capacity * blocks), :]
            total = total + x * x
            rows[s * sources : (s + 1) * sources, c * lanes : (c + 1) * lanes] = (
                x * gain[:, c * lanes : (c + 1) * lanes]
            ).astype(BF16)
        sums.append(total)
    squares[...] = nt_dot(
        jnp.ones((squares.shape[0], lanes), F32), jnp.concatenate(sums, axis=0), HIGHEST
    )
    x = rows[...]
    pair = gu0.shape[1]
    keep[:, 0:pair] = dot(x, gu0[...])
    send[:, 0:pair] = dot(x, gu1[...]).astype(BF16)
    keep[:, pair:] = dot(x, gu2[...])
    send[:, pair:] = dot(x, gu3[...]).astype(BF16)


def relay_kernel(keep, came, onward):
    pair = onward.shape[1]
    onward[...] = (keep[:, pair:] + came[:, pair:].astype(F32)).astype(BF16)


def hidden_kernel(width, keep, came, last, s0, s1, s2, s3, hidden):
    pair = last.shape[1]
    units = pair // 2
    total = keep[:, 0:pair] + came[:, 0:pair].astype(F32) + last[...].astype(F32)
    squares = (s0[...] + s1[...]) + (s2[...] + s3[...])
    scale = lax.rsqrt(jnp.transpose(squares)[:, 0:1] / width + EPS)
    hidden[...] = (jax.nn.silu(total[:, 0:units] * scale) * (total[:, units:] * scale)).astype(BF16)


def leave_kernel(capacity, hidden, d0, d1, d2, d3, out, wide):
    t = lax.axis_index("tp")
    lanes = out.shape[1]
    total = dot(hidden[t], d0[...])
    for m, d in ((1, d1), (2, d2), (3, d3)):
        total = total + dot(hidden[t ^ m], d[...])
    blocks = total.shape[1] // lanes
    sources = total.shape[0] // capacity
    for s in range(capacity):
        for c in range(blocks):
            wide[pl.ds(c * capacity + s, sources, stride=capacity * blocks), :] = total[
                s * sources : (s + 1) * sources, c * lanes : (c + 1) * lanes
            ]
    out[...] = wide[...].astype(BF16)


def final_kernel(returned, w0, w1, share0, share1, resid, blend, p0, p1, p2, p3, out):
    rows, quarter = resid.shape
    lanes = returned.shape[1]
    back = returned[...]
    first = dot(w0[...], back)
    second = dot(w1[...], back)
    for c in range(quarter // lanes):
        cols = slice(c * lanes, (c + 1) * lanes)
        near = slice(c * rows, (c + 1) * rows)
        moe = share0[...] * first[near] + share1[...] * second[near]
        dense = (p0[:, cols].astype(F32) + p1[:, cols].astype(F32)) + (
            p2[:, cols].astype(F32) + p3[:, cols].astype(F32)
        )
        out[:, cols] = (resid[:, cols] + moe + blend[...] * dense).astype(BF16)


def call(kernel, name, outs, ins, out_specs=None, scratch=()):
    return pl.pallas_call(
        kernel,
        name=name,
        out_shape=tuple(jax.ShapeDtypeStruct(s, d) for s, d in outs),
        in_specs=list(ins),
        out_specs=tuple(out_specs or [VMEM] * len(outs)),
        scratch_shapes=list(scratch),
    )


def per_device(
    tokens,
    norm_gain,
    in_weight,
    sequence_state_real,
    sequence_state_imaginary,
    eigen_decay_real,
    log_step,
    input_matrix_real,
    input_matrix_imaginary,
    output_matrix_real,
    output_matrix_imaginary,
    channel_skip_scale,
    out_weight,
    ffn_gain,
    routes,
    group_weight,
    expert_logit,
    expert_gate,
    expert_up,
    expert_down,
    dense_gate,
    dense_up,
    dense_down,
    blend_weight,
):
    rows, width = tokens.shape
    tp = lax.axis_size("tp")
    ep = lax.axis_size("ep")
    quarter = width // tp
    lanes = 128
    blocks = quarter // lanes
    capacity = max(2, 2 * rows * routes.shape[1] // (ep * expert_gate.shape[0]))
    slots = ep * capacity
    groups, entries, channels = input_matrix_real.shape
    hid = expert_gate.shape[2]
    gate = expert_gate.reshape(width, hid)
    up = expert_up.reshape(width, hid)
    down = expert_down.reshape(hid, width)
    piece = ((rows, quarter), BF16)

    def by_channel(matrix):
        return jnp.swapaxes(matrix, 1, 2).reshape(groups * channels, entries)

    states = ((rows, groups * entries), F32)
    new_re, new_im, *made = call(
        state_kernel,
        "state",
        [states] * 2
        + [piece] * 4
        + [((quarter, 2 * hid), BF16)] * 4
        + [((hid, quarter), BF16)] * 4,
        [SMEM] + [VMEM] * 12 + [ANY] * 3,
        [VMEM] * 6 + [ANY] * 8,
        [pltpu.SemaphoreType.DMA((12,))],
    )(
        log_step,
        tokens,
        norm_gain.reshape(1, width),
        in_weight,
        sequence_state_real,
        sequence_state_imaginary,
        eigen_decay_real,
        by_channel(input_matrix_real),
        by_channel(input_matrix_imaginary),
        output_matrix_real.reshape(groups * channels, entries),
        output_matrix_imaginary.reshape(groups * channels, entries),
        channel_skip_scale,
        out_weight,
        gate,
        up,
        down,
    )
    mix, gate_up, downs = made[0:4], made[4:8], made[8:12]
    mix = [mix[0]] + [exchanged(mix[m], m) for m in (1, 2, 3)]
    z, w0, w1, share0, share1 = call(
        functools.partial(route_kernel, capacity),
        "route",
        [((slots * blocks, lanes * blocks), BF16)]
        + [((rows * blocks, slots * blocks), BF16)] * 2
        + [((rows, lanes), F32)] * 2,
        [VMEM] * 3,
        scratch=[pltpu.VMEM((8, lanes), jnp.int32)],
    )(routes.T, group_weight.reshape(1, rows), expert_logit.T)
    resid, resid16, packed = call(
        pack_kernel,
        "pack",
        [((rows, quarter), F32), piece, ((slots * blocks, lanes), BF16)],
        [VMEM] * 6,
    )(tokens, *mix, z)
    arrived = lax.all_to_all(
        packed.reshape(ep, capacity * blocks, lanes), "ep", 0, 0, tiled=True
    ).reshape(slots * blocks, lanes)
    near = [resid16] + [exchanged(resid16, m) for m in (1, 2, 3)]
    gains = ffn_gain.reshape(1, width)
    *dense, blend = call(
        dense_kernel,
        "dense",
        [piece] * 4 + [((rows, lanes), F32)],
        [VMEM] * 9,
        scratch=[pltpu.VMEM((rows, width), BF16)],
    )(gains, *near, dense_gate, dense_up, dense_down, blend_weight.reshape(1, width))
    dense = [dense[0]] + [exchanged(dense[m], m) for m in (1, 2, 3)]
    gate_up = [gate_up[0]] + [exchanged(gate_up[m], m) for m in (1, 2, 3)]
    downs = [downs[0]] + [exchanged(downs[m], m) for m in (1, 2, 3)]
    keep, send, squares = call(
        functools.partial(enter_kernel, capacity),
        "enter",
        [((slots, 4 * hid), F32), ((slots, 4 * hid), BF16), ((8, slots), F32)],
        [VMEM] * 6,
        scratch=[
            pltpu.VMEM((slots * blocks, lanes), F32),
            pltpu.VMEM((slots, quarter), BF16),
        ],
    )(arrived, gains, *gate_up)
    came = exchanged(send, 1)
    squares = [squares] + [exchanged(squares, m) for m in (1, 2, 3)]
    (onward,) = call(relay_kernel, "relay", [((slots, 2 * hid), BF16)], [VMEM] * 2)(keep, came)
    last = exchanged(onward, 2)
    (hidden,) = call(
        functools.partial(hidden_kernel, float(width)),
        "hidden",
        [((slots, hid), BF16)],
        [VMEM] * 7,
    )(keep, came, last, *squares)
    hidden = lax.all_gather(hidden, "tp")
    (sent,) = call(
        functools.partial(leave_kernel, capacity),
        "leave",
        [((slots * blocks, lanes), BF16)],
        [VMEM] * 5,
        scratch=[pltpu.VMEM((slots * blocks, lanes), F32)],
    )(hidden, *downs)
    returned = lax.all_to_all(
        sent.reshape(ep, capacity * blocks, lanes), "ep", 0, 0, tiled=True
    ).reshape(slots * blocks, lanes)
    (new_tokens,) = call(final_kernel, "final", [piece], [VMEM] * 11)(
        returned, w0, w1, share0, share1, resid, blend, *dense
    )
    return (new_tokens, new_re, new_im)


def solution(mesh):
    in_specs = (
        P("ep", None),
        P(),
        P(None, "tp"),
        P("ep", "tp"),
        P("ep", "tp"),
        P("tp", None),
        P("tp"),
        P("tp", None, None),
        P("tp", None, None),
        P("tp", None, None),
        P("tp", None, None),
        P("tp", None),
        P("tp", None),
        P(),
        P("ep", None),
        P("ep"),
        P("ep", None),
        P("ep", None, "tp"),
        P("ep", None, "tp"),
        P("ep", "tp", None),
        P(None, "tp"),
        P(None, "tp"),
        P("tp", None),
        P(),
    )
    out_specs = (P("ep", "tp"), P("ep", "tp"), P("ep", "tp"))
    return jax.shard_map(
        per_device, mesh=mesh, in_specs=in_specs, out_specs=out_specs, check_vma=False
    )
```

```python
import functools
import math

import jax
import jax.numpy as jnp
from jax import lax
from jax.experimental import pallas as pl
from jax.experimental.pallas import tpu as pltpu
from jax.sharding import PartitionSpec as P

EPS = 1e-06
F32 = jnp.float32
BF16 = jnp.bfloat16
HIGHEST = lax.Precision.HIGHEST
VMEM = pl.BlockSpec(memory_space=pltpu.VMEM)
SMEM = pl.BlockSpec(memory_space=pltpu.SMEM)
ANY = pl.BlockSpec(memory_space=pl.ANY)
HBM = pl.BlockSpec(memory_space=pltpu.HBM)
FREE = pl.BlockSpec(memory_space=pltpu.VMEM)


def iota(shape, dim):
    return lax.broadcasted_iota(jnp.int32, shape, dim)


def nt_dot(a, b, precision=None):
    return lax.dot_general(
        a, b, (((1,), (1,)), ((), ())), precision=precision, preferred_element_type=F32
    )


def dot(a, b, precision=None):
    return jnp.dot(a, b, precision=precision, preferred_element_type=F32)


def cols_of(index, size):
    return pl.ds(pl.multiple_of(index * size, size), size)


def exchanged(value, mask):
    return lax.ppermute(value, "tp", [(i, i ^ mask) for i in range(4)])


def spread_blocks(small, channels):
    rows, entries = small.shape
    groups = rows // channels
    width = groups * entries
    tiler = (iota((entries, width), 1) % entries == iota((entries, width), 0)).astype(BF16)
    tiled = dot(small.astype(BF16), tiler)
    mine = iota((rows, width), 0) // channels == iota((rows, width), 1) // entries
    return jnp.where(mine, tiled, 0.0).astype(BF16)


def row_of(small):
    groups, n = small.shape
    width = groups * n
    tiler = (iota((n, width), 1) % n == iota((n, width), 0)).astype(F32)
    tiled = dot(small, tiler, HIGHEST)
    mine = iota((groups, width), 0) == iota((groups, width), 1) // n
    return jnp.sum(jnp.where(mine, tiled, 0.0), axis=0, keepdims=True)


def state_kernel(log_step, *refs):
    inputs, (p0, p1, p2, p3, new_re, new_im), held = refs[0:12], refs[12:18], refs[18:30]
    fresh_re_v, fresh_im_v, sems = refs[30:]
    t = lax.axis_index("tp")
    loads = [
        pltpu.make_async_copy(a, b, sems.at[i]) for i, (a, b) in enumerate(zip(inputs, held))
    ]
    for load in loads:
        load.start()
    decay, skip, tokens_v, gain, in_v, b_re, b_im, re_v, im_v, c_re, c_im, out_v = held
    groups, entries = decay.shape
    channels = skip.shape[1]
    width = groups * entries
    of_group = iota((1, width), 1) // entries
    logs = jnp.zeros((1, width), F32)
    for g in range(groups):
        logs = jnp.where(of_group == g, log_step[g], logs)
    step = jnp.exp(logs)
    loads[0].wait()
    eigen = row_of(decay[...])
    freq = math.pi * (iota((1, width), 1) % entries).astype(F32)
    magnitude = jnp.exp(eigen * step)
    turned = freq * step
    lam_re = magnitude * jnp.cos(turned)
    lam_im = magnitude * jnp.sin(turned)
    denom = eigen * eigen + freq * freq
    fac_re = ((lam_re - 1.0) * eigen + lam_im * freq) / denom
    fac_im = (lam_im * eigen - (lam_re - 1.0) * freq) / denom
    loads[2].wait()
    loads[3].wait()
    x = tokens_v[...].astype(F32)
    scale = lax.rsqrt(jnp.mean(x * x, axis=-1, keepdims=True) + EPS)
    normed = (x * scale * gain[...].astype(F32)).astype(BF16)
    loads[4].wait()
    drive = dot(normed, in_v[...]).astype(BF16)
    loads[5].wait()
    loads[6].wait()
    in_re = dot(drive, spread_blocks(b_re[...], channels))
    in_im = dot(drive, spread_blocks(b_im[...], channels))
    loads[7].wait()
    loads[8].wait()
    was_re, was_im = re_v[...], im_v[...]
    fresh_re = lam_re * was_re - lam_im * was_im + (fac_re * in_re - fac_im * in_im)
    fresh_im = lam_re * was_im + lam_im * was_re + (fac_re * in_im + fac_im * in_re)
    fresh_re_v[...] = fresh_re
    fresh_im_v[...] = fresh_im
    stores = [
        pltpu.make_async_copy(fresh_re_v, new_re, sems.at[12]),
        pltpu.make_async_copy(fresh_im_v, new_im, sems.at[13]),
    ]
    for store in stores:
        store.start()
    for i in (1, 9, 10):
        loads[i].wait()
    mixed = (
        nt_dot(fresh_re.astype(BF16), spread_blocks(c_re[...], channels))
        - nt_dot(fresh_im.astype(BF16), spread_blocks(c_im[...], channels))
        + row_of(skip[...]) * drive.astype(F32)
    )
    act = jax.nn.gelu(mixed).astype(BF16)
    loads[11].wait()
    for m, p in enumerate((p0, p1, p2, p3)):
        p[...] = dot(act, out_v[:, cols_of(t ^ m, p.shape[1])]).astype(BF16)
    for store in stores:
        store.wait()


def reshard_kernel(gate, up, down, gu1, gu2, gu3, d1, d2, d3):
    t = lax.axis_index("tp")
    hid = gate.shape[1]
    for m, gu, d in ((1, gu1, d1), (2, gu2, d2), (3, gu3, d3)):
        part = cols_of(t ^ m, gu.shape[0])
        gu[:, 0:hid] = gate[part, :]
        gu[:, hid:] = up[part, :]
        d[...] = down[:, cols_of(t ^ m, d.shape[1])]


def route_kernel(experts, routes, group_weight, logits, z, w, share0, share1, padded):
    rows = routes.shape[1]
    slots, lanes = z.shape
    padded[...] = jnp.full(padded.shape, -1, jnp.int32)
    padded[0:2, 0:rows] = routes[...]
    named = [padded[k : k + 1, :] for k in range(2)]
    hot = [(iota((experts, lanes), 0) == r).astype(F32) for r in named]
    earlier = (iota((lanes, lanes), 0) < iota((lanes, lanes), 1)).astype(BF16)
    before = dot((hot[0] + hot[1]).astype(BF16), earlier)
    place = [jnp.sum(before * h, axis=0, keepdims=True).astype(jnp.int32) for h in hot]
    slot = [jnp.where(r >= 0, p * experts + r, -1) for r, p in zip(named, place)]
    at = iota((slots, lanes), 0)
    z[...] = jnp.logical_or(at == slot[0], at == slot[1]).astype(F32).astype(BF16)
    eye = iota((lanes, lanes), 0) == iota((lanes, lanes), 1)
    at = iota((rows, slots), 1)
    for k in range(2):
        column = jnp.sum(jnp.where(eye, slot[k], 0), axis=1, keepdims=True)[0:rows]
        w[k * rows : (k + 1) * rows, :] = (at == column).astype(F32).astype(BF16)
    expo = jnp.exp(logits[...])
    share = group_weight[...] * expo / (expo[0:1] + expo[1:2])
    small_eye = iota((rows, rows), 0) == iota((rows, rows), 1)
    for k, out in enumerate((share0, share1)):
        column = jnp.sum(jnp.where(small_eye, share[k : k + 1], 0.0), axis=1, keepdims=True)
        out[...] = jnp.broadcast_to(column, out.shape)


def places(capacity, wide, quarter):
    blocks = quarter // wide.shape[1]
    peers = wide.shape[0] // (capacity * blocks)
    for s in range(capacity):
        for c in range(blocks):
            yield (
                pl.ds(c * capacity + s, peers, stride=capacity * blocks),
                slice(s * peers, (s + 1) * peers),
                slice(c * wide.shape[1], (c + 1) * wide.shape[1]),
            )


def pack_kernel(capacity, tokens, p0, p1, p2, p3, z, *refs):
    resid, resid16, packed, wide = refs[-4:]
    t = lax.axis_index("tp")
    quarter = p0.shape[1]
    total = tokens[:, cols_of(t, quarter)].astype(F32) + (
        (p0[...].astype(F32) + p1[...].astype(F32)) + (p2[...].astype(F32) + p3[...].astype(F32))
    )
    resid[...] = total
    short = total.astype(BF16)
    resid16[...] = short
    gap = jnp.zeros((z.shape[1] - short.shape[0], quarter), BF16)
    spread = dot(z[...], jnp.concatenate([short, gap], axis=0))
    for strided, near, cols in places(capacity, wide, quarter):
        wide[strided, :] = spread[near, cols]
    packed[...] = wide[...].astype(BF16)


def dense_kernel(
    gains, a0, a1, a2, a3, gate, up, down, blend_weight, p0, p1, p2, p3, blend, full
):
    t = lax.axis_index("tp")
    quarter = a0.shape[1]
    for m, a in enumerate((a0, a1, a2, a3)):
        full[:, cols_of(t ^ m, quarter)] = a[...]
    x = full[...].astype(F32)
    scale = lax.rsqrt(jnp.mean(x * x, axis=-1, keepdims=True) + EPS)
    normed = (x * scale * gains[...].astype(F32)).astype(BF16)
    pre_gate = dot(normed, gate[...])
    pre_up = dot(normed, up[...])
    hidden = (jax.nn.silu(pre_gate) * pre_up).astype(BF16)
    for m, p in enumerate((p0, p1, p2, p3)):
        p[...] = dot(hidden, down[:, cols_of(t ^ m, quarter)]).astype(BF16)
    score = jnp.sum(
        normed.astype(F32) * blend_weight[...].astype(F32), axis=-1, keepdims=True
    )
    blend[...] = jnp.broadcast_to(jax.nn.sigmoid(score), blend.shape)


def enter_kernel(capacity, arrived, gains, gate, up, gu1, gu2, gu3, *refs):
    keep, send, squares, wide, rows, sums = refs[-6:]
    t = lax.axis_index("tp")
    lanes = arrived.shape[1]
    quarter = rows.shape[1]
    wide[...] = arrived[...].astype(F32)
    gain = gains[:, cols_of(t, quarter)].astype(F32)
    for strided, near, cols in places(capacity, wide, quarter):
        x = wide[strided, :]
        sums[near, :] = x * x if cols.start == 0 else sums[near, :] + x * x
        rows[near, cols] = (x * gain[:, cols]).astype(BF16)
    squares[...] = nt_dot(jnp.ones((squares.shape[0], lanes), F32), sums[...], HIGHEST)
    x = rows[...]
    pair = gu1.shape[1]
    part = cols_of(t, quarter)
    keep[:, 0 : pair // 2] = dot(x, gate[part, :])
    keep[:, pair // 2 : pair] = dot(x, up[part, :])
    send[:, 0:pair] = dot(x, gu1[...]).astype(BF16)
    keep[:, pair:] = dot(x, gu2[...])
    send[:, pair:] = dot(x, gu3[...]).astype(BF16)


def relay_kernel(keep, came, onward):
    pair = onward.shape[1]
    onward[...] = (keep[:, pair:] + came[:, pair:].astype(F32)).astype(BF16)


def hidden_kernel(width, keep, came, last, s0, s1, s2, s3, hidden):
    pair = last.shape[1]
    units = pair // 2
    total = keep[:, 0:pair] + came[:, 0:pair].astype(F32) + last[...].astype(F32)
    squares = (s0[...] + s1[...]) + (s2[...] + s3[...])
    scale = lax.rsqrt(jnp.transpose(squares)[:, 0:1] / width + EPS)
    hidden[...] = (jax.nn.silu(total[:, 0:units] * scale) * (total[:, units:] * scale)).astype(BF16)


def leave_kernel(capacity, hidden, down, d1, d2, d3, out, wide):
    t = lax.axis_index("tp")
    total = dot(hidden[t], down[:, cols_of(t, d1.shape[1])])
    for m, d in ((1, d1), (2, d2), (3, d3)):
        total = total + dot(hidden[t ^ m], d[...])
    for strided, near, cols in places(capacity, wide, total.shape[1]):
        wide[strided, :] = total[near, cols]
    out[...] = wide[...].astype(BF16)


def final_kernel(
    capacity, returned, w, share0, share1, resid, blend, p0, p1, p2, p3, out, wide, rows
):
    count, quarter = resid.shape
    wide[...] = returned[...].astype(F32)
    for strided, near, cols in places(capacity, wide, quarter):
        rows[near, cols] = wide[strided, :].astype(BF16)
    picked = dot(w[...], rows[...])
    lanes = wide.shape[1]
    for c in range(quarter // lanes):
        cols = slice(c * lanes, (c + 1) * lanes)
        moe = share0[...] * picked[0:count, cols] + share1[...] * picked[count:, cols]
        dense = (p0[:, cols].astype(F32) + p1[:, cols].astype(F32)) + (
            p2[:, cols].astype(F32) + p3[:, cols].astype(F32)
        )
        out[:, cols] = (resid[:, cols] + moe + blend[...] * dense).astype(BF16)


def call(kernel, name, outs, scratch=(), limit=4, in_specs=None, out_specs=None):
    out_specs = out_specs or [VMEM] * len(outs)
    out_shape = [
        pltpu.VMEM(s, d) if spec is VMEM else jax.ShapeDtypeStruct(s, d)
        for (s, d), spec in zip(outs, out_specs)
    ]

    def run(*args):
        specs = in_specs or [VMEM] * len(args)
        spaces = {id(VMEM): pltpu.VMEM, id(HBM): pltpu.HBM}
        fixed = [
            pltpu.with_memory_space_constraint(a, spaces.get(id(spec), pl.ANY))
            for a, spec in zip(args, specs)
        ]
        return pl.pallas_call(
            kernel,
            name=name,
            out_shape=tuple(out_shape),
            in_specs=specs,
            out_specs=tuple(out_specs),
            scratch_shapes=list(scratch),
            compiler_params=pltpu.CompilerParams(vmem_limit_bytes=limit << 20),
        )(*fixed)

    return run


def per_device(
    tokens,
    norm_gain,
    in_weight,
    sequence_state_real,
    sequence_state_imaginary,
    eigen_decay_real,
    log_step,
    input_matrix_real,
    input_matrix_imaginary,
    output_matrix_real,
    output_matrix_imaginary,
    channel_skip_scale,
    out_weight,
    ffn_gain,
    routes,
    group_weight,
    expert_logit,
    expert_gate,
    expert_up,
    expert_down,
    dense_gate,
    dense_up,
    dense_down,
    blend_weight,
):
    rows, width = tokens.shape
    tp = lax.axis_size("tp")
    ep = lax.axis_size("ep")
    quarter = width // tp
    lanes = 128
    blocks = quarter // lanes
    capacity = max(2, 2 * rows * routes.shape[1] // (ep * expert_gate.shape[0]))
    slots = ep * capacity
    groups, entries, channels = input_matrix_real.shape
    hid = expert_gate.shape[2]
    gate = expert_gate.reshape(width, hid)
    up = expert_up.reshape(width, hid)
    down = expert_down.reshape(hid, width)
    piece = ((rows, quarter), BF16)

    def by_channel(matrix):
        return jnp.swapaxes(matrix, 1, 2).reshape(groups * channels, entries)

    states = ((rows, groups * entries), F32)
    state_inputs = (
        eigen_decay_real,
        channel_skip_scale,
        tokens,
        norm_gain.reshape(1, width),
        in_weight,
        by_channel(input_matrix_real),
        by_channel(input_matrix_imaginary),
        sequence_state_real,
        sequence_state_imaginary,
        output_matrix_real.reshape(groups * channels, entries),
        output_matrix_imaginary.reshape(groups * channels, entries),
        out_weight,
    )
    *mix, new_re, new_im = call(
        state_kernel,
        "state",
        [piece] * 4 + [states] * 2,
        [pltpu.VMEM(x.shape, x.dtype) for x in state_inputs]
        + [pltpu.VMEM(states[0], F32)] * 2
        + [pltpu.SemaphoreType.DMA((14,))],
        20,
        [SMEM] + [HBM] * 12,
        [VMEM] * 4 + [HBM] * 2,
    )(log_step, *state_inputs)
    mix = [mix[0]] + [exchanged(mix[m], m) for m in (1, 2, 3)]
    *moved, d1, d2, d3 = call(
        reshard_kernel,
        "reshard",
        [((quarter, 2 * hid), BF16)] * 3 + [((hid, quarter), BF16)] * 3,
    )(gate, up, down)
    z, w, share0, share1 = call(
        functools.partial(route_kernel, ep),
        "route",
        [((slots, lanes), BF16), ((2 * rows, slots), BF16)] + [((rows, lanes), F32)] * 2,
        [pltpu.VMEM((8, lanes), jnp.int32)],
    )(routes.T, group_weight.reshape(1, rows), expert_logit.T)
    wide = pltpu.VMEM((slots * blocks, lanes), F32)
    resid, resid16, packed = call(
        functools.partial(pack_kernel, capacity),
        "pack",
        [((rows, quarter), F32), piece, ((slots * blocks, lanes), BF16)],
        [wide],
        8,
        [VMEM] * 6 + [ANY],
    )(tokens, *mix, z, moved[0])
    moved = [exchanged(moved[m - 1], m) for m in (1, 2, 3)]
    downs = [exchanged(d, m) for m, d in ((1, d1), (2, d2), (3, d3))]
    arrived = lax.all_to_all(
        packed.reshape(ep, capacity * blocks, lanes), "ep", 0, 0, tiled=True
    ).reshape(slots * blocks, lanes)
    near = [resid16] + [exchanged(resid16, m) for m in (1, 2, 3)]
    gains = ffn_gain.reshape(1, width)
    *dense, blend = call(
        dense_kernel,
        "dense",
        [piece] * 4 + [((rows, lanes), F32)],
        [pltpu.VMEM((rows, width), BF16)],
        8,
    )(gains, *near, dense_gate, dense_up, dense_down, blend_weight.reshape(1, width))
    dense = [dense[0]] + [exchanged(dense[m], m) for m in (1, 2, 3)]
    keep, send, squares = call(
        functools.partial(enter_kernel, capacity),
        "enter",
        [((slots, 4 * hid), F32), ((slots, 4 * hid), BF16), ((8, slots), F32)],
        [wide, pltpu.VMEM((slots, quarter), BF16), pltpu.VMEM((slots, lanes), F32)],
        8,
        [VMEM] * 7 + [ANY] * 3,
    )(arrived, gains, gate, up, *moved, *near[1:])
    came = exchanged(send, 1)
    squares = [squares] + [exchanged(squares, m) for m in (1, 2, 3)]
    (onward,) = call(relay_kernel, "relay", [((slots, 2 * hid), BF16)])(keep, came)
    last = exchanged(onward, 2)
    (hidden,) = call(
        functools.partial(hidden_kernel, float(width)), "hidden", [((slots, hid), BF16)]
    )(keep, came, last, *squares)
    hidden = lax.all_gather(hidden, "tp")
    (sent,) = call(
        functools.partial(leave_kernel, capacity),
        "leave",
        [((slots * blocks, lanes), BF16)],
        [wide],
        8,
    )(hidden, down, *downs)
    returned = lax.all_to_all(
        sent.reshape(ep, capacity * blocks, lanes), "ep", 0, 0, tiled=True
    ).reshape(slots * blocks, lanes)
    (new_tokens,) = call(
        functools.partial(final_kernel, capacity),
        "final",
        [piece],
        [wide, pltpu.VMEM((slots, quarter), BF16)],
        8,
        out_specs=[FREE],
    )(returned, w, share0, share1, resid, blend, *dense)
    return (new_tokens, new_re, new_im)


def solution(mesh):
    in_specs = (
        P("ep", None),
        P(),
        P(None, "tp"),
        P("ep", "tp"),
        P("ep", "tp"),
        P("tp", None),
        P("tp"),
        P("tp", None, None),
        P("tp", None, None),
        P("tp", None, None),
        P("tp", None, None),
        P("tp", None),
        P("tp", None),
        P(),
        P("ep", None),
        P("ep"),
        P("ep", None),
        P("ep", None, "tp"),
        P("ep", None, "tp"),
        P("ep", "tp", None),
        P(None, "tp"),
        P(None, "tp"),
        P("tp", None),
        P(),
    )
    out_specs = (P("ep", "tp"), P("ep", "tp"), P("ep", "tp"))
    return jax.shard_map(
        per_device, mesh=mesh, in_specs=in_specs, out_specs=out_specs, check_vma=False
    )
```

```python
import functools
import math

import jax
import jax.numpy as jnp
from jax import lax
from jax.experimental import pallas as pl
from jax.experimental.pallas import tpu as pltpu
from jax.sharding import PartitionSpec as P


EPS = 1e-06
F32 = jnp.float32
BF16 = jnp.bfloat16
HIGHEST = lax.Precision.HIGHEST
VMEM = pl.BlockSpec(memory_space=pltpu.VMEM)
SMEM = pl.BlockSpec(memory_space=pltpu.SMEM)
ANY = pl.BlockSpec(memory_space=pl.ANY)
HBM = pl.BlockSpec(memory_space=pltpu.HBM)
FREE = pl.BlockSpec(memory_space=pltpu.VMEM)


def iota(shape, dim):
    return lax.broadcasted_iota(jnp.int32, shape, dim)


def nt_dot(a, b, precision=None):
    return lax.dot_general(
        a, b, (((1,), (1,)), ((), ())), precision=precision, preferred_element_type=F32
    )


def dot(a, b, precision=None):
    return jnp.dot(a, b, precision=precision, preferred_element_type=F32)


def cols_of(index, size):
    return pl.ds(pl.multiple_of(index * size, size), size)


def exchanged(value, mask):
    return lax.ppermute(value, "tp", [(i, i ^ mask) for i in range(4)])


def gathered(value):
    across = exchanged(value, 2)
    return [value, exchanged(value, 1), across, exchanged(across, 1)]


def spread_blocks(small, channels):
    rows, entries = small.shape
    groups = rows // channels
    width = groups * entries
    tiler = (iota((entries, width), 1) % entries == iota((entries, width), 0)).astype(BF16)
    tiled = dot(small.astype(BF16), tiler)
    mine = iota((rows, width), 0) // channels == iota((rows, width), 1) // entries
    return jnp.where(mine, tiled, 0.0).astype(BF16)


def row_of(small):
    groups, n = small.shape
    width = groups * n
    tiler = (iota((n, width), 1) % n == iota((n, width), 0)).astype(F32)
    tiled = dot(small, tiler, HIGHEST)
    mine = iota((groups, width), 0) == iota((groups, width), 1) // n
    return jnp.sum(jnp.where(mine, tiled, 0.0), axis=0, keepdims=True)


def state_kernel(*refs):
    inputs, (p0, p1, p2, p3, new_re, new_im), held = refs[0:13], refs[13:19], refs[19:32]
    fresh_re_v, fresh_im_v, sems = refs[32:]
    t = lax.axis_index("tp")
    loads = [
        pltpu.make_async_copy(a, b, sems.at[i]) for i, (a, b) in enumerate(zip(inputs, held))
    ]
    for load in loads:
        load.start()
    decay, skip, tokens_v, gain, in_v, b_re, b_im, re_v, im_v, c_re, c_im, out_v, log_step = held
    groups, entries = decay.shape
    channels = skip.shape[1]
    width = groups * entries
    of_group = iota((1, width), 1) // entries
    loads[12].wait()
    logs = jnp.zeros((1, width), F32)
    for g in range(groups):
        logs = jnp.where(of_group == g, log_step[g], logs)
    step = jnp.exp(logs)
    loads[0].wait()
    eigen = row_of(decay[...])
    freq = math.pi * (iota((1, width), 1) % entries).astype(F32)
    magnitude = jnp.exp(eigen * step)
    turned = freq * step
    lam_re = magnitude * jnp.cos(turned)
    lam_im = magnitude * jnp.sin(turned)
    denom = eigen * eigen + freq * freq
    fac_re = ((lam_re - 1.0) * eigen + lam_im * freq) / denom
    fac_im = (lam_im * eigen - (lam_re - 1.0) * freq) / denom
    loads[2].wait()
    loads[3].wait()
    x = tokens_v[...].astype(F32)
    scale = lax.rsqrt(jnp.mean(x * x, axis=-1, keepdims=True) + EPS)
    normed = (x * scale * gain[...].astype(F32).reshape(1, -1)).astype(BF16)
    loads[4].wait()
    drive = dot(normed, in_v[...]).astype(BF16)
    loads[5].wait()
    loads[6].wait()
    in_re = dot(drive, spread_blocks(b_re[...], channels))
    in_im = dot(drive, spread_blocks(b_im[...], channels))
    loads[7].wait()
    loads[8].wait()
    was_re, was_im = re_v[...], im_v[...]
    fresh_re = lam_re * was_re - lam_im * was_im + (fac_re * in_re - fac_im * in_im)
    fresh_im = lam_re * was_im + lam_im * was_re + (fac_re * in_im + fac_im * in_re)
    fresh_re_v[...] = fresh_re
    fresh_im_v[...] = fresh_im
    stores = [
        pltpu.make_async_copy(fresh_re_v, new_re, sems.at[13]),
        pltpu.make_async_copy(fresh_im_v, new_im, sems.at[14]),
    ]
    for store in stores:
        store.start()
    for i in (1, 9, 10):
        loads[i].wait()
    mixed = (
        nt_dot(fresh_re.astype(BF16), spread_blocks(c_re[...], channels))
        - nt_dot(fresh_im.astype(BF16), spread_blocks(c_im[...], channels))
        + row_of(skip[...]) * drive.astype(F32)
    )
    act = jax.nn.gelu(mixed).astype(BF16)
    loads[11].wait()
    for m, p in enumerate((p0, p1, p2, p3)):
        p[...] = dot(act, out_v[:, cols_of(t ^ m, p.shape[1])]).astype(BF16)
    for store in stores:
        store.wait()


def reshard_kernel(gate, up, down, *pieces):
    t = lax.axis_index("tp")
    hid = gate.shape[1]
    for m, (gu, d) in enumerate(zip(pieces[:4], pieces[4:])):
        part = cols_of(t ^ m, gu.shape[0])
        gu[:, 0:hid] = gate[part, :]
        gu[:, hid:] = up[part, :]
        d[...] = down[:, cols_of(t ^ m, d.shape[1])]


def route_kernel(experts, routes, group_weight, logits, z, w, share0, share1, padded):
    rows = routes.shape[1]
    slots, lanes = z.shape
    padded[...] = jnp.full(padded.shape, -1, jnp.int32)
    padded[0:2, 0:rows] = routes[...]
    named = [padded[k : k + 1, :] for k in range(2)]
    hot = [(iota((experts, lanes), 0) == r).astype(F32) for r in named]
    earlier = (iota((lanes, lanes), 0) < iota((lanes, lanes), 1)).astype(BF16)
    before = dot((hot[0] + hot[1]).astype(BF16), earlier)
    place = [jnp.sum(before * h, axis=0, keepdims=True).astype(jnp.int32) for h in hot]
    slot = [jnp.where(r >= 0, p * experts + r, -1) for r, p in zip(named, place)]
    at = iota((slots, lanes), 0)
    z[...] = jnp.logical_or(at == slot[0], at == slot[1]).astype(F32).astype(BF16)
    eye = iota((lanes, lanes), 0) == iota((lanes, lanes), 1)
    at = iota((rows, slots), 1)
    for k in range(2):
        column = jnp.sum(jnp.where(eye, slot[k], 0), axis=1, keepdims=True)[0:rows]
        w[k * rows : (k + 1) * rows, :] = (at == column).astype(F32).astype(BF16)
    expo = jnp.exp(logits[...])
    share = group_weight[...] * expo / (expo[0:1] + expo[1:2])
    small_eye = iota((rows, rows), 0) == iota((rows, rows), 1)
    for k, out in enumerate((share0, share1)):
        column = jnp.sum(jnp.where(small_eye, share[k : k + 1], 0.0), axis=1, keepdims=True)
        out[...] = jnp.broadcast_to(column, out.shape)


def places(capacity, wide, quarter):
    blocks = quarter // wide.shape[1]
    peers = wide.shape[0] // (capacity * blocks)
    for s in range(capacity):
        for c in range(blocks):
            yield (
                pl.ds(c * capacity + s, peers, stride=capacity * blocks),
                slice(s * peers, (s + 1) * peers),
                slice(c * wide.shape[1], (c + 1) * wide.shape[1]),
            )


def three_terms(row, size):
    if row.shape[1] < size:
        row = jnp.concatenate([row, jnp.zeros((1, size - row.shape[1]), F32)], axis=1)
    high = row.astype(BF16).astype(F32)
    middle = (row - high).astype(BF16).astype(F32)
    low = row - high - middle
    at = iota((8, size), 0)
    block = jnp.where(at == 0, high, jnp.where(at == 1, middle, jnp.where(at == 2, low, 0.0)))
    return block.astype(BF16)


def sum_terms(block):
    return jnp.sum(block.astype(F32), axis=0, keepdims=True)


def pack_kernel(capacity, tokens, p0, p1, p2, p3, z, *refs):
    resid16, packed, wide = refs[-3:]
    t = lax.axis_index("tp")
    quarter = p0.shape[1]
    total = tokens[:, cols_of(t, quarter)].astype(F32) + (
        (p0[...].astype(F32) + p1[...].astype(F32)) + (p2[...].astype(F32) + p3[...].astype(F32))
    )
    short = total.astype(BF16)
    resid16[...] = short
    gap = jnp.zeros((z.shape[1] - short.shape[0], quarter), BF16)
    spread = dot(z[...], jnp.concatenate([short, gap], axis=0))
    for strided, near, cols in places(capacity, wide, quarter):
        wide[strided, :] = spread[near, cols]
    packed[...] = wide[...].astype(BF16)


def dense_kernel(
    gains, a0, a1, a2, a3, blend_weight, gate, up, down, p0, p1, p2, p3, blend,
    full, gate_v, up_v, down_v, sems,
):
    t = lax.axis_index("tp")
    loads = [
        pltpu.make_async_copy(a, b, sems.at[i])
        for i, (a, b) in enumerate(((gate, gate_v), (up, up_v), (down, down_v)))
    ]
    for load in loads:
        load.start()
    quarter = a0.shape[1]
    for m, a in enumerate((a0, a1, a2, a3)):
        full[:, cols_of(t ^ m, quarter)] = a[...]
    x = full[...].astype(F32)
    scale = lax.rsqrt(jnp.mean(x * x, axis=-1, keepdims=True) + EPS)
    normed = (x * scale * gains[...].astype(F32)).astype(BF16)
    score = jnp.sum(
        normed.astype(F32) * blend_weight[...].astype(F32), axis=-1, keepdims=True
    )
    blend[...] = jnp.broadcast_to(jax.nn.sigmoid(score), blend.shape)
    loads[0].wait()
    pre_gate = dot(normed, gate_v[...])
    loads[1].wait()
    pre_up = dot(normed, up_v[...])
    hidden = (jax.nn.silu(pre_gate) * pre_up).astype(BF16)
    loads[2].wait()
    for m, p in enumerate((p0, p1, p2, p3)):
        p[...] = dot(hidden, down_v[:, cols_of(t ^ m, quarter)]).astype(BF16)


def enter_kernel(capacity, arrived, gains, gu0, gu1, gu2, gu3, keep, send, wide, rows, sums):
    t = lax.axis_index("tp")
    lanes = arrived.shape[1]
    quarter = rows.shape[1]
    wide[...] = arrived[...].astype(F32)
    gain = gains[:, cols_of(t, quarter)].astype(F32)
    for strided, near, cols in places(capacity, wide, quarter):
        x = wide[strided, :]
        sums[near, :] = x * x if cols.start == 0 else sums[near, :] + x * x
        rows[near, cols] = (x * gain[:, cols]).astype(BF16)
    squares = nt_dot(jnp.ones((8, lanes), F32), sums[...], HIGHEST)[0:1]
    count = rows.shape[0]
    keep[count:, :] = jnp.broadcast_to(
        jnp.concatenate([squares, jnp.zeros((1, keep.shape[1] - count), F32)], axis=1),
        (8, keep.shape[1]),
    )
    send[count:, :] = three_terms(squares, send.shape[1])
    x = rows[...]
    pair = gu0.shape[1]
    keep[0:count, 0:pair] = dot(x, gu0[...])
    send[0:count, 0:pair] = dot(x, gu1[...]).astype(BF16)
    keep[0:count, pair:] = dot(x, gu2[...])
    send[0:count, pair:] = dot(x, gu3[...]).astype(BF16)


def relay_kernel(keep, came, onward):
    pair = onward.shape[1]
    count = keep.shape[0] - 8
    onward[0:count, :] = (keep[0:count, pair:] + came[0:count, pair:].astype(F32)).astype(BF16)
    squares = keep[count : count + 1, :] + sum_terms(came[count:, :])
    onward[count : count + 8, :] = three_terms(squares[:, 0:pair], pair)
    onward[count + 8 :, :] = three_terms(squares[:, pair:], pair)


def hidden_kernel(width, keep, came, last, hidden):
    count, units = hidden.shape
    pair = 2 * units
    total = (
        keep[0:count, 0:pair] + came[0:count, 0:pair].astype(F32) + last[0:count, :].astype(F32)
    )
    squares = keep[count : count + 1, :] + sum_terms(came[count:, :])
    squares = squares + jnp.concatenate(
        [sum_terms(last[count : count + 8, :]), sum_terms(last[count + 8 :, :])], axis=1
    )
    column = jnp.transpose(jnp.broadcast_to(squares[:, 0:count], (8, count)))[:, 0:1]
    scale = lax.rsqrt(column / width + EPS)
    hidden[...] = (jax.nn.silu(total[:, 0:units] * scale) * (total[:, units:] * scale)).astype(BF16)


def leave_kernel(capacity, h0, h1, h2, h3, d0, d1, d2, d3, out, wide):
    total = dot(h0[...], d0[...])
    for h, d in ((h1, d1), (h2, d2), (h3, d3)):
        total = total + dot(h[...], d[...])
    for strided, near, cols in places(capacity, wide, total.shape[1]):
        wide[strided, :] = total[near, cols]
    out[...] = wide[...].astype(BF16)


def final_kernel(
    capacity, returned, w, share0, share1, resid, blend, p0, p1, p2, p3, out, wide, rows
):
    count, quarter = resid.shape
    wide[...] = returned[...].astype(F32)
    for strided, near, cols in places(capacity, wide, quarter):
        rows[near, cols] = wide[strided, :].astype(BF16)
    picked = dot(w[...], rows[...])
    lanes = wide.shape[1]
    for c in range(quarter // lanes):
        cols = slice(c * lanes, (c + 1) * lanes)
        moe = share0[...] * picked[0:count, cols] + share1[...] * picked[count:, cols]
        dense = (p0[:, cols].astype(F32) + p1[:, cols].astype(F32)) + (
            p2[:, cols].astype(F32) + p3[:, cols].astype(F32)
        )
        out[:, cols] = (resid[:, cols].astype(F32) + moe + blend[...] * dense).astype(BF16)


def call(kernel, outs, scratch=(), limit=4, in_specs=None, out_specs=None):
    out_specs = out_specs or [VMEM] * len(outs)
    out_shape = [
        pltpu.VMEM(s, d) if spec is VMEM else jax.ShapeDtypeStruct(s, d)
        for (s, d), spec in zip(outs, out_specs)
    ]

    def run(*args):
        specs = in_specs or [VMEM] * len(args)
        spaces = {id(VMEM): pltpu.VMEM, id(HBM): pltpu.HBM}
        fixed = [
            pltpu.with_memory_space_constraint(a, spaces.get(id(spec), pl.ANY))
            for a, spec in zip(args, specs)
        ]
        return pl.pallas_call(
            kernel,
            out_shape=tuple(out_shape),
            in_specs=specs,
            out_specs=tuple(out_specs),
            scratch_shapes=list(scratch),
            compiler_params=pltpu.CompilerParams(vmem_limit_bytes=limit << 20),
        )(*fixed)

    return run


def per_device(
    tokens,
    norm_gain,
    in_weight,
    sequence_state_real,
    sequence_state_imaginary,
    eigen_decay_real,
    log_step,
    input_matrix_real,
    input_matrix_imaginary,
    output_matrix_real,
    output_matrix_imaginary,
    channel_skip_scale,
    out_weight,
    ffn_gain,
    routes,
    group_weight,
    expert_logit,
    expert_gate,
    expert_up,
    expert_down,
    dense_gate,
    dense_up,
    dense_down,
    blend_weight,
):
    rows, width = tokens.shape
    tp = lax.axis_size("tp")
    ep = lax.axis_size("ep")
    quarter = width // tp
    lanes = 128
    blocks = quarter // lanes
    capacity = max(2, 2 * rows * routes.shape[1] // (ep * expert_gate.shape[0]))
    slots = ep * capacity
    groups, entries, channels = input_matrix_real.shape
    hid = expert_gate.shape[2]
    gate = expert_gate.reshape(width, hid)
    up = expert_up.reshape(width, hid)
    down = expert_down.reshape(hid, width)
    piece = ((rows, quarter), BF16)

    def by_channel(matrix):
        return jnp.swapaxes(matrix, 1, 2).reshape(groups * channels, entries)

    states = ((rows, groups * entries), F32)
    state_inputs = (
        eigen_decay_real,
        channel_skip_scale,
        tokens,
        norm_gain,
        in_weight,
        by_channel(input_matrix_real),
        by_channel(input_matrix_imaginary),
        sequence_state_real,
        sequence_state_imaginary,
        output_matrix_real.reshape(groups * channels, entries),
        output_matrix_imaginary.reshape(groups * channels, entries),
        out_weight,
        log_step,
    )
    *mix, new_re, new_im = call(
        state_kernel,
        [piece] * 4 + [states] * 2,
        [pltpu.VMEM(x.shape, x.dtype) for x in state_inputs[:-1]]
        + [pltpu.SMEM(log_step.shape, F32)]
        + [pltpu.VMEM(states[0], F32)] * 2
        + [pltpu.SemaphoreType.DMA((15,))],
        20,
        [HBM] * 13,
        [VMEM] * 4 + [HBM] * 2,
    )(*state_inputs)
    mix = [mix[0]] + [exchanged(mix[m], m) for m in (1, 2, 3)]
    pieces = call(
        reshard_kernel, [((quarter, 2 * hid), BF16)] * 4 + [((hid, quarter), BF16)] * 4
    )(gate, up, down)
    moved = [pieces[0]] + [exchanged(pieces[m], m) for m in (1, 2, 3)]
    downs = [pieces[4]] + [exchanged(pieces[4 + m], m) for m in (1, 2, 3)]
    z, w, share0, share1 = call(
        functools.partial(route_kernel, ep),
        [((slots, lanes), BF16), ((2 * rows, slots), BF16)] + [((rows, lanes), F32)] * 2,
        [pltpu.VMEM((8, lanes), jnp.int32)],
    )(routes.T, group_weight.reshape(1, rows), expert_logit.T)
    wide = pltpu.VMEM((slots * blocks, lanes), F32)
    resid16, packed = call(
        functools.partial(pack_kernel, capacity),
        [piece, ((slots * blocks, lanes), BF16)],
        [wide],
        8,
        out_specs=[VMEM, FREE],
    )(tokens, *mix, z)
    arrived = lax.all_to_all(
        packed.reshape(ep, capacity * blocks, lanes), "ep", 0, 0, tiled=True
    ).reshape(slots * blocks, lanes)
    near = gathered(resid16)
    gains = ffn_gain.reshape(1, width)
    *dense, blend = call(
        dense_kernel,
        [piece] * 4 + [((rows, lanes), F32)],
        [pltpu.VMEM((rows, width), BF16)]
        + [pltpu.VMEM(x.shape, BF16) for x in (dense_gate, dense_up, dense_down)]
        + [pltpu.SemaphoreType.DMA((3,))],
        12,
        [VMEM] * 6 + [HBM] * 3,
    )(gains, *near, blend_weight.reshape(1, width), dense_gate, dense_up, dense_down)
    dense = [dense[0]] + [exchanged(dense[m], m) for m in (1, 2, 3)]
    keep, send = call(
        functools.partial(enter_kernel, capacity),
        [((slots + 8, 4 * hid), F32), ((slots + 8, 4 * hid), BF16)],
        [wide, pltpu.VMEM((slots, quarter), BF16), pltpu.VMEM((slots, lanes), F32)],
        8,
    )(arrived, gains, *moved)
    came = exchanged(send, 1)
    (onward,) = call(relay_kernel, [((slots + 16, 2 * hid), BF16)])(keep, came)
    last = exchanged(onward, 2)
    (hidden,) = call(
        functools.partial(hidden_kernel, float(width)), [((slots, hid), BF16)]
    )(keep, came, last)
    (sent,) = call(
        functools.partial(leave_kernel, capacity),
        [((slots * blocks, lanes), BF16)],
        [wide],
        8,
        out_specs=[FREE],
    )(*gathered(hidden), *downs)
    returned = lax.all_to_all(
        sent.reshape(ep, capacity * blocks, lanes), "ep", 0, 0, tiled=True
    ).reshape(slots * blocks, lanes)
    (new_tokens,) = call(
        functools.partial(final_kernel, capacity),
        [piece],
        [wide, pltpu.VMEM((slots, quarter), BF16)],
        8,
        out_specs=[FREE],
    )(returned, w, share0, share1, resid16, blend, *dense)
    return (new_tokens, new_re, new_im)


def solution(mesh):
    in_specs = (
        P("ep", None),
        P(),
        P(None, "tp"),
        P("ep", "tp"),
        P("ep", "tp"),
        P("tp", None),
        P("tp"),
        P("tp", None, None),
        P("tp", None, None),
        P("tp", None, None),
        P("tp", None, None),
        P("tp", None),
        P("tp", None),
        P(),
        P("ep", None),
        P("ep"),
        P("ep", None),
        P("ep", None, "tp"),
        P("ep", None, "tp"),
        P("ep", "tp", None),
        P(None, "tp"),
        P(None, "tp"),
        P("tp", None),
        P(),
    )
    out_specs = (P("ep", "tp"), P("ep", "tp"), P("ep", "tp"))

    return jax.shard_map(
        per_device, mesh=mesh, in_specs=in_specs, out_specs=out_specs, check_vma=False
    )
```

```python
import functools
import math

import jax
import jax.numpy as jnp
from jax import lax
from jax.experimental import pallas as pl
from jax.experimental.pallas import tpu as pltpu
from jax.sharding import PartitionSpec as P


EPS = 1e-06
F32 = jnp.float32
BF16 = jnp.bfloat16
HIGHEST = lax.Precision.HIGHEST
VMEM = pl.BlockSpec(memory_space=pltpu.VMEM)
SMEM = pl.BlockSpec(memory_space=pltpu.SMEM)
ANY = pl.BlockSpec(memory_space=pl.ANY)
HBM = pl.BlockSpec(memory_space=pltpu.HBM)
FREE = pl.BlockSpec(memory_space=pltpu.VMEM)


def iota(shape, dim):
    return lax.broadcasted_iota(jnp.int32, shape, dim)


def nt_dot(a, b, precision=None):
    return lax.dot_general(
        a, b, (((1,), (1,)), ((), ())), precision=precision, preferred_element_type=F32
    )


def dot(a, b, precision=None):
    return jnp.dot(a, b, precision=precision, preferred_element_type=F32)


def cols_of(index, size):
    return pl.ds(pl.multiple_of(index * size, size), size)


def exchanged(value, mask):
    return lax.ppermute(value, "tp", [(i, i ^ mask) for i in range(4)])


def gathered(value):
    across = exchanged(value, 2)
    return [value, exchanged(value, 1), across, exchanged(across, 1)]


def spread_blocks(small, channels):
    rows, entries = small.shape
    groups = rows // channels
    width = groups * entries
    tiler = (iota((entries, width), 1) % entries == iota((entries, width), 0)).astype(BF16)
    tiled = dot(small.astype(BF16), tiler)
    mine = iota((rows, width), 0) // channels == iota((rows, width), 1) // entries
    return jnp.where(mine, tiled, 0.0).astype(BF16)


def row_of(small):
    groups, n = small.shape
    width = groups * n
    tiler = (iota((n, width), 1) % n == iota((n, width), 0)).astype(F32)
    tiled = dot(small, tiler, HIGHEST)
    mine = iota((groups, width), 0) == iota((groups, width), 1) // n
    return jnp.sum(jnp.where(mine, tiled, 0.0), axis=0, keepdims=True)


def state_kernel(*refs):
    inputs, (p0, p1, p2, p3, new_re, new_im), held = refs[0:13], refs[13:19], refs[19:32]
    fresh_re_v, fresh_im_v, sems = refs[32:]
    t = lax.axis_index("tp")
    loads = [
        pltpu.make_async_copy(a, b, sems.at[i]) for i, (a, b) in enumerate(zip(inputs, held))
    ]
    for load in loads:
        load.start()
    decay, skip, tokens_v, gain, in_v, b_re, b_im, re_v, im_v, c_re, c_im, out_v, log_step = held
    groups, entries = decay.shape
    channels = skip.shape[1]
    width = groups * entries
    of_group = iota((1, width), 1) // entries
    loads[12].wait()
    logs = jnp.zeros((1, width), F32)
    for g in range(groups):
        logs = jnp.where(of_group == g, log_step[g], logs)
    step = jnp.exp(logs)
    loads[0].wait()
    eigen = row_of(decay[...])
    freq = math.pi * (iota((1, width), 1) % entries).astype(F32)
    magnitude = jnp.exp(eigen * step)
    turned = freq * step
    lam_re = magnitude * jnp.cos(turned)
    lam_im = magnitude * jnp.sin(turned)
    denom = eigen * eigen + freq * freq
    fac_re = ((lam_re - 1.0) * eigen + lam_im * freq) / denom
    fac_im = (lam_im * eigen - (lam_re - 1.0) * freq) / denom
    loads[2].wait()
    loads[3].wait()
    x = tokens_v[...].astype(F32)
    scale = lax.rsqrt(jnp.mean(x * x, axis=-1, keepdims=True) + EPS)
    normed = (x * scale * gain[...].astype(F32).reshape(1, -1)).astype(BF16)
    loads[4].wait()
    drive = dot(normed, in_v[...]).astype(BF16)
    loads[5].wait()
    loads[6].wait()
    in_re = dot(drive, spread_blocks(b_re[...], channels))
    in_im = dot(drive, spread_blocks(b_im[...], channels))
    loads[7].wait()
    loads[8].wait()
    was_re, was_im = re_v[...], im_v[...]
    fresh_re = lam_re * was_re - lam_im * was_im + (fac_re * in_re - fac_im * in_im)
    fresh_im = lam_re * was_im + lam_im * was_re + (fac_re * in_im + fac_im * in_re)
    fresh_re_v[...] = fresh_re
    fresh_im_v[...] = fresh_im
    stores = [
        pltpu.make_async_copy(fresh_re_v, new_re, sems.at[13]),
        pltpu.make_async_copy(fresh_im_v, new_im, sems.at[14]),
    ]
    for store in stores:
        store.start()
    for i in (1, 9, 10):
        loads[i].wait()
    mixed = (
        nt_dot(fresh_re.astype(BF16), spread_blocks(c_re[...], channels))
        - nt_dot(fresh_im.astype(BF16), spread_blocks(c_im[...], channels))
        + row_of(skip[...]) * drive.astype(F32)
    )
    act = jax.nn.gelu(mixed).astype(BF16)
    loads[11].wait()
    for m, p in enumerate((p0, p1, p2, p3)):
        p[...] = dot(act, out_v[:, cols_of(t ^ m, p.shape[1])]).astype(BF16)
    for store in stores:
        store.wait()


def reshard_kernel(gate, up, down, *pieces):
    t = lax.axis_index("tp")
    hid = gate.shape[1]
    for m, piece in enumerate(pieces):
        rows = piece.shape[0] - 2 * hid
        part = cols_of(t ^ m, rows)
        piece[0:rows, 0:hid] = gate[part, :]
        piece[0:rows, hid:] = up[part, :]
        for half in range(2):
            low = rows + half * hid
            piece[low : low + hid, :] = down[:, cols_of(2 * (t ^ m) + half, 2 * hid)]


def route_kernel(experts, routes, group_weight, logits, z, w, share0, share1, padded):
    rows = routes.shape[1]
    slots, lanes = z.shape
    padded[...] = jnp.full(padded.shape, -1, jnp.int32)
    padded[0:2, 0:rows] = routes[...]
    named = [padded[k : k + 1, :] for k in range(2)]
    hot = [(iota((experts, lanes), 0) == r).astype(F32) for r in named]
    earlier = (iota((lanes, lanes), 0) < iota((lanes, lanes), 1)).astype(BF16)
    before = dot((hot[0] + hot[1]).astype(BF16), earlier)
    place = [jnp.sum(before * h, axis=0, keepdims=True).astype(jnp.int32) for h in hot]
    slot = [jnp.where(r >= 0, p * experts + r, -1) for r, p in zip(named, place)]
    at = iota((slots, lanes), 0)
    z[...] = jnp.logical_or(at == slot[0], at == slot[1]).astype(F32).astype(BF16)
    eye = iota((lanes, lanes), 0) == iota((lanes, lanes), 1)
    at = iota((rows, slots), 1)
    for k in range(2):
        column = jnp.sum(jnp.where(eye, slot[k], 0), axis=1, keepdims=True)[0:rows]
        w[k * rows : (k + 1) * rows, :] = (at == column).astype(F32).astype(BF16)
    expo = jnp.exp(logits[...])
    share = group_weight[...] * expo / (expo[0:1] + expo[1:2])
    small_eye = iota((rows, rows), 0) == iota((rows, rows), 1)
    for k, out in enumerate((share0, share1)):
        column = jnp.sum(jnp.where(small_eye, share[k : k + 1], 0.0), axis=1, keepdims=True)
        out[...] = jnp.broadcast_to(column, out.shape)


def places(capacity, wide, quarter):
    blocks = quarter // wide.shape[1]
    peers = wide.shape[0] // (capacity * blocks)
    for s in range(capacity):
        for c in range(blocks):
            yield (
                pl.ds(c * capacity + s, peers, stride=capacity * blocks),
                slice(s * peers, (s + 1) * peers),
                slice(c * wide.shape[1], (c + 1) * wide.shape[1]),
            )


def three_terms(row, size):
    if row.shape[1] < size:
        row = jnp.concatenate([row, jnp.zeros((1, size - row.shape[1]), F32)], axis=1)
    high = row.astype(BF16).astype(F32)
    middle = (row - high).astype(BF16).astype(F32)
    low = row - high - middle
    at = iota((8, size), 0)
    block = jnp.where(at == 0, high, jnp.where(at == 1, middle, jnp.where(at == 2, low, 0.0)))
    return block.astype(BF16)


def sum_terms(block):
    return jnp.sum(block.astype(F32), axis=0, keepdims=True)


def pack_kernel(capacity, tokens, p0, p1, p2, p3, z, *refs):
    resid16, packed, wide = refs[-3:]
    t = lax.axis_index("tp")
    quarter = p0.shape[1]
    total = tokens[:, cols_of(t, quarter)].astype(F32) + (
        (p0[...].astype(F32) + p1[...].astype(F32)) + (p2[...].astype(F32) + p3[...].astype(F32))
    )
    short = total.astype(BF16)
    resid16[...] = short
    gap = jnp.zeros((z.shape[1] - short.shape[0], quarter), BF16)
    spread = dot(z[...], jnp.concatenate([short, gap], axis=0))
    for strided, near, cols in places(capacity, wide, quarter):
        wide[strided, :] = spread[near, cols]
    packed[...] = wide[...].astype(BF16)


def dense_kernel(
    gains, a0, a1, a2, a3, blend_weight, gate, up, down, p0, p1, p2, p3, blend,
    full, gate_v, up_v, down_v, sems,
):
    t = lax.axis_index("tp")
    loads = [
        pltpu.make_async_copy(a, b, sems.at[i])
        for i, (a, b) in enumerate(((gate, gate_v), (up, up_v), (down, down_v)))
    ]
    for load in loads:
        load.start()
    quarter = a0.shape[1]
    for m, a in enumerate((a0, a1, a2, a3)):
        full[:, cols_of(t ^ m, quarter)] = a[...]
    x = full[...].astype(F32)
    scale = lax.rsqrt(jnp.mean(x * x, axis=-1, keepdims=True) + EPS)
    normed = (x * scale * gains[...].astype(F32)).astype(BF16)
    score = jnp.sum(
        normed.astype(F32) * blend_weight[...].astype(F32), axis=-1, keepdims=True
    )
    blend[...] = jnp.broadcast_to(jax.nn.sigmoid(score), blend.shape)
    loads[0].wait()
    pre_gate = dot(normed, gate_v[...])
    loads[1].wait()
    pre_up = dot(normed, up_v[...])
    hidden = (jax.nn.silu(pre_gate) * pre_up).astype(BF16)
    loads[2].wait()
    for m, p in enumerate((p0, p1, p2, p3)):
        p[...] = dot(hidden, down_v[:, cols_of(t ^ m, quarter)]).astype(BF16)


def enter_kernel(capacity, arrived, gains, w0, w1, w2, w3, keep, send, wide, rows, sums):
    t = lax.axis_index("tp")
    lanes = arrived.shape[1]
    quarter = rows.shape[1]
    wide[...] = arrived[...].astype(F32)
    gain = gains[:, cols_of(t, quarter)].astype(F32)
    for strided, near, cols in places(capacity, wide, quarter):
        x = wide[strided, :]
        sums[near, :] = x * x if cols.start == 0 else sums[near, :] + x * x
        rows[near, cols] = (x * gain[:, cols]).astype(BF16)
    squares = nt_dot(jnp.ones((8, lanes), F32), sums[...], HIGHEST)[0:1]
    count = rows.shape[0]
    keep[count:, :] = jnp.broadcast_to(
        jnp.concatenate([squares, jnp.zeros((1, keep.shape[1] - count), F32)], axis=1),
        (8, keep.shape[1]),
    )
    send[count:, :] = three_terms(squares, send.shape[1])
    x = rows[...]
    pair = w0.shape[1]
    keep[0:count, 0:pair] = dot(x, w0[0:quarter, :])
    send[0:count, 0:pair] = dot(x, w1[0:quarter, :]).astype(BF16)
    keep[0:count, pair:] = dot(x, w2[0:quarter, :])
    send[0:count, pair:] = dot(x, w3[0:quarter, :]).astype(BF16)


def relay_kernel(keep, came, onward):
    pair = onward.shape[1]
    count = keep.shape[0] - 8
    onward[0:count, :] = (keep[0:count, pair:] + came[0:count, pair:].astype(F32)).astype(BF16)
    squares = keep[count : count + 1, :] + sum_terms(came[count:, :])
    onward[count : count + 8, :] = three_terms(squares[:, 0:pair], pair)
    onward[count + 8 :, :] = three_terms(squares[:, pair:], pair)


def hidden_kernel(width, keep, came, last, hidden):
    count, units = hidden.shape
    pair = 2 * units
    total = (
        keep[0:count, 0:pair] + came[0:count, 0:pair].astype(F32) + last[0:count, :].astype(F32)
    )
    squares = keep[count : count + 1, :] + sum_terms(came[count:, :])
    squares = squares + jnp.concatenate(
        [sum_terms(last[count : count + 8, :]), sum_terms(last[count + 8 :, :])], axis=1
    )
    column = jnp.transpose(jnp.broadcast_to(squares[:, 0:count], (8, count)))[:, 0:1]
    scale = lax.rsqrt(column / width + EPS)
    hidden[...] = (jax.nn.silu(total[:, 0:units] * scale) * (total[:, units:] * scale)).astype(BF16)


def leave_kernel(capacity, h0, h1, h2, h3, w0, w1, w2, w3, out, wide, total):
    units = h0.shape[1]
    skip = w0.shape[0] - 2 * units
    size = w0.shape[1]
    for half in range(2):
        near = slice(skip + half * units, skip + (half + 1) * units)
        total[:, half * size : (half + 1) * size] = (
            dot(h0[...], w0[near, :]) + dot(h1[...], w1[near, :])
        ) + (dot(h2[...], w2[near, :]) + dot(h3[...], w3[near, :]))
    for strided, near, cols in places(capacity, wide, total.shape[1]):
        wide[strided, :] = total[near, cols]
    out[...] = wide[...].astype(BF16)


def final_kernel(
    capacity, returned, w, share0, share1, resid, blend, p0, p1, p2, p3, out, wide, rows
):
    count, quarter = resid.shape
    wide[...] = returned[...].astype(F32)
    for strided, near, cols in places(capacity, wide, quarter):
        rows[near, cols] = wide[strided, :].astype(BF16)
    picked = dot(w[...], rows[...])
    lanes = wide.shape[1]
    for c in range(quarter // lanes):
        cols = slice(c * lanes, (c + 1) * lanes)
        moe = share0[...] * picked[0:count, cols] + share1[...] * picked[count:, cols]
        dense = (p0[:, cols].astype(F32) + p1[:, cols].astype(F32)) + (
            p2[:, cols].astype(F32) + p3[:, cols].astype(F32)
        )
        out[:, cols] = (resid[:, cols].astype(F32) + moe + blend[...] * dense).astype(BF16)


def call(kernel, outs, scratch=(), limit=4, in_specs=None, out_specs=None):
    out_specs = out_specs or [VMEM] * len(outs)
    out_shape = [
        pltpu.VMEM(s, d) if spec is VMEM else jax.ShapeDtypeStruct(s, d)
        for (s, d), spec in zip(outs, out_specs)
    ]

    def run(*args):
        specs = in_specs or [VMEM] * len(args)
        spaces = {id(VMEM): pltpu.VMEM, id(HBM): pltpu.HBM}
        fixed = [
            pltpu.with_memory_space_constraint(a, spaces.get(id(spec), pl.ANY))
            for a, spec in zip(args, specs)
        ]
        return pl.pallas_call(
            kernel,
            out_shape=tuple(out_shape),
            in_specs=specs,
            out_specs=tuple(out_specs),
            scratch_shapes=list(scratch),
            compiler_params=pltpu.CompilerParams(vmem_limit_bytes=limit << 20),
        )(*fixed)

    return run


def per_device(
    tokens,
    norm_gain,
    in_weight,
    sequence_state_real,
    sequence_state_imaginary,
    eigen_decay_real,
    log_step,
    input_matrix_real,
    input_matrix_imaginary,
    output_matrix_real,
    output_matrix_imaginary,
    channel_skip_scale,
    out_weight,
    ffn_gain,
    routes,
    group_weight,
    expert_logit,
    expert_gate,
    expert_up,
    expert_down,
    dense_gate,
    dense_up,
    dense_down,
    blend_weight,
):
    rows, width = tokens.shape
    tp = lax.axis_size("tp")
    ep = lax.axis_size("ep")
    quarter = width // tp
    lanes = 128
    blocks = quarter // lanes
    capacity = max(2, 2 * rows * routes.shape[1] // (ep * expert_gate.shape[0]))
    slots = ep * capacity
    groups, entries, channels = input_matrix_real.shape
    hid = expert_gate.shape[2]
    gate = expert_gate.reshape(width, hid)
    up = expert_up.reshape(width, hid)
    down = expert_down.reshape(hid, width)
    piece = ((rows, quarter), BF16)

    def by_channel(matrix):
        return jnp.swapaxes(matrix, 1, 2).reshape(groups * channels, entries)

    states = ((rows, groups * entries), F32)
    state_inputs = (
        eigen_decay_real,
        channel_skip_scale,
        tokens,
        norm_gain,
        in_weight,
        by_channel(input_matrix_real),
        by_channel(input_matrix_imaginary),
        sequence_state_real,
        sequence_state_imaginary,
        output_matrix_real.reshape(groups * channels, entries),
        output_matrix_imaginary.reshape(groups * channels, entries),
        out_weight,
        log_step,
    )
    *mix, new_re, new_im = call(
        state_kernel,
        [piece] * 4 + [states] * 2,
        [pltpu.VMEM(x.shape, x.dtype) for x in state_inputs[:-1]]
        + [pltpu.SMEM(log_step.shape, F32)]
        + [pltpu.VMEM(states[0], F32)] * 2
        + [pltpu.SemaphoreType.DMA((15,))],
        20,
        [HBM] * 13,
        [VMEM] * 4 + [HBM] * 2,
    )(*state_inputs)
    mix = [mix[0]] + [exchanged(mix[m], m) for m in (1, 2, 3)]
    pieces = call(reshard_kernel, [((quarter + 2 * hid, 2 * hid), BF16)] * 4)(gate, up, down)
    piece2 = exchanged(pieces[2], 2)
    piece3 = exchanged(pieces[3], 3)
    piece1 = exchanged(pieces[1], 1)
    moved = [pieces[0], piece1, piece2, piece3]
    z, w, share0, share1 = call(
        functools.partial(route_kernel, ep),
        [((slots, lanes), BF16), ((2 * rows, slots), BF16)] + [((rows, lanes), F32)] * 2,
        [pltpu.VMEM((8, lanes), jnp.int32)],
    )(routes.T, group_weight.reshape(1, rows), expert_logit.T)
    wide = pltpu.VMEM((slots * blocks, lanes), F32)
    resid16, packed = call(
        functools.partial(pack_kernel, capacity),
        [piece, ((slots * blocks, lanes), BF16)],
        [wide],
        8,
        out_specs=[VMEM, FREE],
    )(tokens, *mix, z)
    across, beside = exchanged(resid16, 2), exchanged(resid16, 1)
    arrived = lax.all_to_all(
        packed.reshape(ep, capacity * blocks, lanes), "ep", 0, 0, tiled=True
    ).reshape(slots * blocks, lanes)
    near = [resid16, beside, across, exchanged(across, 1)]
    gains = ffn_gain.reshape(1, width)
    *dense, blend = call(
        dense_kernel,
        [piece] * 4 + [((rows, lanes), F32)],
        [pltpu.VMEM((rows, width), BF16)]
        + [pltpu.VMEM(x.shape, BF16) for x in (dense_gate, dense_up, dense_down)]
        + [pltpu.SemaphoreType.DMA((3,))],
        12,
        [VMEM] * 6 + [HBM] * 3,
    )(gains, *near, blend_weight.reshape(1, width), dense_gate, dense_up, dense_down)
    dense = [dense[0]] + [exchanged(dense[m], m) for m in (1, 2, 3)]
    keep, send = call(
        functools.partial(enter_kernel, capacity),
        [((slots + 8, 4 * hid), F32), ((slots + 8, 4 * hid), BF16)],
        [wide, pltpu.VMEM((slots, quarter), BF16), pltpu.VMEM((slots, lanes), F32)],
        8,
    )(arrived, gains, *moved)
    came = exchanged(send, 1)
    (onward,) = call(relay_kernel, [((slots + 16, 2 * hid), BF16)])(keep, came)
    last = exchanged(onward, 2)
    (hidden,) = call(
        functools.partial(hidden_kernel, float(width)), [((slots, hid), BF16)]
    )(keep, came, last)
    hidden = gathered(hidden)
    (sent,) = call(
        functools.partial(leave_kernel, capacity),
        [((slots * blocks, lanes), BF16)],
        [wide, pltpu.VMEM((slots, quarter), F32)],
        8,
        out_specs=[FREE],
    )(*hidden, *moved)
    returned = lax.all_to_all(
        sent.reshape(ep, capacity * blocks, lanes), "ep", 0, 0, tiled=True
    ).reshape(slots * blocks, lanes)
    (new_tokens,) = call(
        functools.partial(final_kernel, capacity),
        [piece],
        [wide, pltpu.VMEM((slots, quarter), BF16)],
        8,
        out_specs=[FREE],
    )(returned, w, share0, share1, resid16, blend, *dense)
    return (new_tokens, new_re, new_im)


def solution(mesh):
    in_specs = (
        P("ep", None),
        P(),
        P(None, "tp"),
        P("ep", "tp"),
        P("ep", "tp"),
        P("tp", None),
        P("tp"),
        P("tp", None, None),
        P("tp", None, None),
        P("tp", None, None),
        P("tp", None, None),
        P("tp", None),
        P("tp", None),
        P(),
        P("ep", None),
        P("ep"),
        P("ep", None),
        P("ep", None, "tp"),
        P("ep", None, "tp"),
        P("ep", "tp", None),
        P(None, "tp"),
        P(None, "tp"),
        P("tp", None),
        P(),
    )
    out_specs = (P("ep", "tp"), P("ep", "tp"), P("ep", "tp"))

    return jax.shard_map(
        per_device, mesh=mesh, in_specs=in_specs, out_specs=out_specs, check_vma=False
    )
```

```python
import functools
import math

import jax
import jax.numpy as jnp
from jax import lax
from jax.experimental import pallas as pl
from jax.experimental.pallas import tpu as pltpu
from jax.sharding import PartitionSpec as P


EPS = 1e-06
F32 = jnp.float32
BF16 = jnp.bfloat16
HIGHEST = lax.Precision.HIGHEST
VMEM = pl.BlockSpec(memory_space=pltpu.VMEM)
SMEM = pl.BlockSpec(memory_space=pltpu.SMEM)
ANY = pl.BlockSpec(memory_space=pl.ANY)
HBM = pl.BlockSpec(memory_space=pltpu.HBM)
FREE = pl.BlockSpec(memory_space=pltpu.VMEM)


def iota(shape, dim):
    return lax.broadcasted_iota(jnp.int32, shape, dim)


def nt_dot(a, b, precision=None):
    return lax.dot_general(
        a, b, (((1,), (1,)), ((), ())), precision=precision, preferred_element_type=F32
    )


def dot(a, b, precision=None):
    return jnp.dot(a, b, precision=precision, preferred_element_type=F32)


def cols_of(index, size):
    return pl.ds(pl.multiple_of(index * size, size), size)


def exchanged(value, mask):
    return lax.ppermute(value, "tp", [(i, i ^ mask) for i in range(4)])


def gathered(value):
    across = exchanged(value, 2)
    return [value, exchanged(value, 1), across, exchanged(across, 1)]


def spread_blocks(small, channels):
    rows, entries = small.shape
    groups = rows // channels
    width = groups * entries
    tiler = (iota((entries, width), 1) % entries == iota((entries, width), 0)).astype(BF16)
    tiled = dot(small.astype(BF16), tiler)
    mine = iota((rows, width), 0) // channels == iota((rows, width), 1) // entries
    return jnp.where(mine, tiled, 0.0).astype(BF16)


def row_of(small):
    groups, n = small.shape
    width = groups * n
    tiler = (iota((n, width), 1) % n == iota((n, width), 0)).astype(F32)
    tiled = dot(small, tiler, HIGHEST)
    mine = iota((groups, width), 0) == iota((groups, width), 1) // n
    return jnp.sum(jnp.where(mine, tiled, 0.0), axis=0, keepdims=True)


def state_kernel(*refs):
    inputs, (p0, p1, p2, p3, new_re, new_im), held = refs[0:13], refs[13:19], refs[19:32]
    fresh_re_v, fresh_im_v, blocks_v, sems = refs[32:]
    t = lax.axis_index("tp")
    loads = [
        pltpu.make_async_copy(a, b, sems.at[i]) for i, (a, b) in enumerate(zip(inputs, held))
    ]
    for load in loads:
        load.start()
    log_step, decay, skip, b_re, b_im, c_re, c_im, tokens_v, gain, in_v, re_v, im_v, out_v = held
    groups, entries = decay.shape
    channels = skip.shape[1]
    width = groups * entries
    of_group = iota((1, width), 1) // entries
    for load in loads[0:3]:
        load.wait()
    logs = jnp.zeros((1, width), F32)
    for g in range(groups):
        logs = jnp.where(of_group == g, log_step[g], logs)
    step = jnp.exp(logs)
    eigen = row_of(decay[...])
    direct = row_of(skip[...])
    freq = math.pi * (iota((1, width), 1) % entries).astype(F32)
    magnitude = jnp.exp(eigen * step)
    turned = freq * step
    lam_re = magnitude * jnp.cos(turned)
    lam_im = magnitude * jnp.sin(turned)
    denom = eigen * eigen + freq * freq
    fac_re = ((lam_re - 1.0) * eigen + lam_im * freq) / denom
    fac_im = (lam_im * eigen - (lam_re - 1.0) * freq) / denom
    for load in loads[3:7]:
        load.wait()
    for k, small in enumerate((b_re, b_im, c_re, c_im)):
        blocks_v[k] = spread_blocks(small[...], channels)
    loads[7].wait()
    loads[8].wait()
    x = tokens_v[...].astype(F32)
    scale = lax.rsqrt(jnp.mean(x * x, axis=-1, keepdims=True) + EPS)
    normed = (x * scale * gain[...].astype(F32).reshape(1, -1)).astype(BF16)
    loads[9].wait()
    drive = dot(normed, in_v[...]).astype(BF16)
    in_re = dot(drive, blocks_v[0])
    in_im = dot(drive, blocks_v[1])
    loads[10].wait()
    loads[11].wait()
    was_re, was_im = re_v[...], im_v[...]
    fresh_re = lam_re * was_re - lam_im * was_im + (fac_re * in_re - fac_im * in_im)
    fresh_im = lam_re * was_im + lam_im * was_re + (fac_re * in_im + fac_im * in_re)
    fresh_re_v[...] = fresh_re
    fresh_im_v[...] = fresh_im
    stores = [
        pltpu.make_async_copy(fresh_re_v, new_re, sems.at[13]),
        pltpu.make_async_copy(fresh_im_v, new_im, sems.at[14]),
    ]
    for store in stores:
        store.start()
    mixed = (
        nt_dot(fresh_re.astype(BF16), blocks_v[2])
        - nt_dot(fresh_im.astype(BF16), blocks_v[3])
        + direct * drive.astype(F32)
    )
    act = jax.nn.gelu(mixed).astype(BF16)
    loads[12].wait()
    for m, p in enumerate((p0, p1, p2, p3)):
        p[...] = dot(act, out_v[:, cols_of(t ^ m, p.shape[1])]).astype(BF16)
    for store in stores:
        store.wait()


def reshard_kernel(gate, up, down, *pieces):
    t = lax.axis_index("tp")
    hid = gate.shape[1]
    for m, (wide, deep) in enumerate(zip(pieces[:4], pieces[4:])):
        part = cols_of(t ^ m, wide.shape[0])
        wide[:, 0:hid] = gate[part, :]
        wide[:, hid:] = up[part, :]
        deep[...] = down[:, cols_of(t ^ m, deep.shape[1])]


def route_kernel(experts, routes, group_weight, logits, z, w, share0, share1, padded):
    rows = routes.shape[1]
    slots, lanes = z.shape
    padded[...] = jnp.full(padded.shape, -1, jnp.int32)
    padded[0:2, 0:rows] = routes[...]
    named = [padded[k : k + 1, :] for k in range(2)]
    hot = [(iota((experts, lanes), 0) == r).astype(F32) for r in named]
    earlier = (iota((lanes, lanes), 0) < iota((lanes, lanes), 1)).astype(BF16)
    before = dot((hot[0] + hot[1]).astype(BF16), earlier)
    place = [jnp.sum(before * h, axis=0, keepdims=True).astype(jnp.int32) for h in hot]
    slot = [jnp.where(r >= 0, p * experts + r, -1) for r, p in zip(named, place)]
    at = iota((slots, lanes), 0)
    z[...] = jnp.logical_or(at == slot[0], at == slot[1]).astype(F32).astype(BF16)
    eye = iota((lanes, lanes), 0) == iota((lanes, lanes), 1)
    at = iota((rows, slots), 1)
    for k in range(2):
        column = jnp.sum(jnp.where(eye, slot[k], 0), axis=1, keepdims=True)[0:rows]
        w[k * rows : (k + 1) * rows, :] = (at == column).astype(F32).astype(BF16)
    expo = jnp.exp(logits[...])
    share = group_weight[...] * expo / (expo[0:1] + expo[1:2])
    small_eye = iota((rows, rows), 0) == iota((rows, rows), 1)
    for k, out in enumerate((share0, share1)):
        column = jnp.sum(jnp.where(small_eye, share[k : k + 1], 0.0), axis=1, keepdims=True)
        out[...] = jnp.broadcast_to(column, out.shape)


def places(capacity, wide, quarter):
    blocks = quarter // wide.shape[1]
    peers = wide.shape[0] // (capacity * blocks)
    for s in range(capacity):
        for c in range(blocks):
            yield (
                pl.ds(c * capacity + s, peers, stride=capacity * blocks),
                slice(s * peers, (s + 1) * peers),
                slice(c * wide.shape[1], (c + 1) * wide.shape[1]),
            )


def three_terms(row, size):
    if row.shape[1] < size:
        row = jnp.concatenate([row, jnp.zeros((1, size - row.shape[1]), F32)], axis=1)
    high = row.astype(BF16).astype(F32)
    middle = (row - high).astype(BF16).astype(F32)
    low = row - high - middle
    at = iota((8, size), 0)
    block = jnp.where(at == 0, high, jnp.where(at == 1, middle, jnp.where(at == 2, low, 0.0)))
    return block.astype(BF16)


def sum_terms(block):
    return jnp.sum(block.astype(F32), axis=0, keepdims=True)


def pack_kernel(capacity, tokens, p0, p1, p2, p3, z, *refs):
    resid16, packed, wide = refs[-3:]
    t = lax.axis_index("tp")
    quarter = p0.shape[1]
    total = tokens[:, cols_of(t, quarter)].astype(F32) + (
        (p0[...].astype(F32) + p1[...].astype(F32)) + (p2[...].astype(F32) + p3[...].astype(F32))
    )
    short = total.astype(BF16)
    resid16[...] = short
    gap = jnp.zeros((z.shape[1] - short.shape[0], quarter), BF16)
    spread = dot(z[...], jnp.concatenate([short, gap], axis=0))
    for strided, near, cols in places(capacity, wide, quarter):
        wide[strided, :] = spread[near, cols]
    packed[...] = wide[...].astype(BF16)


def dense_kernel(
    gains, a0, a1, a2, a3, blend_weight, gate, up, down, p0, p1, p2, p3, blend,
    full, gate_v, up_v, down_v, sems,
):
    t = lax.axis_index("tp")
    loads = [
        pltpu.make_async_copy(a, b, sems.at[i])
        for i, (a, b) in enumerate(((gate, gate_v), (up, up_v), (down, down_v)))
    ]
    for load in loads:
        load.start()
    quarter = a0.shape[1]
    for m, a in enumerate((a0, a1, a2, a3)):
        full[:, cols_of(t ^ m, quarter)] = a[...]
    x = full[...].astype(F32)
    scale = lax.rsqrt(jnp.mean(x * x, axis=-1, keepdims=True) + EPS)
    normed = (x * scale * gains[...].astype(F32)).astype(BF16)
    score = jnp.sum(
        normed.astype(F32) * blend_weight[...].astype(F32), axis=-1, keepdims=True
    )
    blend[...] = jnp.broadcast_to(jax.nn.sigmoid(score), blend.shape)
    loads[0].wait()
    pre_gate = dot(normed, gate_v[...])
    loads[1].wait()
    pre_up = dot(normed, up_v[...])
    hidden = (jax.nn.silu(pre_gate) * pre_up).astype(BF16)
    loads[2].wait()
    for m, p in enumerate((p0, p1, p2, p3)):
        p[...] = dot(hidden, down_v[:, cols_of(t ^ m, quarter)]).astype(BF16)


def enter_kernel(capacity, arrived, gains, w0, w1, w2, w3, keep, send, wide, rows, sums):
    t = lax.axis_index("tp")
    lanes = arrived.shape[1]
    quarter = rows.shape[1]
    wide[...] = arrived[...].astype(F32)
    gain = gains[:, cols_of(t, quarter)].astype(F32)
    for strided, near, cols in places(capacity, wide, quarter):
        x = wide[strided, :]
        sums[near, :] = x * x if cols.start == 0 else sums[near, :] + x * x
        rows[near, cols] = (x * gain[:, cols]).astype(BF16)
    squares = nt_dot(jnp.ones((8, lanes), F32), sums[...], HIGHEST)[0:1]
    count = rows.shape[0]
    keep[count:, :] = jnp.broadcast_to(
        jnp.concatenate([squares, jnp.zeros((1, keep.shape[1] - count), F32)], axis=1),
        (8, keep.shape[1]),
    )
    send[count:, :] = three_terms(squares, send.shape[1])
    x = rows[...]
    pair = w0.shape[1]
    keep[0:count, 0:pair] = dot(x, w0[...])
    send[0:count, 0:pair] = dot(x, w1[...]).astype(BF16)
    keep[0:count, pair:] = dot(x, w2[...])
    send[0:count, pair:] = dot(x, w3[...]).astype(BF16)


def relay_kernel(keep, came, onward):
    pair = onward.shape[1]
    count = keep.shape[0] - 8
    onward[0:count, :] = (keep[0:count, pair:] + came[0:count, pair:].astype(F32)).astype(BF16)
    squares = keep[count : count + 1, :] + sum_terms(came[count:, :])
    onward[count : count + 8, :] = three_terms(squares[:, 0:pair], pair)
    onward[count + 8 :, :] = three_terms(squares[:, pair:], pair)


def hidden_kernel(width, keep, came, last, hidden):
    count, units = hidden.shape
    pair = 2 * units
    total = (
        keep[0:count, 0:pair] + came[0:count, 0:pair].astype(F32) + last[0:count, :].astype(F32)
    )
    squares = keep[count : count + 1, :] + sum_terms(came[count:, :])
    squares = squares + jnp.concatenate(
        [sum_terms(last[count : count + 8, :]), sum_terms(last[count + 8 :, :])], axis=1
    )
    column = jnp.transpose(jnp.broadcast_to(squares[:, 0:count], (8, count)))[:, 0:1]
    scale = lax.rsqrt(column / width + EPS)
    hidden[...] = (jax.nn.silu(total[:, 0:units] * scale) * (total[:, units:] * scale)).astype(BF16)


def leave_kernel(capacity, h0, h1, h2, h3, w0, w1, w2, w3, out, wide):
    total = (dot(h0[...], w0[...]) + dot(h1[...], w1[...])) + (
        dot(h2[...], w2[...]) + dot(h3[...], w3[...])
    )
    for strided, near, cols in places(capacity, wide, total.shape[1]):
        wide[strided, :] = total[near, cols]
    out[...] = wide[...].astype(BF16)


def final_kernel(
    capacity, returned, w, share0, share1, resid, blend, p0, p1, p2, p3, out, wide, rows
):
    count, quarter = resid.shape
    wide[...] = returned[...].astype(F32)
    for strided, near, cols in places(capacity, wide, quarter):
        rows[near, cols] = wide[strided, :].astype(BF16)
    picked = dot(w[...], rows[...])
    lanes = wide.shape[1]
    for c in range(quarter // lanes):
        cols = slice(c * lanes, (c + 1) * lanes)
        moe = share0[...] * picked[0:count, cols] + share1[...] * picked[count:, cols]
        dense = (p0[:, cols].astype(F32) + p1[:, cols].astype(F32)) + (
            p2[:, cols].astype(F32) + p3[:, cols].astype(F32)
        )
        out[:, cols] = (resid[:, cols].astype(F32) + moe + blend[...] * dense).astype(BF16)


def call(kernel, outs, scratch=(), limit=4, in_specs=None, out_specs=None):
    out_specs = out_specs or [VMEM] * len(outs)
    out_shape = [
        pltpu.VMEM(s, d) if spec is VMEM else jax.ShapeDtypeStruct(s, d)
        for (s, d), spec in zip(outs, out_specs)
    ]

    def run(*args):
        specs = in_specs or [VMEM] * len(args)
        spaces = {id(VMEM): pltpu.VMEM, id(HBM): pltpu.HBM}
        fixed = [
            pltpu.with_memory_space_constraint(a, spaces.get(id(spec), pl.ANY))
            for a, spec in zip(args, specs)
        ]
        return pl.pallas_call(
            kernel,
            out_shape=tuple(out_shape),
            in_specs=specs,
            out_specs=tuple(out_specs),
            scratch_shapes=list(scratch),
            compiler_params=pltpu.CompilerParams(vmem_limit_bytes=limit << 20),
        )(*fixed)

    return run


def per_device(
    tokens,
    norm_gain,
    in_weight,
    sequence_state_real,
    sequence_state_imaginary,
    eigen_decay_real,
    log_step,
    input_matrix_real,
    input_matrix_imaginary,
    output_matrix_real,
    output_matrix_imaginary,
    channel_skip_scale,
    out_weight,
    ffn_gain,
    routes,
    group_weight,
    expert_logit,
    expert_gate,
    expert_up,
    expert_down,
    dense_gate,
    dense_up,
    dense_down,
    blend_weight,
):
    rows, width = tokens.shape
    tp = lax.axis_size("tp")
    ep = lax.axis_size("ep")
    quarter = width // tp
    lanes = 128
    blocks = quarter // lanes
    capacity = max(2, 2 * rows * routes.shape[1] // (ep * expert_gate.shape[0]))
    slots = ep * capacity
    groups, entries, channels = input_matrix_real.shape
    hid = expert_gate.shape[2]
    gate = expert_gate.reshape(width, hid)
    up = expert_up.reshape(width, hid)
    down = expert_down.reshape(hid, width)
    piece = ((rows, quarter), BF16)

    def by_channel(matrix):
        return jnp.swapaxes(matrix, 1, 2).reshape(groups * channels, entries)

    states = ((rows, groups * entries), F32)
    state_inputs = (
        log_step,
        eigen_decay_real,
        channel_skip_scale,
        by_channel(input_matrix_real),
        by_channel(input_matrix_imaginary),
        output_matrix_real.reshape(groups * channels, entries),
        output_matrix_imaginary.reshape(groups * channels, entries),
        tokens,
        norm_gain,
        in_weight,
        sequence_state_real,
        sequence_state_imaginary,
        out_weight,
    )
    *mix, new_re, new_im = call(
        state_kernel,
        [piece] * 4 + [states] * 2,
        [pltpu.SMEM(log_step.shape, F32)]
        + [pltpu.VMEM(x.shape, x.dtype) for x in state_inputs[1:]]
        + [pltpu.VMEM(states[0], F32)] * 2
        + [pltpu.VMEM((4, groups * channels, groups * entries), BF16)]
        + [pltpu.SemaphoreType.DMA((15,))],
        20,
        [HBM] * 13,
        [VMEM] * 4 + [HBM] * 2,
    )(*state_inputs)
    mix = [mix[0]] + [exchanged(mix[m], m) for m in (1, 2, 3)]
    pieces = call(
        reshard_kernel, [((quarter, 2 * hid), BF16)] * 4 + [((hid, quarter), BF16)] * 4
    )(gate, up, down)
    wide2 = exchanged(pieces[2], 2)
    wide3 = exchanged(pieces[3], 3)
    moved = [pieces[0], exchanged(pieces[1], 1), wide2, wide3]
    downs = [pieces[4]] + [exchanged(pieces[4 + m], m) for m in (1, 2, 3)]
    z, w, share0, share1 = call(
        functools.partial(route_kernel, ep),
        [((slots, lanes), BF16), ((2 * rows, slots), BF16)] + [((rows, lanes), F32)] * 2,
        [pltpu.VMEM((8, lanes), jnp.int32)],
    )(routes.T, group_weight.reshape(1, rows), expert_logit.T)
    wide = pltpu.VMEM((slots * blocks, lanes), F32)
    resid16, packed = call(
        functools.partial(pack_kernel, capacity),
        [piece, ((slots * blocks, lanes), BF16)],
        [wide],
        8,
        out_specs=[VMEM, FREE],
    )(tokens, *mix, z)
    across = exchanged(resid16, 2)
    arrived = lax.all_to_all(
        packed.reshape(ep, capacity * blocks, lanes), "ep", 0, 0, tiled=True
    ).reshape(slots * blocks, lanes)
    near = [resid16, exchanged(resid16, 1), across, exchanged(across, 1)]
    gains = ffn_gain.reshape(1, width)
    *dense, blend = call(
        dense_kernel,
        [piece] * 4 + [((rows, lanes), F32)],
        [pltpu.VMEM((rows, width), BF16)]
        + [pltpu.VMEM(x.shape, BF16) for x in (dense_gate, dense_up, dense_down)]
        + [pltpu.SemaphoreType.DMA((3,))],
        12,
        [VMEM] * 6 + [HBM] * 3,
        [FREE] * 5,
    )(gains, *near, blend_weight.reshape(1, width), dense_gate, dense_up, dense_down)
    dense = [dense[0]] + [exchanged(dense[m], m) for m in (1, 2, 3)]
    keep, send = call(
        functools.partial(enter_kernel, capacity),
        [((slots + 8, 4 * hid), F32), ((slots + 8, 4 * hid), BF16)],
        [wide, pltpu.VMEM((slots, quarter), BF16), pltpu.VMEM((slots, lanes), F32)],
        8,
    )(arrived, gains, *moved)
    came = exchanged(send, 1)
    (onward,) = call(relay_kernel, [((slots + 16, 2 * hid), BF16)])(keep, came)
    last = exchanged(onward, 2)
    (hidden,) = call(
        functools.partial(hidden_kernel, float(width)), [((slots, hid), BF16)]
    )(keep, came, last)
    hidden = gathered(hidden)
    (sent,) = call(
        functools.partial(leave_kernel, capacity),
        [((slots * blocks, lanes), BF16)],
        [wide],
        8,
        out_specs=[FREE],
    )(*hidden, *downs)
    returned = lax.all_to_all(
        sent.reshape(ep, capacity * blocks, lanes), "ep", 0, 0, tiled=True
    ).reshape(slots * blocks, lanes)
    (new_tokens,) = call(
        functools.partial(final_kernel, capacity),
        [piece],
        [wide, pltpu.VMEM((slots, quarter), BF16)],
        8,
        out_specs=[FREE],
    )(returned, w, share0, share1, resid16, blend, *dense)
    return (new_tokens, new_re, new_im)


def solution(mesh):
    in_specs = (
        P("ep", None),
        P(),
        P(None, "tp"),
        P("ep", "tp"),
        P("ep", "tp"),
        P("tp", None),
        P("tp"),
        P("tp", None, None),
        P("tp", None, None),
        P("tp", None, None),
        P("tp", None, None),
        P("tp", None),
        P("tp", None),
        P(),
        P("ep", None),
        P("ep"),
        P("ep", None),
        P("ep", None, "tp"),
        P("ep", None, "tp"),
        P("ep", "tp", None),
        P(None, "tp"),
        P(None, "tp"),
        P("tp", None),
        P(),
    )
    out_specs = (P("ep", "tp"), P("ep", "tp"), P("ep", "tp"))

    return jax.shard_map(
        per_device, mesh=mesh, in_specs=in_specs, out_specs=out_specs, check_vma=False
    )
```

```python
import functools
import math

import jax
import jax.numpy as jnp
from jax import lax
from jax.experimental import pallas as pl
from jax.experimental.pallas import tpu as pltpu
from jax.sharding import PartitionSpec as P


EPS = 1e-06
F32 = jnp.float32
BF16 = jnp.bfloat16
HIGHEST = lax.Precision.HIGHEST
VMEM = pl.BlockSpec(memory_space=pltpu.VMEM)
SMEM = pl.BlockSpec(memory_space=pltpu.SMEM)
ANY = pl.BlockSpec(memory_space=pl.ANY)
HBM = pl.BlockSpec(memory_space=pltpu.HBM)
FREE = pl.BlockSpec(memory_space=pltpu.VMEM)


def iota(shape, dim):
    return lax.broadcasted_iota(jnp.int32, shape, dim)


def nt_dot(a, b, precision=None):
    return lax.dot_general(
        a, b, (((1,), (1,)), ((), ())), precision=precision, preferred_element_type=F32
    )


def dot(a, b, precision=None):
    return jnp.dot(a, b, precision=precision, preferred_element_type=F32)


def cols_of(index, size):
    return pl.ds(pl.multiple_of(index * size, size), size)


def exchanged(value, mask):
    return lax.ppermute(value, "tp", [(i, i ^ mask) for i in range(4)])


def gathered(value):
    across = exchanged(value, 2)
    return [value, exchanged(value, 1), across, exchanged(across, 1)]


def spread_blocks(small, channels):
    rows, entries = small.shape
    groups = rows // channels
    width = groups * entries
    tiler = (iota((entries, width), 1) % entries == iota((entries, width), 0)).astype(BF16)
    tiled = dot(small.astype(BF16), tiler)
    mine = iota((rows, width), 0) // channels == iota((rows, width), 1) // entries
    return jnp.where(mine, tiled, 0.0).astype(BF16)


def row_of(small):
    groups, n = small.shape
    width = groups * n
    tiler = (iota((n, width), 1) % n == iota((n, width), 0)).astype(F32)
    tiled = dot(small, tiler, HIGHEST)
    mine = iota((groups, width), 0) == iota((groups, width), 1) // n
    return jnp.sum(jnp.where(mine, tiled, 0.0), axis=0, keepdims=True)


def state_kernel(*refs):
    inputs, (own, beside, new_re, new_im), held = refs[0:13], refs[13:17], refs[17:30]
    fresh_re_v, fresh_im_v, blocks_v, sems = refs[30:]
    t = lax.axis_index("tp")
    loads = [
        pltpu.make_async_copy(a, b, sems.at[i]) for i, (a, b) in enumerate(zip(inputs, held))
    ]
    for load in loads:
        load.start()
    log_step, decay, skip, b_re, b_im, c_re, c_im, tokens_v, gain, in_v, re_v, im_v, out_v = held
    groups, entries = decay.shape
    channels = skip.shape[1]
    width = groups * entries
    of_group = iota((1, width), 1) // entries
    for load in loads[0:3]:
        load.wait()
    logs = jnp.zeros((1, width), F32)
    for g in range(groups):
        logs = jnp.where(of_group == g, log_step[g], logs)
    step = jnp.exp(logs)
    eigen = row_of(decay[...])
    direct = row_of(skip[...])
    freq = math.pi * (iota((1, width), 1) % entries).astype(F32)
    magnitude = jnp.exp(eigen * step)
    turned = freq * step
    lam_re = magnitude * jnp.cos(turned)
    lam_im = magnitude * jnp.sin(turned)
    denom = eigen * eigen + freq * freq
    fac_re = ((lam_re - 1.0) * eigen + lam_im * freq) / denom
    fac_im = (lam_im * eigen - (lam_re - 1.0) * freq) / denom
    for load in loads[3:7]:
        load.wait()
    for k, small in enumerate((b_re, b_im, c_re, c_im)):
        blocks_v[k] = spread_blocks(small[...], channels)
    loads[7].wait()
    loads[8].wait()
    x = tokens_v[...].astype(F32)
    scale = lax.rsqrt(jnp.mean(x * x, axis=-1, keepdims=True) + EPS)
    normed = (x * scale * gain[...].astype(F32).reshape(1, -1)).astype(BF16)
    loads[9].wait()
    drive = dot(normed, in_v[...]).astype(BF16)
    in_re = dot(drive, blocks_v[0])
    in_im = dot(drive, blocks_v[1])
    loads[10].wait()
    loads[11].wait()
    was_re, was_im = re_v[...], im_v[...]
    fresh_re = lam_re * was_re - lam_im * was_im + (fac_re * in_re - fac_im * in_im)
    fresh_im = lam_re * was_im + lam_im * was_re + (fac_re * in_im + fac_im * in_re)
    fresh_re_v[...] = fresh_re
    fresh_im_v[...] = fresh_im
    stores = [
        pltpu.make_async_copy(fresh_re_v, new_re, sems.at[13]),
        pltpu.make_async_copy(fresh_im_v, new_im, sems.at[14]),
    ]
    for store in stores:
        store.start()
    mixed = (
        nt_dot(fresh_re.astype(BF16), blocks_v[2])
        - nt_dot(fresh_im.astype(BF16), blocks_v[3])
        + direct * drive.astype(F32)
    )
    act = jax.nn.gelu(mixed).astype(BF16)
    loads[12].wait()
    quarter = own.shape[1] // 2
    for m, pair in ((1, beside), (3, beside), (0, own), (2, own)):
        near = pl.ds((m // 2) * quarter, quarter)
        pair[:, near] = dot(act, out_v[:, cols_of(t ^ m, quarter)]).astype(BF16)
    for store in stores:
        store.wait()


def half_kernel(own, came, onward):
    quarter = onward.shape[1]
    onward[...] = (own[:, quarter:].astype(F32) + came[:, quarter:].astype(F32)).astype(BF16)


def reshard_kernel(gate, up, down, *refs):
    pieces, sems = refs[:8], refs[8]
    t = lax.axis_index("tp")
    hid = gate.shape[1]
    copies = []
    for m in (3, 2, 1, 0):
        wide, deep = pieces[m], pieces[4 + m]
        part = cols_of(t ^ m, wide.shape[0])
        for source, target in (
            (gate.at[part, :], wide.at[:, pl.ds(0, hid)]),
            (up.at[part, :], wide.at[:, pl.ds(hid, hid)]),
            (down.at[:, cols_of(t ^ m, deep.shape[1])], deep),
        ):
            copies.append(pltpu.make_async_copy(source, target, sems.at[len(copies)]))
    for copy in copies:
        copy.start()
    for copy in copies:
        copy.wait()


def route_kernel(experts, routes, group_weight, logits, z, w, share0, share1, padded):
    rows = routes.shape[1]
    slots, lanes = z.shape
    padded[...] = jnp.full(padded.shape, -1, jnp.int32)
    padded[0:2, 0:rows] = routes[...]
    named = [padded[k : k + 1, :] for k in range(2)]
    hot = [(iota((experts, lanes), 0) == r).astype(F32) for r in named]
    earlier = (iota((lanes, lanes), 0) < iota((lanes, lanes), 1)).astype(BF16)
    before = dot((hot[0] + hot[1]).astype(BF16), earlier)
    place = [jnp.sum(before * h, axis=0, keepdims=True).astype(jnp.int32) for h in hot]
    slot = [jnp.where(r >= 0, p * experts + r, -1) for r, p in zip(named, place)]
    at = iota((slots, lanes), 0)
    z[...] = jnp.logical_or(at == slot[0], at == slot[1]).astype(F32).astype(BF16)
    eye = iota((lanes, lanes), 0) == iota((lanes, lanes), 1)
    at = iota((rows, slots), 1)
    for k in range(2):
        column = jnp.sum(jnp.where(eye, slot[k], 0), axis=1, keepdims=True)[0:rows]
        w[k * rows : (k + 1) * rows, :] = (at == column).astype(F32).astype(BF16)
    expo = jnp.exp(logits[...])
    share = group_weight[...] * expo / (expo[0:1] + expo[1:2])
    small_eye = iota((rows, rows), 0) == iota((rows, rows), 1)
    for k, out in enumerate((share0, share1)):
        column = jnp.sum(jnp.where(small_eye, share[k : k + 1], 0.0), axis=1, keepdims=True)
        out[...] = jnp.broadcast_to(column, out.shape)


def places(capacity, wide, quarter):
    blocks = quarter // wide.shape[1]
    peers = wide.shape[0] // (capacity * blocks)
    for s in range(capacity):
        for c in range(blocks):
            yield (
                pl.ds(c * capacity + s, peers, stride=capacity * blocks),
                slice(s * peers, (s + 1) * peers),
                slice(c * wide.shape[1], (c + 1) * wide.shape[1]),
            )


def three_terms(row, size):
    if row.shape[1] < size:
        row = jnp.concatenate([row, jnp.zeros((1, size - row.shape[1]), F32)], axis=1)
    high = row.astype(BF16).astype(F32)
    middle = (row - high).astype(BF16).astype(F32)
    low = row - high - middle
    at = iota((8, size), 0)
    block = jnp.where(at == 0, high, jnp.where(at == 1, middle, jnp.where(at == 2, low, 0.0)))
    return block.astype(BF16)


def sum_terms(block):
    return jnp.sum(block.astype(F32), axis=0, keepdims=True)


def pack_kernel(capacity, tokens, own, came, last, z, resid16, packed, wide):
    t = lax.axis_index("tp")
    quarter = last.shape[1]
    total = tokens[:, cols_of(t, quarter)].astype(F32) + (
        (own[:, 0:quarter].astype(F32) + came[:, 0:quarter].astype(F32)) + last[...].astype(F32)
    )
    short = total.astype(BF16)
    resid16[...] = short
    gap = jnp.zeros((z.shape[1] - short.shape[0], quarter), BF16)
    spread = dot(z[...], jnp.concatenate([short, gap], axis=0))
    for strided, near, cols in places(capacity, wide, quarter):
        wide[strided, :] = spread[near, cols]
    packed[...] = wide[...].astype(BF16)


def dense_kernel(
    gains, a0, a1, a2, a3, blend_weight, gate, up, down, p0, p1, p2, p3, blend,
    full, gate_v, up_v, down_v, sems,
):
    t = lax.axis_index("tp")
    loads = [
        pltpu.make_async_copy(a, b, sems.at[i])
        for i, (a, b) in enumerate(((gate, gate_v), (up, up_v), (down, down_v)))
    ]
    for load in loads:
        load.start()
    quarter = a0.shape[1]
    for m, a in enumerate((a0, a1, a2, a3)):
        full[:, cols_of(t ^ m, quarter)] = a[...]
    x = full[...].astype(F32)
    scale = lax.rsqrt(jnp.mean(x * x, axis=-1, keepdims=True) + EPS)
    normed = (x * scale * gains[...].astype(F32)).astype(BF16)
    score = jnp.sum(
        normed.astype(F32) * blend_weight[...].astype(F32), axis=-1, keepdims=True
    )
    blend[...] = jnp.broadcast_to(jax.nn.sigmoid(score), blend.shape)
    loads[0].wait()
    pre_gate = dot(normed, gate_v[...])
    loads[1].wait()
    pre_up = dot(normed, up_v[...])
    hidden = (jax.nn.silu(pre_gate) * pre_up).astype(BF16)
    loads[2].wait()
    for m, p in enumerate((p0, p1, p2, p3)):
        p[...] = dot(hidden, down_v[:, cols_of(t ^ m, quarter)]).astype(BF16)


def enter_kernel(capacity, arrived, gains, w0, w1, w2, w3, keep, send, wide, rows, sums):
    t = lax.axis_index("tp")
    lanes = arrived.shape[1]
    quarter = rows.shape[1]
    wide[...] = arrived[...].astype(F32)
    gain = gains[:, cols_of(t, quarter)].astype(F32)
    for strided, near, cols in places(capacity, wide, quarter):
        x = wide[strided, :]
        sums[near, :] = x * x if cols.start == 0 else sums[near, :] + x * x
        rows[near, cols] = (x * gain[:, cols]).astype(BF16)
    squares = nt_dot(jnp.ones((8, lanes), F32), sums[...], HIGHEST)[0:1]
    count = rows.shape[0]
    keep[count:, :] = jnp.broadcast_to(
        jnp.concatenate([squares, jnp.zeros((1, keep.shape[1] - count), F32)], axis=1),
        (8, keep.shape[1]),
    )
    send[count:, :] = three_terms(squares, send.shape[1])
    x = rows[...]
    pair = w0.shape[1]
    keep[0:count, 0:pair] = dot(x, w0[...])
    send[0:count, 0:pair] = dot(x, w1[...]).astype(BF16)
    keep[0:count, pair:] = dot(x, w2[...])
    send[0:count, pair:] = dot(x, w3[...]).astype(BF16)


def relay_kernel(keep, came, onward):
    pair = onward.shape[1]
    count = keep.shape[0] - 8
    onward[0:count, :] = (keep[0:count, pair:] + came[0:count, pair:].astype(F32)).astype(BF16)
    squares = keep[count : count + 1, :] + sum_terms(came[count:, :])
    onward[count : count + 8, :] = three_terms(squares[:, 0:pair], pair)
    onward[count + 8 :, :] = three_terms(squares[:, pair:], pair)


def hidden_kernel(width, keep, came, last, hidden):
    count, units = hidden.shape
    pair = 2 * units
    total = (
        keep[0:count, 0:pair] + came[0:count, 0:pair].astype(F32) + last[0:count, :].astype(F32)
    )
    squares = keep[count : count + 1, :] + sum_terms(came[count:, :])
    squares = squares + jnp.concatenate(
        [sum_terms(last[count : count + 8, :]), sum_terms(last[count + 8 :, :])], axis=1
    )
    column = jnp.transpose(jnp.broadcast_to(squares[:, 0:count], (8, count)))[:, 0:1]
    scale = lax.rsqrt(column / width + EPS)
    hidden[...] = (jax.nn.silu(total[:, 0:units] * scale) * (total[:, units:] * scale)).astype(BF16)


def leave_kernel(capacity, h0, h1, h2, h3, w0, w1, w2, w3, out, wide):
    total = (dot(h0[...], w0[...]) + dot(h1[...], w1[...])) + (
        dot(h2[...], w2[...]) + dot(h3[...], w3[...])
    )
    for strided, near, cols in places(capacity, wide, total.shape[1]):
        wide[strided, :] = total[near, cols]
    out[...] = wide[...].astype(BF16)


def final_kernel(
    capacity, returned, w, share0, share1, resid, blend, p0, p1, p2, p3, out, wide, rows
):
    count, quarter = resid.shape
    wide[...] = returned[...].astype(F32)
    for strided, near, cols in places(capacity, wide, quarter):
        rows[near, cols] = wide[strided, :].astype(BF16)
    picked = dot(w[...], rows[...])
    lanes = wide.shape[1]
    for c in range(quarter // lanes):
        cols = slice(c * lanes, (c + 1) * lanes)
        moe = share0[...] * picked[0:count, cols] + share1[...] * picked[count:, cols]
        dense = (p0[:, cols].astype(F32) + p1[:, cols].astype(F32)) + (
            p2[:, cols].astype(F32) + p3[:, cols].astype(F32)
        )
        out[:, cols] = (resid[:, cols].astype(F32) + moe + blend[...] * dense).astype(BF16)


def call(kernel, outs, scratch=(), limit=4, in_specs=None, out_specs=None):
    out_specs = out_specs or [VMEM] * len(outs)
    out_shape = [
        pltpu.VMEM(s, d) if spec is VMEM else jax.ShapeDtypeStruct(s, d)
        for (s, d), spec in zip(outs, out_specs)
    ]

    def run(*args):
        specs = in_specs or [VMEM] * len(args)
        spaces = {id(VMEM): pltpu.VMEM, id(HBM): pltpu.HBM}
        fixed = [
            pltpu.with_memory_space_constraint(a, spaces.get(id(spec), pl.ANY))
            for a, spec in zip(args, specs)
        ]
        return pl.pallas_call(
            kernel,
            out_shape=tuple(out_shape),
            in_specs=specs,
            out_specs=tuple(out_specs),
            scratch_shapes=list(scratch),
            compiler_params=pltpu.CompilerParams(vmem_limit_bytes=limit << 20),
        )(*fixed)

    return run


def per_device(
    tokens,
    norm_gain,
    in_weight,
    sequence_state_real,
    sequence_state_imaginary,
    eigen_decay_real,
    log_step,
    input_matrix_real,
    input_matrix_imaginary,
    output_matrix_real,
    output_matrix_imaginary,
    channel_skip_scale,
    out_weight,
    ffn_gain,
    routes,
    group_weight,
    expert_logit,
    expert_gate,
    expert_up,
    expert_down,
    dense_gate,
    dense_up,
    dense_down,
    blend_weight,
):
    rows, width = tokens.shape
    tp = lax.axis_size("tp")
    ep = lax.axis_size("ep")
    quarter = width // tp
    lanes = 128
    blocks = quarter // lanes
    capacity = max(2, 2 * rows * routes.shape[1] // (ep * expert_gate.shape[0]))
    slots = ep * capacity
    groups, entries, channels = input_matrix_real.shape
    hid = expert_gate.shape[2]
    gate = expert_gate.reshape(width, hid)
    up = expert_up.reshape(width, hid)
    down = expert_down.reshape(hid, width)
    piece = ((rows, quarter), BF16)

    def by_channel(matrix):
        return jnp.swapaxes(matrix, 1, 2).reshape(groups * channels, entries)

    states = ((rows, groups * entries), F32)
    state_inputs = (
        log_step,
        eigen_decay_real,
        channel_skip_scale,
        by_channel(input_matrix_real),
        by_channel(input_matrix_imaginary),
        output_matrix_real.reshape(groups * channels, entries),
        output_matrix_imaginary.reshape(groups * channels, entries),
        tokens,
        norm_gain,
        in_weight,
        sequence_state_real,
        sequence_state_imaginary,
        out_weight,
    )
    own, beside, new_re, new_im = call(
        state_kernel,
        [((rows, 2 * quarter), BF16)] * 2 + [states] * 2,
        [pltpu.SMEM(log_step.shape, F32)]
        + [pltpu.VMEM(x.shape, x.dtype) for x in state_inputs[1:]]
        + [pltpu.VMEM(states[0], F32)] * 2
        + [pltpu.VMEM((4, groups * channels, groups * entries), BF16)]
        + [pltpu.SemaphoreType.DMA((15,))],
        20,
        [HBM] * 13,
        [VMEM] * 2 + [HBM] * 2,
    )(*state_inputs)
    came_mix = exchanged(beside, 1)
    (onward,) = call(half_kernel, [piece])(own, came_mix)
    last_mix = exchanged(onward, 2)
    reshard = call(
        reshard_kernel,
        [((quarter, 2 * hid), BF16)] * 4 + [((hid, quarter), BF16)] * 4,
        [pltpu.SemaphoreType.DMA((12,))],
        in_specs=[HBM] * 3,
    )
    pieces = reshard(gate, up, down)
    wide2 = exchanged(pieces[2], 2)
    wide3 = exchanged(pieces[3], 3)
    wide1 = exchanged(pieces[1], 1)
    moved = [pieces[0], wide1, wide2, wide3]
    downs = [pieces[4]] + [exchanged(pieces[4 + m], m) for m in (1, 2, 3)]
    z, w, share0, share1 = call(
        functools.partial(route_kernel, ep),
        [((slots, lanes), BF16), ((2 * rows, slots), BF16)] + [((rows, lanes), F32)] * 2,
        [pltpu.VMEM((8, lanes), jnp.int32)],
    )(routes.T, group_weight.reshape(1, rows), expert_logit.T)
    wide = pltpu.VMEM((slots * blocks, lanes), F32)
    resid16, packed = call(
        functools.partial(pack_kernel, capacity),
        [piece, ((slots * blocks, lanes), BF16)],
        [wide],
        8,
        out_specs=[VMEM, FREE],
    )(tokens, own, came_mix, last_mix, z)
    across = exchanged(resid16, 2)
    arrived = lax.all_to_all(
        packed.reshape(ep, capacity * blocks, lanes), "ep", 0, 0, tiled=True
    ).reshape(slots * blocks, lanes)
    near = [resid16, exchanged(resid16, 1), across, exchanged(across, 1)]
    gains = ffn_gain.reshape(1, width)
    *dense, blend = call(
        dense_kernel,
        [piece] * 4 + [((rows, lanes), F32)],
        [pltpu.VMEM((rows, width), BF16)]
        + [pltpu.VMEM(x.shape, BF16) for x in (dense_gate, dense_up, dense_down)]
        + [pltpu.SemaphoreType.DMA((3,))],
        12,
        [VMEM] * 6 + [HBM] * 3,
        [FREE] * 5,
    )(gains, *near, blend_weight.reshape(1, width), dense_gate, dense_up, dense_down)
    dense = [dense[0]] + [exchanged(dense[m], m) for m in (1, 2, 3)]
    keep, send = call(
        functools.partial(enter_kernel, capacity),
        [((slots + 8, 4 * hid), F32), ((slots + 8, 4 * hid), BF16)],
        [wide, pltpu.VMEM((slots, quarter), BF16), pltpu.VMEM((slots, lanes), F32)],
        8,
    )(arrived, gains, *moved)
    came = exchanged(send, 1)
    (onward,) = call(relay_kernel, [((slots + 16, 2 * hid), BF16)])(keep, came)
    last = exchanged(onward, 2)
    (hidden,) = call(
        functools.partial(hidden_kernel, float(width)), [((slots, hid), BF16)]
    )(keep, came, last)
    hidden = gathered(hidden)
    (sent,) = call(
        functools.partial(leave_kernel, capacity),
        [((slots * blocks, lanes), BF16)],
        [wide],
        8,
        out_specs=[FREE],
    )(*hidden, *downs)
    returned = lax.all_to_all(
        sent.reshape(ep, capacity * blocks, lanes), "ep", 0, 0, tiled=True
    ).reshape(slots * blocks, lanes)
    (new_tokens,) = call(
        functools.partial(final_kernel, capacity),
        [piece],
        [wide, pltpu.VMEM((slots, quarter), BF16)],
        8,
        out_specs=[FREE],
    )(returned, w, share0, share1, resid16, blend, *dense)
    return (new_tokens, new_re, new_im)


def solution(mesh):
    in_specs = (
        P("ep", None),
        P(),
        P(None, "tp"),
        P("ep", "tp"),
        P("ep", "tp"),
        P("tp", None),
        P("tp"),
        P("tp", None, None),
        P("tp", None, None),
        P("tp", None, None),
        P("tp", None, None),
        P("tp", None),
        P("tp", None),
        P(),
        P("ep", None),
        P("ep"),
        P("ep", None),
        P("ep", None, "tp"),
        P("ep", None, "tp"),
        P("ep", "tp", None),
        P(None, "tp"),
        P(None, "tp"),
        P("tp", None),
        P(),
    )
    out_specs = (P("ep", "tp"), P("ep", "tp"), P("ep", "tp"))

    return jax.shard_map(
        per_device, mesh=mesh, in_specs=in_specs, out_specs=out_specs, check_vma=False
    )
```

```python
import functools
import math

import jax
import jax.numpy as jnp
from jax import lax
from jax.experimental import pallas as pl
from jax.experimental.pallas import tpu as pltpu
from jax.sharding import PartitionSpec as P


EPS = 1e-06
F32 = jnp.float32
BF16 = jnp.bfloat16
HIGHEST = lax.Precision.HIGHEST
VMEM = pl.BlockSpec(memory_space=pltpu.VMEM)
SMEM = pl.BlockSpec(memory_space=pltpu.SMEM)
ANY = pl.BlockSpec(memory_space=pl.ANY)
HBM = pl.BlockSpec(memory_space=pltpu.HBM)
FREE = pl.BlockSpec(memory_space=pltpu.VMEM)


def iota(shape, dim):
    return lax.broadcasted_iota(jnp.int32, shape, dim)


def nt_dot(a, b, precision=None):
    return lax.dot_general(
        a, b, (((1,), (1,)), ((), ())), precision=precision, preferred_element_type=F32
    )


def dot(a, b, precision=None):
    return jnp.dot(a, b, precision=precision, preferred_element_type=F32)


def cols_of(index, size):
    return pl.ds(pl.multiple_of(index * size, size), size)


def exchanged(value, mask):
    return lax.ppermute(value, "tp", [(i, i ^ mask) for i in range(4)])


def gathered(value):
    across = exchanged(value, 2)
    return [value, exchanged(value, 1), across, exchanged(across, 1)]


def spread_blocks(small, channels):
    rows, entries = small.shape
    groups = rows // channels
    width = groups * entries
    tiler = (iota((entries, width), 1) % entries == iota((entries, width), 0)).astype(BF16)
    tiled = dot(small.astype(BF16), tiler)
    mine = iota((rows, width), 0) // channels == iota((rows, width), 1) // entries
    return jnp.where(mine, tiled, 0.0).astype(BF16)


def row_of(small):
    groups, n = small.shape
    width = groups * n
    tiler = (iota((n, width), 1) % n == iota((n, width), 0)).astype(F32)
    tiled = dot(small, tiler, HIGHEST)
    mine = iota((groups, width), 0) == iota((groups, width), 1) // n
    return jnp.sum(jnp.where(mine, tiled, 0.0), axis=0, keepdims=True)


def state_kernel(*refs):
    inputs, (own, beside, new_re, new_im), held = refs[0:13], refs[13:17], refs[17:30]
    fresh_re_v, fresh_im_v, blocks_v, sems = refs[30:]
    t = lax.axis_index("tp")
    loads = [
        pltpu.make_async_copy(a, b, sems.at[i]) for i, (a, b) in enumerate(zip(inputs, held))
    ]
    for load in loads:
        load.start()
    log_step, decay, skip, b_re, b_im, c_re, c_im, tokens_v, gain, in_v, re_v, im_v, out_v = held
    groups, entries = decay.shape
    channels = skip.shape[1]
    width = groups * entries
    of_group = iota((1, width), 1) // entries
    for load in loads[0:3]:
        load.wait()
    logs = jnp.zeros((1, width), F32)
    for g in range(groups):
        logs = jnp.where(of_group == g, log_step[g], logs)
    step = jnp.exp(logs)
    eigen = row_of(decay[...])
    direct = row_of(skip[...])
    freq = math.pi * (iota((1, width), 1) % entries).astype(F32)
    magnitude = jnp.exp(eigen * step)
    turned = freq * step
    lam_re = magnitude * jnp.cos(turned)
    lam_im = magnitude * jnp.sin(turned)
    denom = eigen * eigen + freq * freq
    fac_re = ((lam_re - 1.0) * eigen + lam_im * freq) / denom
    fac_im = (lam_im * eigen - (lam_re - 1.0) * freq) / denom
    for load in loads[3:7]:
        load.wait()
    for k, small in enumerate((b_re, b_im, c_re, c_im)):
        blocks_v[k] = spread_blocks(small[...], channels)
    loads[7].wait()
    loads[8].wait()
    x = tokens_v[...].astype(F32)
    scale = lax.rsqrt(jnp.mean(x * x, axis=-1, keepdims=True) + EPS)
    normed = (x * scale * gain[...].astype(F32).reshape(1, -1)).astype(BF16)
    loads[9].wait()
    drive = dot(normed, in_v[...]).astype(BF16)
    in_re = dot(drive, blocks_v[0])
    in_im = dot(drive, blocks_v[1])
    loads[10].wait()
    loads[11].wait()
    was_re, was_im = re_v[...], im_v[...]
    fresh_re = lam_re * was_re - lam_im * was_im + (fac_re * in_re - fac_im * in_im)
    fresh_im = lam_re * was_im + lam_im * was_re + (fac_re * in_im + fac_im * in_re)
    fresh_re_v[...] = fresh_re
    fresh_im_v[...] = fresh_im
    stores = [
        pltpu.make_async_copy(fresh_re_v, new_re, sems.at[13]),
        pltpu.make_async_copy(fresh_im_v, new_im, sems.at[14]),
    ]
    for store in stores:
        store.start()
    mixed = (
        nt_dot(fresh_re.astype(BF16), blocks_v[2])
        - nt_dot(fresh_im.astype(BF16), blocks_v[3])
        + direct * drive.astype(F32)
    )
    act = jax.nn.gelu(mixed).astype(BF16)
    loads[12].wait()
    quarter = own.shape[1] // 2
    for m, pair in ((1, beside), (3, beside), (0, own), (2, own)):
        near = pl.ds((m // 2) * quarter, quarter)
        pair[:, near] = dot(act, out_v[:, cols_of(t ^ m, quarter)]).astype(BF16)
    for store in stores:
        store.wait()


def half_kernel(own, came, onward):
    quarter = onward.shape[1]
    onward[...] = (own[:, quarter:].astype(F32) + came[:, quarter:].astype(F32)).astype(BF16)


def reshard_kernel(gate, up, down, *pieces):
    t = lax.axis_index("tp")
    hid = gate.shape[1]
    for m, (wide, deep) in enumerate(zip(pieces[:4], pieces[4:])):
        part = cols_of(t ^ m, wide.shape[0])
        wide[:, 0:hid] = gate[part, :]
        wide[:, hid:] = up[part, :]
        deep[...] = down[:, cols_of(t ^ m, deep.shape[1])]


def route_kernel(experts, routes, group_weight, logits, z, w, share0, share1, padded):
    rows = routes.shape[1]
    slots, lanes = z.shape
    padded[...] = jnp.full(padded.shape, -1, jnp.int32)
    padded[0:2, 0:rows] = routes[...]
    named = [padded[k : k + 1, :] for k in range(2)]
    hot = [(iota((experts, lanes), 0) == r).astype(F32) for r in named]
    earlier = (iota((lanes, lanes), 0) < iota((lanes, lanes), 1)).astype(BF16)
    before = dot((hot[0] + hot[1]).astype(BF16), earlier)
    place = [jnp.sum(before * h, axis=0, keepdims=True).astype(jnp.int32) for h in hot]
    slot = [jnp.where(r >= 0, p * experts + r, -1) for r, p in zip(named, place)]
    at = iota((slots, lanes), 0)
    z[...] = jnp.logical_or(at == slot[0], at == slot[1]).astype(F32).astype(BF16)
    eye = iota((lanes, lanes), 0) == iota((lanes, lanes), 1)
    at = iota((rows, slots), 1)
    for k in range(2):
        column = jnp.sum(jnp.where(eye, slot[k], 0), axis=1, keepdims=True)[0:rows]
        w[k * rows : (k + 1) * rows, :] = (at == column).astype(F32).astype(BF16)
    expo = jnp.exp(logits[...])
    share = group_weight[...] * expo / (expo[0:1] + expo[1:2])
    small_eye = iota((rows, rows), 0) == iota((rows, rows), 1)
    for k, out in enumerate((share0, share1)):
        column = jnp.sum(jnp.where(small_eye, share[k : k + 1], 0.0), axis=1, keepdims=True)
        out[...] = jnp.broadcast_to(column, out.shape)


def places(capacity, wide, quarter):
    blocks = quarter // wide.shape[1]
    peers = wide.shape[0] // (capacity * blocks)
    for s in range(capacity):
        for c in range(blocks):
            yield (
                pl.ds(c * capacity + s, peers, stride=capacity * blocks),
                slice(s * peers, (s + 1) * peers),
                slice(c * wide.shape[1], (c + 1) * wide.shape[1]),
            )


def three_terms(row, size):
    if row.shape[1] < size:
        row = jnp.concatenate([row, jnp.zeros((1, size - row.shape[1]), F32)], axis=1)
    high = row.astype(BF16).astype(F32)
    middle = (row - high).astype(BF16).astype(F32)
    low = row - high - middle
    at = iota((8, size), 0)
    block = jnp.where(at == 0, high, jnp.where(at == 1, middle, jnp.where(at == 2, low, 0.0)))
    return block.astype(BF16)


def sum_terms(block):
    return jnp.sum(block.astype(F32), axis=0, keepdims=True)


def pack_kernel(capacity, tokens, own, came, last, z, resid16, packed, wide):
    t = lax.axis_index("tp")
    quarter = last.shape[1]
    total = tokens[:, cols_of(t, quarter)].astype(F32) + (
        (own[:, 0:quarter].astype(F32) + came[:, 0:quarter].astype(F32)) + last[...].astype(F32)
    )
    short = total.astype(BF16)
    resid16[...] = short
    gap = jnp.zeros((z.shape[1] - short.shape[0], quarter), BF16)
    spread = dot(z[...], jnp.concatenate([short, gap], axis=0))
    for strided, near, cols in places(capacity, wide, quarter):
        wide[strided, :] = spread[near, cols]
    packed[...] = wide[...].astype(BF16)


def dense_kernel(
    gains, a0, a1, a2, a3, blend_weight, gate, up, down, p0, p1, p2, p3, blend,
    full, gate_v, up_v, down_v, sems,
):
    t = lax.axis_index("tp")
    loads = [
        pltpu.make_async_copy(a, b, sems.at[i])
        for i, (a, b) in enumerate(((gate, gate_v), (up, up_v), (down, down_v)))
    ]
    for load in loads:
        load.start()
    quarter = a0.shape[1]
    for m, a in enumerate((a0, a1, a2, a3)):
        full[:, cols_of(t ^ m, quarter)] = a[...]
    x = full[...].astype(F32)
    scale = lax.rsqrt(jnp.mean(x * x, axis=-1, keepdims=True) + EPS)
    normed = (x * scale * gains[...].astype(F32)).astype(BF16)
    score = jnp.sum(
        normed.astype(F32) * blend_weight[...].astype(F32), axis=-1, keepdims=True
    )
    blend[...] = jnp.broadcast_to(jax.nn.sigmoid(score), blend.shape)
    loads[0].wait()
    pre_gate = dot(normed, gate_v[...])
    loads[1].wait()
    pre_up = dot(normed, up_v[...])
    hidden = (jax.nn.silu(pre_gate) * pre_up).astype(BF16)
    loads[2].wait()
    for m, p in enumerate((p0, p1, p2, p3)):
        p[...] = dot(hidden, down_v[:, cols_of(t ^ m, quarter)]).astype(BF16)


def enter_kernel(capacity, arrived, gains, w0, w1, w2, w3, keep, send, wide, rows, sums):
    t = lax.axis_index("tp")
    lanes = arrived.shape[1]
    quarter = rows.shape[1]
    wide[...] = arrived[...].astype(F32)
    gain = gains[:, cols_of(t, quarter)].astype(F32)
    for strided, near, cols in places(capacity, wide, quarter):
        x = wide[strided, :]
        sums[near, :] = x * x if cols.start == 0 else sums[near, :] + x * x
        rows[near, cols] = (x * gain[:, cols]).astype(BF16)
    squares = nt_dot(jnp.ones((8, lanes), F32), sums[...], HIGHEST)[0:1]
    count = rows.shape[0]
    keep[count:, :] = jnp.broadcast_to(
        jnp.concatenate([squares, jnp.zeros((1, keep.shape[1] - count), F32)], axis=1),
        (8, keep.shape[1]),
    )
    send[count:, :] = three_terms(squares, send.shape[1])
    x = rows[...]
    pair = w0.shape[1]
    keep[0:count, 0:pair] = dot(x, w0[...])
    send[0:count, 0:pair] = dot(x, w1[...]).astype(BF16)
    keep[0:count, pair:] = dot(x, w2[...])
    send[0:count, pair:] = dot(x, w3[...]).astype(BF16)


def relay_kernel(keep, came, onward):
    pair = onward.shape[1]
    count = keep.shape[0] - 8
    onward[0:count, :] = (keep[0:count, pair:] + came[0:count, pair:].astype(F32)).astype(BF16)
    squares = keep[count : count + 1, :] + sum_terms(came[count:, :])
    onward[count : count + 8, :] = three_terms(squares[:, 0:pair], pair)
    onward[count + 8 :, :] = three_terms(squares[:, pair:], pair)


def hidden_kernel(width, keep, came, last, hidden):
    count, units = hidden.shape
    pair = 2 * units
    total = (
        keep[0:count, 0:pair] + came[0:count, 0:pair].astype(F32) + last[0:count, :].astype(F32)
    )
    squares = keep[count : count + 1, :] + sum_terms(came[count:, :])
    squares = squares + jnp.concatenate(
        [sum_terms(last[count : count + 8, :]), sum_terms(last[count + 8 :, :])], axis=1
    )
    column = jnp.transpose(jnp.broadcast_to(squares[:, 0:count], (8, count)))[:, 0:1]
    scale = lax.rsqrt(column / width + EPS)
    hidden[...] = (jax.nn.silu(total[:, 0:units] * scale) * (total[:, units:] * scale)).astype(BF16)


def leave_kernel(capacity, h0, h1, h2, h3, w0, w1, w2, w3, out, wide):
    total = (dot(h0[...], w0[...]) + dot(h1[...], w1[...])) + (
        dot(h2[...], w2[...]) + dot(h3[...], w3[...])
    )
    for strided, near, cols in places(capacity, wide, total.shape[1]):
        wide[strided, :] = total[near, cols]
    out[...] = wide[...].astype(BF16)


def final_kernel(
    capacity, returned, w, share0, share1, resid, blend, p0, p1, p2, p3, out, wide, rows
):
    count, quarter = resid.shape
    wide[...] = returned[...].astype(F32)
    for strided, near, cols in places(capacity, wide, quarter):
        rows[near, cols] = wide[strided, :].astype(BF16)
    picked = dot(w[...], rows[...])
    lanes = wide.shape[1]
    for c in range(quarter // lanes):
        cols = slice(c * lanes, (c + 1) * lanes)
        moe = share0[...] * picked[0:count, cols] + share1[...] * picked[count:, cols]
        dense = (p0[:, cols].astype(F32) + p1[:, cols].astype(F32)) + (
            p2[:, cols].astype(F32) + p3[:, cols].astype(F32)
        )
        out[:, cols] = (resid[:, cols].astype(F32) + moe + blend[...] * dense).astype(BF16)


def call(kernel, outs, scratch=(), limit=4, in_specs=None, out_specs=None):
    out_specs = out_specs or [VMEM] * len(outs)
    out_shape = [
        pltpu.VMEM(s, d) if spec is VMEM else jax.ShapeDtypeStruct(s, d)
        for (s, d), spec in zip(outs, out_specs)
    ]

    def run(*args):
        specs = in_specs or [VMEM] * len(args)
        spaces = {id(VMEM): pltpu.VMEM, id(HBM): pltpu.HBM}
        fixed = [
            pltpu.with_memory_space_constraint(a, spaces.get(id(spec), pl.ANY))
            for a, spec in zip(args, specs)
        ]
        return pl.pallas_call(
            kernel,
            out_shape=tuple(out_shape),
            in_specs=specs,
            out_specs=tuple(out_specs),
            scratch_shapes=list(scratch),
            compiler_params=pltpu.CompilerParams(vmem_limit_bytes=limit << 20),
        )(*fixed)

    return run


def per_device(
    tokens,
    norm_gain,
    in_weight,
    sequence_state_real,
    sequence_state_imaginary,
    eigen_decay_real,
    log_step,
    input_matrix_real,
    input_matrix_imaginary,
    output_matrix_real,
    output_matrix_imaginary,
    channel_skip_scale,
    out_weight,
    ffn_gain,
    routes,
    group_weight,
    expert_logit,
    expert_gate,
    expert_up,
    expert_down,
    dense_gate,
    dense_up,
    dense_down,
    blend_weight,
):
    rows, width = tokens.shape
    tp = lax.axis_size("tp")
    ep = lax.axis_size("ep")
    quarter = width // tp
    lanes = 128
    blocks = quarter // lanes
    capacity = max(2, 2 * rows * routes.shape[1] // (ep * expert_gate.shape[0]))
    slots = ep * capacity
    groups, entries, channels = input_matrix_real.shape
    hid = expert_gate.shape[2]
    gate = expert_gate.reshape(width, hid)
    up = expert_up.reshape(width, hid)
    down = expert_down.reshape(hid, width)
    piece = ((rows, quarter), BF16)

    def by_channel(matrix):
        return jnp.swapaxes(matrix, 1, 2).reshape(groups * channels, entries)

    states = ((rows, groups * entries), F32)
    state_inputs = (
        log_step,
        eigen_decay_real,
        channel_skip_scale,
        by_channel(input_matrix_real),
        by_channel(input_matrix_imaginary),
        output_matrix_real.reshape(groups * channels, entries),
        output_matrix_imaginary.reshape(groups * channels, entries),
        tokens,
        norm_gain,
        in_weight,
        sequence_state_real,
        sequence_state_imaginary,
        out_weight,
    )
    own, beside, new_re, new_im = call(
        state_kernel,
        [((rows, 2 * quarter), BF16)] * 2 + [states] * 2,
        [pltpu.SMEM(log_step.shape, F32)]
        + [pltpu.VMEM(x.shape, x.dtype) for x in state_inputs[1:]]
        + [pltpu.VMEM(states[0], F32)] * 2
        + [pltpu.VMEM((4, groups * channels, groups * entries), BF16)]
        + [pltpu.SemaphoreType.DMA((15,))],
        20,
        [HBM] * 13,
        [VMEM] * 2 + [HBM] * 2,
    )(*state_inputs)
    came_mix = exchanged(beside, 1)
    (onward,) = call(half_kernel, [piece])(own, came_mix)
    last_mix = exchanged(onward, 2)
    reshard = call(reshard_kernel, [((quarter, 2 * hid), BF16)] * 4 + [((hid, quarter), BF16)] * 4)
    pieces = reshard(gate, up, down)
    wide2 = exchanged(pieces[2], 2)
    wide3 = exchanged(pieces[3], 3)
    wide1 = exchanged(pieces[1], 1)
    moved = [pieces[0], wide1, wide2, wide3]
    downs = [pieces[4]] + [exchanged(pieces[4 + m], m) for m in (1, 2, 3)]
    z, w, share0, share1 = call(
        functools.partial(route_kernel, ep),
        [((slots, lanes), BF16), ((2 * rows, slots), BF16)] + [((rows, lanes), F32)] * 2,
        [pltpu.VMEM((8, lanes), jnp.int32)],
    )(routes.T, group_weight.reshape(1, rows), expert_logit.T)
    wide = pltpu.VMEM((slots * blocks, lanes), F32)
    resid16, packed = call(
        functools.partial(pack_kernel, capacity),
        [piece, ((slots * blocks, lanes), BF16)],
        [wide],
        8,
        out_specs=[VMEM, FREE],
    )(tokens, own, came_mix, last_mix, z)
    across = exchanged(resid16, 2)
    arrived = lax.all_to_all(
        packed.reshape(ep, capacity * blocks, lanes), "ep", 0, 0, tiled=True
    ).reshape(slots * blocks, lanes)
    near = [resid16, exchanged(resid16, 1), across, exchanged(across, 1)]
    gains = ffn_gain.reshape(1, width)
    *dense, blend = call(
        dense_kernel,
        [piece] * 4 + [((rows, lanes), F32)],
        [pltpu.VMEM((rows, width), BF16)]
        + [pltpu.VMEM(x.shape, BF16) for x in (dense_gate, dense_up, dense_down)]
        + [pltpu.SemaphoreType.DMA((3,))],
        12,
        [VMEM] * 6 + [HBM] * 3,
        [FREE] * 5,
    )(gains, *near, blend_weight.reshape(1, width), dense_gate, dense_up, dense_down)
    dense = [dense[0]] + [exchanged(dense[m], m) for m in (1, 2, 3)]
    keep, send = call(
        functools.partial(enter_kernel, capacity),
        [((slots + 8, 4 * hid), F32), ((slots + 8, 4 * hid), BF16)],
        [wide, pltpu.VMEM((slots, quarter), BF16), pltpu.VMEM((slots, lanes), F32)],
        8,
    )(arrived, gains, *moved)
    came = exchanged(send, 1)
    (onward,) = call(relay_kernel, [((slots + 16, 2 * hid), BF16)])(keep, came)
    last = exchanged(onward, 2)
    (hidden,) = call(
        functools.partial(hidden_kernel, float(width)), [((slots, hid), BF16)]
    )(keep, came, last)
    hidden = gathered(hidden)
    (sent,) = call(
        functools.partial(leave_kernel, capacity),
        [((slots * blocks, lanes), BF16)],
        [wide],
        8,
        out_specs=[FREE],
    )(*hidden, *downs)
    returned = lax.all_to_all(
        sent.reshape(ep, capacity * blocks, lanes), "ep", 0, 0, tiled=True
    ).reshape(slots * blocks, lanes)
    (new_tokens,) = call(
        functools.partial(final_kernel, capacity),
        [piece],
        [wide, pltpu.VMEM((slots, quarter), BF16)],
        8,
        out_specs=[FREE],
    )(returned, w, share0, share1, resid16, blend, *dense)
    return (new_tokens, new_re, new_im)


def solution(mesh):
    in_specs = (
        P("ep", None),
        P(),
        P(None, "tp"),
        P("ep", "tp"),
        P("ep", "tp"),
        P("tp", None),
        P("tp"),
        P("tp", None, None),
        P("tp", None, None),
        P("tp", None, None),
        P("tp", None, None),
        P("tp", None),
        P("tp", None),
        P(),
        P("ep", None),
        P("ep"),
        P("ep", None),
        P("ep", None, "tp"),
        P("ep", None, "tp"),
        P("ep", "tp", None),
        P(None, "tp"),
        P(None, "tp"),
        P("tp", None),
        P(),
    )
    out_specs = (P("ep", "tp"), P("ep", "tp"), P("ep", "tp"))

    return jax.shard_map(
        per_device, mesh=mesh, in_specs=in_specs, out_specs=out_specs, check_vma=False
    )
```

```python
import functools
import math

import jax
import jax.numpy as jnp
from jax import lax
from jax.experimental import pallas as pl
from jax.experimental.pallas import tpu as pltpu
from jax.sharding import PartitionSpec as P


EPS = 1e-06
F32 = jnp.float32
BF16 = jnp.bfloat16
HIGHEST = lax.Precision.HIGHEST
VMEM = pl.BlockSpec(memory_space=pltpu.VMEM)
SMEM = pl.BlockSpec(memory_space=pltpu.SMEM)
ANY = pl.BlockSpec(memory_space=pl.ANY)
HBM = pl.BlockSpec(memory_space=pltpu.HBM)
FREE = pl.BlockSpec(memory_space=pltpu.VMEM)
OUT = pl.BlockSpec()


def iota(shape, dim):
    return lax.broadcasted_iota(jnp.int32, shape, dim)


def nt_dot(a, b, precision=None):
    return lax.dot_general(
        a, b, (((1,), (1,)), ((), ())), precision=precision, preferred_element_type=F32
    )


def dot(a, b, precision=None):
    return jnp.dot(a, b, precision=precision, preferred_element_type=F32)


def cols_of(index, size):
    return pl.ds(pl.multiple_of(index * size, size), size)


def exchanged(value, mask):
    return lax.ppermute(value, "tp", [(i, i ^ mask) for i in range(4)])


def gathered(value):
    across = exchanged(value, 2)
    return [value, exchanged(value, 1), across, exchanged(across, 1)]


def spread_blocks(small, channels):
    rows, entries = small.shape
    groups = rows // channels
    width = groups * entries
    tiler = (iota((entries, width), 1) % entries == iota((entries, width), 0)).astype(BF16)
    tiled = dot(small.astype(BF16), tiler)
    mine = iota((rows, width), 0) // channels == iota((rows, width), 1) // entries
    return jnp.where(mine, tiled, 0.0).astype(BF16)


def row_of(small):
    groups, n = small.shape
    width = groups * n
    tiler = (iota((n, width), 1) % n == iota((n, width), 0)).astype(F32)
    tiled = dot(small, tiler, HIGHEST)
    mine = iota((groups, width), 0) == iota((groups, width), 1) // n
    return jnp.sum(jnp.where(mine, tiled, 0.0), axis=0, keepdims=True)


def state_kernel(*refs):
    inputs, (own, beside, new_re, new_im), held = refs[0:13], refs[13:17], refs[17:30]
    blocks_v, sems = refs[30:]
    t = lax.axis_index("tp")
    loads = [
        pltpu.make_async_copy(a, b, sems.at[i]) for i, (a, b) in enumerate(zip(inputs, held))
    ]
    for load in loads:
        load.start()
    log_step, decay, skip, b_re, b_im, c_re, c_im, tokens_v, gain, in_v, re_v, im_v, out_v = held
    groups, entries = decay.shape
    channels = skip.shape[1]
    width = groups * entries
    of_group = iota((1, width), 1) // entries
    for load in loads[0:3]:
        load.wait()
    logs = jnp.zeros((1, width), F32)
    for g in range(groups):
        logs = jnp.where(of_group == g, log_step[g], logs)
    step = jnp.exp(logs)
    eigen = row_of(decay[...])
    direct = row_of(skip[...])
    freq = math.pi * (iota((1, width), 1) % entries).astype(F32)
    magnitude = jnp.exp(eigen * step)
    turned = freq * step
    lam_re = magnitude * jnp.cos(turned)
    lam_im = magnitude * jnp.sin(turned)
    denom = eigen * eigen + freq * freq
    fac_re = ((lam_re - 1.0) * eigen + lam_im * freq) / denom
    fac_im = (lam_im * eigen - (lam_re - 1.0) * freq) / denom
    for load in loads[3:7]:
        load.wait()
    for k, small in enumerate((b_re, b_im, c_re, c_im)):
        blocks_v[k] = spread_blocks(small[...], channels)
    loads[7].wait()
    loads[8].wait()
    x = tokens_v[...].astype(F32)
    scale = lax.rsqrt(jnp.mean(x * x, axis=-1, keepdims=True) + EPS)
    normed = (x * scale * gain[...].astype(F32).reshape(1, -1)).astype(BF16)
    loads[9].wait()
    drive = dot(normed, in_v[...]).astype(BF16)
    in_re = dot(drive, blocks_v[0])
    in_im = dot(drive, blocks_v[1])
    loads[10].wait()
    loads[11].wait()
    was_re, was_im = re_v[...], im_v[...]
    fresh_re = lam_re * was_re - lam_im * was_im + (fac_re * in_re - fac_im * in_im)
    fresh_im = lam_re * was_im + lam_im * was_re + (fac_re * in_im + fac_im * in_re)
    new_re[...] = fresh_re
    new_im[...] = fresh_im
    mixed = (
        nt_dot(fresh_re.astype(BF16), blocks_v[2])
        - nt_dot(fresh_im.astype(BF16), blocks_v[3])
        + direct * drive.astype(F32)
    )
    act = jax.nn.gelu(mixed).astype(BF16)
    loads[12].wait()
    quarter = own.shape[1] // 2
    for m, pair in ((1, beside), (3, beside), (0, own), (2, own)):
        near = pl.ds((m // 2) * quarter, quarter)
        pair[:, near] = dot(act, out_v[:, cols_of(t ^ m, quarter)]).astype(BF16)


def half_kernel(own, came, onward):
    quarter = onward.shape[1]
    onward[...] = (own[:, quarter:].astype(F32) + came[:, quarter:].astype(F32)).astype(BF16)


def reshard_kernel(gate, up, down, *pieces):
    t = lax.axis_index("tp")
    hid = gate.shape[1]
    for m, (wide, deep) in enumerate(zip(pieces[:4], pieces[4:])):
        part = cols_of(t ^ m, wide.shape[0])
        wide[:, 0:hid] = gate[part, :]
        wide[:, hid:] = up[part, :]
        deep[...] = down[:, cols_of(t ^ m, deep.shape[1])]


def route_kernel(experts, routes, group_weight, logits, z, w, share0, share1, padded):
    rows = routes.shape[1]
    slots, lanes = z.shape
    padded[...] = jnp.full(padded.shape, -1, jnp.int32)
    padded[0:2, 0:rows] = routes[...]
    named = [padded[k : k + 1, :] for k in range(2)]
    hot = [(iota((experts, lanes), 0) == r).astype(F32) for r in named]
    earlier = (iota((lanes, lanes), 0) < iota((lanes, lanes), 1)).astype(BF16)
    before = dot((hot[0] + hot[1]).astype(BF16), earlier)
    place = [jnp.sum(before * h, axis=0, keepdims=True).astype(jnp.int32) for h in hot]
    slot = [jnp.where(r >= 0, p * experts + r, -1) for r, p in zip(named, place)]
    at = iota((slots, lanes), 0)
    z[...] = jnp.logical_or(at == slot[0], at == slot[1]).astype(F32).astype(BF16)
    eye = iota((lanes, lanes), 0) == iota((lanes, lanes), 1)
    at = iota((rows, slots), 1)
    for k in range(2):
        column = jnp.sum(jnp.where(eye, slot[k], 0), axis=1, keepdims=True)[0:rows]
        w[k * rows : (k + 1) * rows, :] = (at == column).astype(F32).astype(BF16)
    expo = jnp.exp(logits[...])
    share = group_weight[...] * expo / (expo[0:1] + expo[1:2])
    small_eye = iota((rows, rows), 0) == iota((rows, rows), 1)
    for k, out in enumerate((share0, share1)):
        column = jnp.sum(jnp.where(small_eye, share[k : k + 1], 0.0), axis=1, keepdims=True)
        out[...] = jnp.broadcast_to(column, out.shape)


def places(capacity, wide, quarter):
    blocks = quarter // wide.shape[1]
    peers = wide.shape[0] // (capacity * blocks)
    for s in range(capacity):
        for c in range(blocks):
            yield (
                pl.ds(c * capacity + s, peers, stride=capacity * blocks),
                slice(s * peers, (s + 1) * peers),
                slice(c * wide.shape[1], (c + 1) * wide.shape[1]),
            )


def three_terms(row, size):
    if row.shape[1] < size:
        row = jnp.concatenate([row, jnp.zeros((1, size - row.shape[1]), F32)], axis=1)
    high = row.astype(BF16).astype(F32)
    middle = (row - high).astype(BF16).astype(F32)
    low = row - high - middle
    at = iota((8, size), 0)
    block = jnp.where(at == 0, high, jnp.where(at == 1, middle, jnp.where(at == 2, low, 0.0)))
    return block.astype(BF16)


def sum_terms(block):
    return jnp.sum(block.astype(F32), axis=0, keepdims=True)


def pack_kernel(capacity, tokens, own, came, last, z, resid16, packed, wide):
    t = lax.axis_index("tp")
    quarter = last.shape[1]
    total = tokens[:, cols_of(t, quarter)].astype(F32) + (
        (own[:, 0:quarter].astype(F32) + came[:, 0:quarter].astype(F32)) + last[...].astype(F32)
    )
    short = total.astype(BF16)
    resid16[...] = short
    gap = jnp.zeros((z.shape[1] - short.shape[0], quarter), BF16)
    spread = dot(z[...], jnp.concatenate([short, gap], axis=0))
    for strided, near, cols in places(capacity, wide, quarter):
        wide[strided, :] = spread[near, cols]
    packed[...] = wide[...].astype(BF16)


def dense_kernel(
    gains, a0, a1, a2, a3, blend_weight, gate, up, down, p0, p1, p2, p3, blend,
    full, gate_v, up_v, down_v, sems,
):
    t = lax.axis_index("tp")
    loads = [
        pltpu.make_async_copy(a, b, sems.at[i])
        for i, (a, b) in enumerate(((gate, gate_v), (up, up_v), (down, down_v)))
    ]
    for load in loads:
        load.start()
    quarter = a0.shape[1]
    for m, a in enumerate((a0, a1, a2, a3)):
        full[:, cols_of(t ^ m, quarter)] = a[...]
    x = full[...].astype(F32)
    scale = lax.rsqrt(jnp.mean(x * x, axis=-1, keepdims=True) + EPS)
    normed = (x * scale * gains[...].astype(F32)).astype(BF16)
    score = jnp.sum(
        normed.astype(F32) * blend_weight[...].astype(F32), axis=-1, keepdims=True
    )
    blend[...] = jnp.broadcast_to(jax.nn.sigmoid(score), blend.shape)
    loads[0].wait()
    pre_gate = dot(normed, gate_v[...])
    loads[1].wait()
    pre_up = dot(normed, up_v[...])
    hidden = (jax.nn.silu(pre_gate) * pre_up).astype(BF16)
    loads[2].wait()
    for m, p in enumerate((p0, p1, p2, p3)):
        p[...] = dot(hidden, down_v[:, cols_of(t ^ m, quarter)]).astype(BF16)


def enter_kernel(capacity, arrived, gains, w0, w1, w2, w3, keep, send, wide, rows, sums):
    t = lax.axis_index("tp")
    lanes = arrived.shape[1]
    quarter = rows.shape[1]
    wide[...] = arrived[...].astype(F32)
    gain = gains[:, cols_of(t, quarter)].astype(F32)
    for strided, near, cols in places(capacity, wide, quarter):
        x = wide[strided, :]
        sums[near, :] = x * x if cols.start == 0 else sums[near, :] + x * x
        rows[near, cols] = (x * gain[:, cols]).astype(BF16)
    squares = nt_dot(jnp.ones((8, lanes), F32), sums[...], HIGHEST)[0:1]
    count = rows.shape[0]
    keep[count:, :] = jnp.broadcast_to(
        jnp.concatenate([squares, jnp.zeros((1, keep.shape[1] - count), F32)], axis=1),
        (8, keep.shape[1]),
    )
    send[count:, :] = three_terms(squares, send.shape[1])
    x = rows[...]
    pair = w0.shape[1]
    keep[0:count, 0:pair] = dot(x, w0[...])
    send[0:count, 0:pair] = dot(x, w1[...]).astype(BF16)
    keep[0:count, pair:] = dot(x, w2[...])
    send[0:count, pair:] = dot(x, w3[...]).astype(BF16)


def relay_kernel(keep, came, onward):
    pair = onward.shape[1]
    count = keep.shape[0] - 8
    onward[0:count, :] = (keep[0:count, pair:] + came[0:count, pair:].astype(F32)).astype(BF16)
    squares = keep[count : count + 1, :] + sum_terms(came[count:, :])
    onward[count : count + 8, :] = three_terms(squares[:, 0:pair], pair)
    onward[count + 8 :, :] = three_terms(squares[:, pair:], pair)


def hidden_kernel(width, keep, came, last, hidden):
    count, units = hidden.shape
    pair = 2 * units
    total = (
        keep[0:count, 0:pair] + came[0:count, 0:pair].astype(F32) + last[0:count, :].astype(F32)
    )
    squares = keep[count : count + 1, :] + sum_terms(came[count:, :])
    squares = squares + jnp.concatenate(
        [sum_terms(last[count : count + 8, :]), sum_terms(last[count + 8 :, :])], axis=1
    )
    column = jnp.transpose(jnp.broadcast_to(squares[:, 0:count], (8, count)))[:, 0:1]
    scale = lax.rsqrt(column / width + EPS)
    hidden[...] = (jax.nn.silu(total[:, 0:units] * scale) * (total[:, units:] * scale)).astype(BF16)


def leave_kernel(capacity, h0, h1, h2, h3, w0, w1, w2, w3, out, wide):
    total = (dot(h0[...], w0[...]) + dot(h1[...], w1[...])) + (
        dot(h2[...], w2[...]) + dot(h3[...], w3[...])
    )
    for strided, near, cols in places(capacity, wide, total.shape[1]):
        wide[strided, :] = total[near, cols]
    out[...] = wide[...].astype(BF16)


def final_kernel(
    capacity, returned, w, share0, share1, resid, blend, p0, p1, p2, p3, out, wide, rows
):
    count, quarter = resid.shape
    wide[...] = returned[...].astype(F32)
    for strided, near, cols in places(capacity, wide, quarter):
        rows[near, cols] = wide[strided, :].astype(BF16)
    picked = dot(w[...], rows[...])
    lanes = wide.shape[1]
    for c in range(quarter // lanes):
        cols = slice(c * lanes, (c + 1) * lanes)
        moe = share0[...] * picked[0:count, cols] + share1[...] * picked[count:, cols]
        dense = (p0[:, cols].astype(F32) + p1[:, cols].astype(F32)) + (
            p2[:, cols].astype(F32) + p3[:, cols].astype(F32)
        )
        out[:, cols] = (resid[:, cols].astype(F32) + moe + blend[...] * dense).astype(BF16)


def call(kernel, outs, scratch=(), limit=4, in_specs=None, out_specs=None):
    out_specs = out_specs or [VMEM] * len(outs)
    kinds = {id(VMEM): pltpu.VMEM, id(OUT): pltpu.HBM}
    out_shape = [
        kinds.get(id(spec), jax.ShapeDtypeStruct)(s, d) for (s, d), spec in zip(outs, out_specs)
    ]

    def run(*args):
        specs = in_specs or [VMEM] * len(args)
        spaces = {id(VMEM): pltpu.VMEM, id(HBM): pltpu.HBM}
        fixed = [
            pltpu.with_memory_space_constraint(a, spaces.get(id(spec), pl.ANY))
            for a, spec in zip(args, specs)
        ]
        return pl.pallas_call(
            kernel,
            out_shape=tuple(out_shape),
            in_specs=specs,
            out_specs=tuple(out_specs),
            scratch_shapes=list(scratch),
            compiler_params=pltpu.CompilerParams(vmem_limit_bytes=limit << 20),
        )(*fixed)

    return run


def per_device(
    tokens,
    norm_gain,
    in_weight,
    sequence_state_real,
    sequence_state_imaginary,
    eigen_decay_real,
    log_step,
    input_matrix_real,
    input_matrix_imaginary,
    output_matrix_real,
    output_matrix_imaginary,
    channel_skip_scale,
    out_weight,
    ffn_gain,
    routes,
    group_weight,
    expert_logit,
    expert_gate,
    expert_up,
    expert_down,
    dense_gate,
    dense_up,
    dense_down,
    blend_weight,
):
    rows, width = tokens.shape
    tp = lax.axis_size("tp")
    ep = lax.axis_size("ep")
    quarter = width // tp
    lanes = 128
    blocks = quarter // lanes
    capacity = max(2, 2 * rows * routes.shape[1] // (ep * expert_gate.shape[0]))
    slots = ep * capacity
    groups, entries, channels = input_matrix_real.shape
    hid = expert_gate.shape[2]
    gate = expert_gate.reshape(width, hid)
    up = expert_up.reshape(width, hid)
    down = expert_down.reshape(hid, width)
    piece = ((rows, quarter), BF16)

    def by_channel(matrix):
        return jnp.swapaxes(matrix, 1, 2).reshape(groups * channels, entries)

    states = ((rows, groups * entries), F32)
    state_inputs = (
        log_step,
        eigen_decay_real,
        channel_skip_scale,
        by_channel(input_matrix_real),
        by_channel(input_matrix_imaginary),
        output_matrix_real.reshape(groups * channels, entries),
        output_matrix_imaginary.reshape(groups * channels, entries),
        tokens,
        norm_gain,
        in_weight,
        sequence_state_real,
        sequence_state_imaginary,
        out_weight,
    )
    own, beside, new_re, new_im = call(
        state_kernel,
        [((rows, 2 * quarter), BF16)] * 2 + [states] * 2,
        [pltpu.SMEM(log_step.shape, F32)]
        + [pltpu.VMEM(x.shape, x.dtype) for x in state_inputs[1:]]
        + [pltpu.VMEM((4, groups * channels, groups * entries), BF16)]
        + [pltpu.SemaphoreType.DMA((13,))],
        20,
        [HBM] * 13,
        [VMEM] * 4,
    )(*state_inputs)
    came_mix = exchanged(beside, 1)
    (onward,) = call(half_kernel, [piece])(own, came_mix)
    last_mix = exchanged(onward, 2)
    reshard = call(reshard_kernel, [((quarter, 2 * hid), BF16)] * 4 + [((hid, quarter), BF16)] * 4)
    pieces = reshard(gate, up, down)
    wide2 = exchanged(pieces[2], 2)
    wide3 = exchanged(pieces[3], 3)
    wide1 = exchanged(pieces[1], 1)
    moved = [pieces[0], wide1, wide2, wide3]
    downs = [pieces[4]] + [exchanged(pieces[4 + m], m) for m in (1, 2, 3)]
    z, w, share0, share1 = call(
        functools.partial(route_kernel, ep),
        [((slots, lanes), BF16), ((2 * rows, slots), BF16)] + [((rows, lanes), F32)] * 2,
        [pltpu.VMEM((8, lanes), jnp.int32)],
    )(routes.T, group_weight.reshape(1, rows), expert_logit.T)
    wide = pltpu.VMEM((slots * blocks, lanes), F32)
    resid16, packed = call(
        functools.partial(pack_kernel, capacity),
        [piece, ((slots * blocks, lanes), BF16)],
        [wide],
        8,
        out_specs=[VMEM, FREE],
    )(tokens, own, came_mix, last_mix, z)
    across = exchanged(resid16, 2)
    arrived = lax.all_to_all(
        packed.reshape(ep, capacity * blocks, lanes), "ep", 0, 0, tiled=True
    ).reshape(slots * blocks, lanes)
    near = [resid16, exchanged(resid16, 1), across, exchanged(across, 1)]
    gains = ffn_gain.reshape(1, width)
    *dense, blend = call(
        dense_kernel,
        [piece] * 4 + [((rows, lanes), F32)],
        [pltpu.VMEM((rows, width), BF16)]
        + [pltpu.VMEM(x.shape, BF16) for x in (dense_gate, dense_up, dense_down)]
        + [pltpu.SemaphoreType.DMA((3,))],
        12,
        [VMEM] * 6 + [HBM] * 3,
        [OUT] * 5,
    )(gains, *near, blend_weight.reshape(1, width), dense_gate, dense_up, dense_down)
    dense = [dense[0]] + [exchanged(dense[m], m) for m in (1, 2, 3)]
    keep, send = call(
        functools.partial(enter_kernel, capacity),
        [((slots + 8, 4 * hid), F32), ((slots + 8, 4 * hid), BF16)],
        [wide, pltpu.VMEM((slots, quarter), BF16), pltpu.VMEM((slots, lanes), F32)],
        8,
    )(arrived, gains, *moved)
    came = exchanged(send, 1)
    (onward,) = call(relay_kernel, [((slots + 16, 2 * hid), BF16)])(keep, came)
    last = exchanged(onward, 2)
    (hidden,) = call(
        functools.partial(hidden_kernel, float(width)), [((slots, hid), BF16)]
    )(keep, came, last)
    hidden = gathered(hidden)
    (sent,) = call(
        functools.partial(leave_kernel, capacity),
        [((slots * blocks, lanes), BF16)],
        [wide],
        8,
        out_specs=[FREE],
    )(*hidden, *downs)
    returned = lax.all_to_all(
        sent.reshape(ep, capacity * blocks, lanes), "ep", 0, 0, tiled=True
    ).reshape(slots * blocks, lanes)
    (new_tokens,) = call(
        functools.partial(final_kernel, capacity),
        [piece],
        [wide, pltpu.VMEM((slots, quarter), BF16)],
        8,
        out_specs=[FREE],
    )(returned, w, share0, share1, resid16, blend, *dense)
    return (new_tokens, new_re, new_im)


def solution(mesh):
    in_specs = (
        P("ep", None),
        P(),
        P(None, "tp"),
        P("ep", "tp"),
        P("ep", "tp"),
        P("tp", None),
        P("tp"),
        P("tp", None, None),
        P("tp", None, None),
        P("tp", None, None),
        P("tp", None, None),
        P("tp", None),
        P("tp", None),
        P(),
        P("ep", None),
        P("ep"),
        P("ep", None),
        P("ep", None, "tp"),
        P("ep", None, "tp"),
        P("ep", "tp", None),
        P(None, "tp"),
        P(None, "tp"),
        P("tp", None),
        P(),
    )
    out_specs = (P("ep", "tp"), P("ep", "tp"), P("ep", "tp"))

    return jax.shard_map(
        per_device, mesh=mesh, in_specs=in_specs, out_specs=out_specs, check_vma=False
    )
```

```python
import functools
import math

import jax
import jax.numpy as jnp
from jax import lax
from jax.experimental import pallas as pl
from jax.experimental.pallas import tpu as pltpu
from jax.sharding import PartitionSpec as P


EPS = 1e-06
F32 = jnp.float32
BF16 = jnp.bfloat16
HIGHEST = lax.Precision.HIGHEST
VMEM = pl.BlockSpec(memory_space=pltpu.VMEM)
SMEM = pl.BlockSpec(memory_space=pltpu.SMEM)
ANY = pl.BlockSpec(memory_space=pl.ANY)
HBM = pl.BlockSpec(memory_space=pltpu.HBM)
FREE = pl.BlockSpec(memory_space=pltpu.VMEM)
OUT = pl.BlockSpec()


def iota(shape, dim):
    return lax.broadcasted_iota(jnp.int32, shape, dim)


def nt_dot(a, b, precision=None):
    return lax.dot_general(
        a, b, (((1,), (1,)), ((), ())), precision=precision, preferred_element_type=F32
    )


def dot(a, b, precision=None):
    return jnp.dot(a, b, precision=precision, preferred_element_type=F32)


def cols_of(index, size):
    return pl.ds(pl.multiple_of(index * size, size), size)


def exchanged(value, mask):
    return lax.ppermute(value, "tp", [(i, i ^ mask) for i in range(4)])


def gathered(value):
    across = exchanged(value, 2)
    return [value, exchanged(value, 1), across, exchanged(across, 1)]


def spread_blocks(small, channels):
    rows, entries = small.shape
    groups = rows // channels
    width = groups * entries
    tiler = (iota((entries, width), 1) % entries == iota((entries, width), 0)).astype(BF16)
    tiled = dot(small.astype(BF16), tiler)
    mine = iota((rows, width), 0) // channels == iota((rows, width), 1) // entries
    return jnp.where(mine, tiled, 0.0).astype(BF16)


def row_of(small):
    groups, n = small.shape
    width = groups * n
    tiler = (iota((n, width), 1) % n == iota((n, width), 0)).astype(F32)
    tiled = dot(small, tiler, HIGHEST)
    mine = iota((groups, width), 0) == iota((groups, width), 1) // n
    return jnp.sum(jnp.where(mine, tiled, 0.0), axis=0, keepdims=True)


def state_kernel(*refs):
    inputs, (own, beside, new_re, new_im), held = refs[0:13], refs[13:17], refs[17:30]
    blocks_v, sems = refs[30:]
    t = lax.axis_index("tp")
    loads = [
        pltpu.make_async_copy(a, b, sems.at[i]) for i, (a, b) in enumerate(zip(inputs, held))
    ]
    for load in loads:
        load.start()
    log_step, decay, skip, b_re, b_im, c_re, c_im, tokens_v, gain, in_v, re_v, im_v, out_v = held
    groups, entries = decay.shape
    channels = skip.shape[1]
    width = groups * entries
    of_group = iota((1, width), 1) // entries
    for load in loads[0:3]:
        load.wait()
    logs = jnp.zeros((1, width), F32)
    for g in range(groups):
        logs = jnp.where(of_group == g, log_step[g], logs)
    step = jnp.exp(logs)
    eigen = row_of(decay[...])
    direct = row_of(skip[...])
    freq = math.pi * (iota((1, width), 1) % entries).astype(F32)
    magnitude = jnp.exp(eigen * step)
    turned = freq * step
    lam_re = magnitude * jnp.cos(turned)
    lam_im = magnitude * jnp.sin(turned)
    denom = eigen * eigen + freq * freq
    fac_re = ((lam_re - 1.0) * eigen + lam_im * freq) / denom
    fac_im = (lam_im * eigen - (lam_re - 1.0) * freq) / denom
    for load in loads[3:7]:
        load.wait()
    for k, small in enumerate((b_re, b_im, c_re, c_im)):
        blocks_v[k] = spread_blocks(small[...], channels)
    loads[7].wait()
    loads[8].wait()
    x = tokens_v[...].astype(F32)
    scale = lax.rsqrt(jnp.mean(x * x, axis=-1, keepdims=True) + EPS)
    normed = (x * scale * gain[...].astype(F32).reshape(1, -1)).astype(BF16)
    loads[9].wait()
    drive = dot(normed, in_v[...]).astype(BF16)
    in_re = dot(drive, blocks_v[0])
    in_im = dot(drive, blocks_v[1])
    loads[10].wait()
    loads[11].wait()
    was_re, was_im = re_v[...], im_v[...]
    fresh_re = lam_re * was_re - lam_im * was_im + (fac_re * in_re - fac_im * in_im)
    fresh_im = lam_re * was_im + lam_im * was_re + (fac_re * in_im + fac_im * in_re)
    new_re[...] = fresh_re
    new_im[...] = fresh_im
    mixed = (
        nt_dot(fresh_re.astype(BF16), blocks_v[2])
        - nt_dot(fresh_im.astype(BF16), blocks_v[3])
        + direct * drive.astype(F32)
    )
    act = jax.nn.gelu(mixed).astype(BF16)
    loads[12].wait()
    quarter = own.shape[1] // 2
    for m, pair in ((1, beside), (3, beside), (0, own), (2, own)):
        near = pl.ds((m // 2) * quarter, quarter)
        pair[:, near] = dot(act, out_v[:, cols_of(t ^ m, quarter)]).astype(BF16)


def half_kernel(own, came, onward):
    quarter = onward.shape[1]
    onward[...] = (own[:, quarter:].astype(F32) + came[:, quarter:].astype(F32)).astype(BF16)


def reshard_kernel(gate, up, down, *pieces):
    t = lax.axis_index("tp")
    hid = gate.shape[1]
    for m, (wide, deep) in enumerate(zip(pieces[:4], pieces[4:])):
        part = cols_of(t ^ m, wide.shape[0])
        wide[:, 0:hid] = gate[part, :]
        wide[:, hid:] = up[part, :]
        deep[...] = down[:, cols_of(t ^ m, deep.shape[1])]


def route_kernel(experts, routes, group_weight, logits, z, w, share0, share1, padded):
    rows = routes.shape[1]
    slots, lanes = z.shape
    padded[...] = jnp.full(padded.shape, -1, jnp.int32)
    padded[0:2, 0:rows] = routes[...]
    named = [padded[k : k + 1, :] for k in range(2)]
    hot = [(iota((experts, lanes), 0) == r).astype(F32) for r in named]
    earlier = (iota((lanes, lanes), 0) < iota((lanes, lanes), 1)).astype(BF16)
    before = dot((hot[0] + hot[1]).astype(BF16), earlier)
    place = [jnp.sum(before * h, axis=0, keepdims=True).astype(jnp.int32) for h in hot]
    slot = [jnp.where(r >= 0, p * experts + r, -1) for r, p in zip(named, place)]
    at = iota((slots, lanes), 0)
    z[...] = jnp.logical_or(at == slot[0], at == slot[1]).astype(F32).astype(BF16)
    eye = iota((lanes, lanes), 0) == iota((lanes, lanes), 1)
    at = iota((rows, slots), 1)
    for k in range(2):
        column = jnp.sum(jnp.where(eye, slot[k], 0), axis=1, keepdims=True)[0:rows]
        w[k * rows : (k + 1) * rows, :] = (at == column).astype(F32).astype(BF16)
    expo = jnp.exp(logits[...])
    share = group_weight[...] * expo / (expo[0:1] + expo[1:2])
    small_eye = iota((rows, rows), 0) == iota((rows, rows), 1)
    for k, out in enumerate((share0, share1)):
        column = jnp.sum(jnp.where(small_eye, share[k : k + 1], 0.0), axis=1, keepdims=True)
        out[...] = jnp.broadcast_to(column, out.shape)


def places(capacity, wide, quarter):
    blocks = quarter // wide.shape[1]
    peers = wide.shape[0] // (capacity * blocks)
    for s in range(capacity):
        for c in range(blocks):
            yield (
                pl.ds(c * capacity + s, peers, stride=capacity * blocks),
                slice(s * peers, (s + 1) * peers),
                slice(c * wide.shape[1], (c + 1) * wide.shape[1]),
            )


def three_terms(row, size):
    if row.shape[1] < size:
        row = jnp.concatenate([row, jnp.zeros((1, size - row.shape[1]), F32)], axis=1)
    high = row.astype(BF16).astype(F32)
    middle = (row - high).astype(BF16).astype(F32)
    low = row - high - middle
    at = iota((8, size), 0)
    block = jnp.where(at == 0, high, jnp.where(at == 1, middle, jnp.where(at == 2, low, 0.0)))
    return block.astype(BF16)


def sum_terms(block):
    return jnp.sum(block.astype(F32), axis=0, keepdims=True)


def pack_kernel(capacity, tokens, own, came, last, z, resid16, packed, wide):
    t = lax.axis_index("tp")
    quarter = last.shape[1]
    total = tokens[:, cols_of(t, quarter)].astype(F32) + (
        (own[:, 0:quarter].astype(F32) + came[:, 0:quarter].astype(F32)) + last[...].astype(F32)
    )
    short = total.astype(BF16)
    resid16[...] = short
    gap = jnp.zeros((z.shape[1] - short.shape[0], quarter), BF16)
    spread = dot(z[...], jnp.concatenate([short, gap], axis=0))
    for strided, near, cols in places(capacity, wide, quarter):
        wide[strided, :] = spread[near, cols]
    packed[...] = wide[...].astype(BF16)


def dense_kernel(
    gains, a0, a1, a2, a3, blend_weight, gate, up, down, own, beside, blend,
    full, gate_v, up_v, down_v, sems,
):
    t = lax.axis_index("tp")
    loads = [
        pltpu.make_async_copy(a, b, sems.at[i])
        for i, (a, b) in enumerate(((gate, gate_v), (up, up_v), (down, down_v)))
    ]
    for load in loads:
        load.start()
    quarter = a0.shape[1]
    for m, a in enumerate((a0, a1, a2, a3)):
        full[:, cols_of(t ^ m, quarter)] = a[...]
    x = full[...].astype(F32)
    scale = lax.rsqrt(jnp.mean(x * x, axis=-1, keepdims=True) + EPS)
    normed = (x * scale * gains[...].astype(F32)).astype(BF16)
    score = jnp.sum(
        normed.astype(F32) * blend_weight[...].astype(F32), axis=-1, keepdims=True
    )
    blend[...] = jnp.broadcast_to(jax.nn.sigmoid(score), blend.shape)
    loads[0].wait()
    pre_gate = dot(normed, gate_v[...])
    loads[1].wait()
    pre_up = dot(normed, up_v[...])
    hidden = (jax.nn.silu(pre_gate) * pre_up).astype(BF16)
    loads[2].wait()
    for m, pair in ((1, beside), (3, beside), (0, own), (2, own)):
        near = pl.ds((m // 2) * quarter, quarter)
        pair[:, near] = dot(hidden, down_v[:, cols_of(t ^ m, quarter)]).astype(BF16)


def enter_kernel(capacity, arrived, gains, w0, w1, w2, w3, keep, send, wide, rows, sums):
    t = lax.axis_index("tp")
    lanes = arrived.shape[1]
    quarter = rows.shape[1]
    wide[...] = arrived[...].astype(F32)
    gain = gains[:, cols_of(t, quarter)].astype(F32)
    for strided, near, cols in places(capacity, wide, quarter):
        x = wide[strided, :]
        sums[near, :] = x * x if cols.start == 0 else sums[near, :] + x * x
        rows[near, cols] = (x * gain[:, cols]).astype(BF16)
    squares = nt_dot(jnp.ones((8, lanes), F32), sums[...], HIGHEST)[0:1]
    count = rows.shape[0]
    keep[count:, :] = jnp.broadcast_to(
        jnp.concatenate([squares, jnp.zeros((1, keep.shape[1] - count), F32)], axis=1),
        (8, keep.shape[1]),
    )
    send[count:, :] = three_terms(squares, send.shape[1])
    x = rows[...]
    pair = w0.shape[1]
    keep[0:count, 0:pair] = dot(x, w0[...])
    send[0:count, 0:pair] = dot(x, w1[...]).astype(BF16)
    keep[0:count, pair:] = dot(x, w2[...])
    send[0:count, pair:] = dot(x, w3[...]).astype(BF16)


def relay_kernel(keep, came, onward):
    pair = onward.shape[1]
    count = keep.shape[0] - 8
    onward[0:count, :] = (keep[0:count, pair:] + came[0:count, pair:].astype(F32)).astype(BF16)
    squares = keep[count : count + 1, :] + sum_terms(came[count:, :])
    onward[count : count + 8, :] = three_terms(squares[:, 0:pair], pair)
    onward[count + 8 :, :] = three_terms(squares[:, pair:], pair)


def hidden_kernel(width, keep, came, last, hidden):
    count, units = hidden.shape
    pair = 2 * units
    total = (
        keep[0:count, 0:pair] + came[0:count, 0:pair].astype(F32) + last[0:count, :].astype(F32)
    )
    squares = keep[count : count + 1, :] + sum_terms(came[count:, :])
    squares = squares + jnp.concatenate(
        [sum_terms(last[count : count + 8, :]), sum_terms(last[count + 8 :, :])], axis=1
    )
    column = jnp.transpose(jnp.broadcast_to(squares[:, 0:count], (8, count)))[:, 0:1]
    scale = lax.rsqrt(column / width + EPS)
    hidden[...] = (jax.nn.silu(total[:, 0:units] * scale) * (total[:, units:] * scale)).astype(BF16)


def leave_kernel(capacity, h0, h1, h2, h3, w0, w1, w2, w3, out, wide):
    total = (dot(h0[...], w0[...]) + dot(h1[...], w1[...])) + (
        dot(h2[...], w2[...]) + dot(h3[...], w3[...])
    )
    for strided, near, cols in places(capacity, wide, total.shape[1]):
        wide[strided, :] = total[near, cols]
    out[...] = wide[...].astype(BF16)


def final_kernel(
    capacity, returned, w, share0, share1, resid, blend, own, came, last, out, wide, rows
):
    count, quarter = resid.shape
    wide[...] = returned[...].astype(F32)
    for strided, near, cols in places(capacity, wide, quarter):
        rows[near, cols] = wide[strided, :].astype(BF16)
    picked = dot(w[...], rows[...])
    lanes = wide.shape[1]
    for c in range(quarter // lanes):
        cols = slice(c * lanes, (c + 1) * lanes)
        moe = share0[...] * picked[0:count, cols] + share1[...] * picked[count:, cols]
        dense = (own[:, cols].astype(F32) + came[:, cols].astype(F32)) + last[:, cols].astype(F32)
        out[:, cols] = (resid[:, cols].astype(F32) + moe + blend[...] * dense).astype(BF16)


def call(kernel, outs, scratch=(), limit=4, in_specs=None, out_specs=None):
    out_specs = out_specs or [VMEM] * len(outs)
    kinds = {id(VMEM): pltpu.VMEM, id(OUT): pltpu.HBM}
    out_shape = [
        kinds.get(id(spec), jax.ShapeDtypeStruct)(s, d) for (s, d), spec in zip(outs, out_specs)
    ]

    def run(*args):
        specs = in_specs or [VMEM] * len(args)
        spaces = {id(VMEM): pltpu.VMEM, id(HBM): pltpu.HBM}
        fixed = [
            pltpu.with_memory_space_constraint(a, spaces.get(id(spec), pl.ANY))
            for a, spec in zip(args, specs)
        ]
        return pl.pallas_call(
            kernel,
            out_shape=tuple(out_shape),
            in_specs=specs,
            out_specs=tuple(out_specs),
            scratch_shapes=list(scratch),
            compiler_params=pltpu.CompilerParams(vmem_limit_bytes=limit << 20),
        )(*fixed)

    return run


def per_device(
    tokens,
    norm_gain,
    in_weight,
    sequence_state_real,
    sequence_state_imaginary,
    eigen_decay_real,
    log_step,
    input_matrix_real,
    input_matrix_imaginary,
    output_matrix_real,
    output_matrix_imaginary,
    channel_skip_scale,
    out_weight,
    ffn_gain,
    routes,
    group_weight,
    expert_logit,
    expert_gate,
    expert_up,
    expert_down,
    dense_gate,
    dense_up,
    dense_down,
    blend_weight,
):
    rows, width = tokens.shape
    tp = lax.axis_size("tp")
    ep = lax.axis_size("ep")
    quarter = width // tp
    lanes = 128
    blocks = quarter // lanes
    capacity = max(2, 2 * rows * routes.shape[1] // (ep * expert_gate.shape[0]))
    slots = ep * capacity
    groups, entries, channels = input_matrix_real.shape
    hid = expert_gate.shape[2]
    gate = expert_gate.reshape(width, hid)
    up = expert_up.reshape(width, hid)
    down = expert_down.reshape(hid, width)
    piece = ((rows, quarter), BF16)

    def by_channel(matrix):
        return jnp.swapaxes(matrix, 1, 2).reshape(groups * channels, entries)

    states = ((rows, groups * entries), F32)
    state_inputs = (
        log_step,
        eigen_decay_real,
        channel_skip_scale,
        by_channel(input_matrix_real),
        by_channel(input_matrix_imaginary),
        output_matrix_real.reshape(groups * channels, entries),
        output_matrix_imaginary.reshape(groups * channels, entries),
        tokens,
        norm_gain,
        in_weight,
        sequence_state_real,
        sequence_state_imaginary,
        out_weight,
    )
    own, beside, new_re, new_im = call(
        state_kernel,
        [((rows, 2 * quarter), BF16)] * 2 + [states] * 2,
        [pltpu.SMEM(log_step.shape, F32)]
        + [pltpu.VMEM(x.shape, x.dtype) for x in state_inputs[1:]]
        + [pltpu.VMEM((4, groups * channels, groups * entries), BF16)]
        + [pltpu.SemaphoreType.DMA((13,))],
        20,
        [HBM] * 13,
        [VMEM] * 4,
    )(*state_inputs)
    came_mix = exchanged(beside, 1)
    (onward,) = call(half_kernel, [piece])(own, came_mix)
    last_mix = exchanged(onward, 2)
    reshard = call(reshard_kernel, [((quarter, 2 * hid), BF16)] * 4 + [((hid, quarter), BF16)] * 4)
    pieces = reshard(gate, up, down)
    wide2 = exchanged(pieces[2], 2)
    wide3 = exchanged(pieces[3], 3)
    wide1 = exchanged(pieces[1], 1)
    moved = [pieces[0], wide1, wide2, wide3]
    downs = [pieces[4]] + [exchanged(pieces[4 + m], m) for m in (1, 2, 3)]
    z, w, share0, share1 = call(
        functools.partial(route_kernel, ep),
        [((slots, lanes), BF16), ((2 * rows, slots), BF16)] + [((rows, lanes), F32)] * 2,
        [pltpu.VMEM((8, lanes), jnp.int32)],
    )(routes.T, group_weight.reshape(1, rows), expert_logit.T)
    wide = pltpu.VMEM((slots * blocks, lanes), F32)
    resid16, packed = call(
        functools.partial(pack_kernel, capacity),
        [piece, ((slots * blocks, lanes), BF16)],
        [wide],
        8,
        out_specs=[VMEM, FREE],
    )(tokens, own, came_mix, last_mix, z)
    across = exchanged(resid16, 2)
    arrived = lax.all_to_all(
        packed.reshape(ep, capacity * blocks, lanes), "ep", 0, 0, tiled=True
    ).reshape(slots * blocks, lanes)
    near = [resid16, exchanged(resid16, 1), across, exchanged(across, 1)]
    gains = ffn_gain.reshape(1, width)
    dense_own, dense_beside, blend = call(
        dense_kernel,
        [((rows, 2 * quarter), BF16)] * 2 + [((rows, lanes), F32)],
        [pltpu.VMEM((rows, width), BF16)]
        + [pltpu.VMEM(x.shape, BF16) for x in (dense_gate, dense_up, dense_down)]
        + [pltpu.SemaphoreType.DMA((3,))],
        12,
        [VMEM] * 6 + [HBM] * 3,
        [OUT] * 3,
    )(gains, *near, blend_weight.reshape(1, width), dense_gate, dense_up, dense_down)
    dense_came = exchanged(dense_beside, 1)
    keep, send = call(
        functools.partial(enter_kernel, capacity),
        [((slots + 8, 4 * hid), F32), ((slots + 8, 4 * hid), BF16)],
        [wide, pltpu.VMEM((slots, quarter), BF16), pltpu.VMEM((slots, lanes), F32)],
        8,
    )(arrived, gains, *moved)
    came = exchanged(send, 1)
    (onward,) = call(relay_kernel, [((slots + 16, 2 * hid), BF16)])(keep, came)
    last = exchanged(onward, 2)
    (dense_onward,) = call(half_kernel, [piece], out_specs=[OUT])(dense_own, dense_came)
    dense_last = exchanged(dense_onward, 2)
    (hidden,) = call(
        functools.partial(hidden_kernel, float(width)), [((slots, hid), BF16)]
    )(keep, came, last)
    hidden = gathered(hidden)
    (sent,) = call(
        functools.partial(leave_kernel, capacity),
        [((slots * blocks, lanes), BF16)],
        [wide],
        8,
        out_specs=[FREE],
    )(*hidden, *downs)
    returned = lax.all_to_all(
        sent.reshape(ep, capacity * blocks, lanes), "ep", 0, 0, tiled=True
    ).reshape(slots * blocks, lanes)
    (new_tokens,) = call(
        functools.partial(final_kernel, capacity),
        [piece],
        [wide, pltpu.VMEM((slots, quarter), BF16)],
        8,
        out_specs=[FREE],
    )(returned, w, share0, share1, resid16, blend, dense_own, dense_came, dense_last)
    return (new_tokens, new_re, new_im)


def solution(mesh):
    in_specs = (
        P("ep", None),
        P(),
        P(None, "tp"),
        P("ep", "tp"),
        P("ep", "tp"),
        P("tp", None),
        P("tp"),
        P("tp", None, None),
        P("tp", None, None),
        P("tp", None, None),
        P("tp", None, None),
        P("tp", None),
        P("tp", None),
        P(),
        P("ep", None),
        P("ep"),
        P("ep", None),
        P("ep", None, "tp"),
        P("ep", None, "tp"),
        P("ep", "tp", None),
        P(None, "tp"),
        P(None, "tp"),
        P("tp", None),
        P(),
    )
    out_specs = (P("ep", "tp"), P("ep", "tp"), P("ep", "tp"))

    return jax.shard_map(
        per_device, mesh=mesh, in_specs=in_specs, out_specs=out_specs, check_vma=False
    )
```

```python
import functools
import math

import jax
import jax.numpy as jnp
from jax import lax
from jax.experimental import pallas as pl
from jax.experimental.pallas import tpu as pltpu
from jax.sharding import PartitionSpec as P


EPS = 1e-06
F32 = jnp.float32
BF16 = jnp.bfloat16
HIGHEST = lax.Precision.HIGHEST
VMEM = pl.BlockSpec(memory_space=pltpu.VMEM)
SMEM = pl.BlockSpec(memory_space=pltpu.SMEM)
ANY = pl.BlockSpec(memory_space=pl.ANY)
HBM = pl.BlockSpec(memory_space=pltpu.HBM)
FREE = pl.BlockSpec(memory_space=pltpu.VMEM)
OUT = pl.BlockSpec()


def iota(shape, dim):
    return lax.broadcasted_iota(jnp.int32, shape, dim)


def nt_dot(a, b, precision=None):
    return lax.dot_general(
        a, b, (((1,), (1,)), ((), ())), precision=precision, preferred_element_type=F32
    )


def dot(a, b, precision=None):
    return jnp.dot(a, b, precision=precision, preferred_element_type=F32)


def cols_of(index, size):
    return pl.ds(pl.multiple_of(index * size, size), size)


def exchanged(value, mask):
    return lax.ppermute(value, "tp", [(i, i ^ mask) for i in range(4)])


def gathered(value):
    across = exchanged(value, 2)
    return [value, exchanged(value, 1), across, exchanged(across, 1)]


def spread_blocks(out, small, channels):
    rows, entries = small.shape
    width = 2 * entries
    tiler = (iota((entries, width), 1) % entries == iota((entries, width), 0)).astype(BF16)
    tiled = dot(small.astype(BF16), tiler)
    mine = iota((rows, width), 0) // channels % 2 == iota((rows, width), 1) // entries
    tiled = jnp.where(mine, tiled, 0.0).astype(BF16)
    out[...] = jnp.zeros(out.shape, BF16)
    for pair in range(rows // (2 * channels)):
        near = slice(2 * channels * pair, 2 * channels * (pair + 1))
        out[near, width * pair : width * (pair + 1)] = tiled[near, :]


def row_of(small):
    groups, n = small.shape
    width = groups * n
    tiler = (iota((n, width), 1) % n == iota((n, width), 0)).astype(F32)
    tiled = dot(small, tiler, HIGHEST)
    mine = iota((groups, width), 0) == iota((groups, width), 1) // n
    return jnp.sum(jnp.where(mine, tiled, 0.0), axis=0, keepdims=True)


def state_kernel(*refs):
    inputs, (own, beside, new_re, new_im), held = refs[0:13], refs[13:17], refs[17:30]
    blocks_v, sems = refs[30:]
    t = lax.axis_index("tp")
    loads = [
        pltpu.make_async_copy(a, b, sems.at[i]) for i, (a, b) in enumerate(zip(inputs, held))
    ]
    for load in loads:
        load.start()
    log_step, decay, skip, b_re, b_im, c_re, c_im, tokens_v, gain, in_v, re_v, im_v, out_v = held
    groups, entries = decay.shape
    channels = skip.shape[1]
    width = groups * entries
    of_group = iota((1, width), 1) // entries
    for load in loads[0:3]:
        load.wait()
    logs = jnp.zeros((1, width), F32)
    for g in range(groups):
        logs = jnp.where(of_group == g, log_step[g], logs)
    step = jnp.exp(logs)
    eigen = row_of(decay[...])
    direct = row_of(skip[...])
    freq = math.pi * (iota((1, width), 1) % entries).astype(F32)
    magnitude = jnp.exp(eigen * step)
    turned = freq * step
    lam_re = magnitude * jnp.cos(turned)
    lam_im = magnitude * jnp.sin(turned)
    denom = eigen * eigen + freq * freq
    fac_re = ((lam_re - 1.0) * eigen + lam_im * freq) / denom
    fac_im = (lam_im * eigen - (lam_re - 1.0) * freq) / denom
    for load in loads[3:7]:
        load.wait()
    for k, small in enumerate((b_re, b_im, c_re, c_im)):
        spread_blocks(blocks_v.at[k], small[...], channels)
    loads[7].wait()
    loads[8].wait()
    x = tokens_v[...].astype(F32)
    scale = lax.rsqrt(jnp.mean(x * x, axis=-1, keepdims=True) + EPS)
    normed = (x * scale * gain[...].astype(F32).reshape(1, -1)).astype(BF16)
    loads[9].wait()
    drive = dot(normed, in_v[...]).astype(BF16)
    in_re = dot(drive, blocks_v[0])
    in_im = dot(drive, blocks_v[1])
    loads[10].wait()
    loads[11].wait()
    was_re, was_im = re_v[...], im_v[...]
    fresh_re = lam_re * was_re - lam_im * was_im + (fac_re * in_re - fac_im * in_im)
    fresh_im = lam_re * was_im + lam_im * was_re + (fac_re * in_im + fac_im * in_re)
    new_re[...] = fresh_re
    new_im[...] = fresh_im
    mixed = (
        nt_dot(fresh_re.astype(BF16), blocks_v[2])
        - nt_dot(fresh_im.astype(BF16), blocks_v[3])
        + direct * drive.astype(F32)
    )
    act = jax.nn.gelu(mixed).astype(BF16)
    loads[12].wait()
    quarter = own.shape[1] // 2
    for m, pair in ((1, beside), (3, beside), (0, own), (2, own)):
        near = pl.ds((m // 2) * quarter, quarter)
        pair[:, near] = dot(act, out_v[:, cols_of(t ^ m, quarter)]).astype(BF16)


def half_kernel(own, came, onward):
    quarter = onward.shape[1]
    onward[...] = (own[:, quarter:].astype(F32) + came[:, quarter:].astype(F32)).astype(BF16)


def reshard_kernel(gate, up, down, *pieces):
    t = lax.axis_index("tp")
    hid = gate.shape[1]
    for m, (wide, deep) in enumerate(zip(pieces[:4], pieces[4:])):
        part = cols_of(t ^ m, wide.shape[0])
        wide[:, 0:hid] = gate[part, :]
        wide[:, hid:] = up[part, :]
        deep[...] = down[:, cols_of(t ^ m, deep.shape[1])]


def route_kernel(experts, routes, group_weight, logits, z, w, share0, share1, padded):
    rows = routes.shape[1]
    slots, lanes = z.shape
    padded[...] = jnp.full(padded.shape, -1, jnp.int32)
    padded[0:2, 0:rows] = routes[...]
    named = [padded[k : k + 1, :] for k in range(2)]
    hot = [(iota((experts, lanes), 0) == r).astype(F32) for r in named]
    earlier = (iota((lanes, lanes), 0) < iota((lanes, lanes), 1)).astype(BF16)
    before = dot((hot[0] + hot[1]).astype(BF16), earlier)
    place = [jnp.sum(before * h, axis=0, keepdims=True).astype(jnp.int32) for h in hot]
    slot = [jnp.where(r >= 0, p * experts + r, -1) for r, p in zip(named, place)]
    at = iota((slots, lanes), 0)
    z[...] = jnp.logical_or(at == slot[0], at == slot[1]).astype(F32).astype(BF16)
    eye = iota((lanes, lanes), 0) == iota((lanes, lanes), 1)
    at = iota((rows, slots), 1)
    for k in range(2):
        column = jnp.sum(jnp.where(eye, slot[k], 0), axis=1, keepdims=True)[0:rows]
        w[k * rows : (k + 1) * rows, :] = (at == column).astype(F32).astype(BF16)
    expo = jnp.exp(logits[...])
    share = group_weight[...] * expo / (expo[0:1] + expo[1:2])
    small_eye = iota((rows, rows), 0) == iota((rows, rows), 1)
    for k, out in enumerate((share0, share1)):
        column = jnp.sum(jnp.where(small_eye, share[k : k + 1], 0.0), axis=1, keepdims=True)
        out[...] = jnp.broadcast_to(column, out.shape)


def places(capacity, wide, quarter):
    blocks = quarter // wide.shape[1]
    peers = wide.shape[0] // (capacity * blocks)
    for s in range(capacity):
        for c in range(blocks):
            yield (
                pl.ds(c * capacity + s, peers, stride=capacity * blocks),
                slice(s * peers, (s + 1) * peers),
                slice(c * wide.shape[1], (c + 1) * wide.shape[1]),
            )


def three_terms(row, size):
    if row.shape[1] < size:
        row = jnp.concatenate([row, jnp.zeros((1, size - row.shape[1]), F32)], axis=1)
    high = row.astype(BF16).astype(F32)
    middle = (row - high).astype(BF16).astype(F32)
    low = row - high - middle
    at = iota((8, size), 0)
    block = jnp.where(at == 0, high, jnp.where(at == 1, middle, jnp.where(at == 2, low, 0.0)))
    return block.astype(BF16)


def sum_terms(block):
    return jnp.sum(block.astype(F32), axis=0, keepdims=True)


def pack_kernel(capacity, tokens, own, came, last, z, resid16, packed, wide):
    t = lax.axis_index("tp")
    quarter = last.shape[1]
    total = tokens[:, cols_of(t, quarter)].astype(F32) + (
        (own[:, 0:quarter].astype(F32) + came[:, 0:quarter].astype(F32)) + last[...].astype(F32)
    )
    short = total.astype(BF16)
    resid16[...] = short
    gap = jnp.zeros((z.shape[1] - short.shape[0], quarter), BF16)
    spread = dot(z[...], jnp.concatenate([short, gap], axis=0))
    for strided, near, cols in places(capacity, wide, quarter):
        wide[strided, :] = spread[near, cols]
    packed[...] = wide[...].astype(BF16)


def dense_kernel(
    gains, a0, a1, a2, a3, blend_weight, gate, up, down, own, beside, blend,
    full, gate_v, up_v, down_v, sems,
):
    t = lax.axis_index("tp")
    loads = [
        pltpu.make_async_copy(a, b, sems.at[i])
        for i, (a, b) in enumerate(((gate, gate_v), (up, up_v), (down, down_v)))
    ]
    for load in loads:
        load.start()
    quarter = a0.shape[1]
    for m, a in enumerate((a0, a1, a2, a3)):
        full[:, cols_of(t ^ m, quarter)] = a[...]
    x = full[...].astype(F32)
    scale = lax.rsqrt(jnp.mean(x * x, axis=-1, keepdims=True) + EPS)
    normed = (x * scale * gains[...].astype(F32)).astype(BF16)
    score = jnp.sum(
        normed.astype(F32) * blend_weight[...].astype(F32), axis=-1, keepdims=True
    )
    blend[...] = jnp.broadcast_to(jax.nn.sigmoid(score), blend.shape)
    loads[0].wait()
    pre_gate = dot(normed, gate_v[...])
    loads[1].wait()
    pre_up = dot(normed, up_v[...])
    hidden = (jax.nn.silu(pre_gate) * pre_up).astype(BF16)
    loads[2].wait()
    for m, pair in ((1, beside), (3, beside), (0, own), (2, own)):
        near = pl.ds((m // 2) * quarter, quarter)
        pair[:, near] = dot(hidden, down_v[:, cols_of(t ^ m, quarter)]).astype(BF16)


def enter_kernel(capacity, arrived, gains, w1, w3, send, rows, squares, wide, sums):
    t = lax.axis_index("tp")
    lanes = arrived.shape[1]
    count, quarter = rows.shape
    wide[...] = arrived[...].astype(F32)
    gain = gains[:, cols_of(t, quarter)].astype(F32)
    for strided, near, cols in places(capacity, wide, quarter):
        x = wide[strided, :]
        sums[near, :] = x * x if cols.start == 0 else sums[near, :] + x * x
        rows[near, cols] = (x * gain[:, cols]).astype(BF16)
    total = nt_dot(jnp.ones((8, lanes), F32), sums[...], HIGHEST)
    squares[...] = total
    send[count:, :] = three_terms(total[0:1], send.shape[1])
    pair = w1.shape[1]
    x = rows[...]
    send[0:count, 0:pair] = dot(x, w1[...]).astype(BF16)
    send[0:count, pair:] = dot(x, w3[...]).astype(BF16)


def stay_kernel(rows, squares, w0, w2, keep):
    count = rows.shape[0]
    gap = jnp.zeros((8, keep.shape[1] - count), F32)
    keep[count:, :] = jnp.concatenate([squares[...], gap], axis=1)
    pair = w0.shape[1]
    x = rows[...]
    keep[0:count, 0:pair] = dot(x, w0[...])
    keep[0:count, pair:] = dot(x, w2[...])


def relay_kernel(keep, came, onward):
    pair = onward.shape[1]
    count = keep.shape[0] - 8
    onward[0:count, :] = (keep[0:count, pair:] + came[0:count, pair:].astype(F32)).astype(BF16)
    squares = keep[count : count + 1, :] + sum_terms(came[count:, :])
    onward[count : count + 8, :] = three_terms(squares[:, 0:pair], pair)
    onward[count + 8 :, :] = three_terms(squares[:, pair:], pair)


def hidden_kernel(width, keep, came, last, hidden):
    count, units = hidden.shape
    pair = 2 * units
    total = (
        keep[0:count, 0:pair] + came[0:count, 0:pair].astype(F32) + last[0:count, :].astype(F32)
    )
    squares = keep[count : count + 1, :] + sum_terms(came[count:, :])
    squares = squares + jnp.concatenate(
        [sum_terms(last[count : count + 8, :]), sum_terms(last[count + 8 :, :])], axis=1
    )
    column = jnp.transpose(jnp.broadcast_to(squares[:, 0:count], (8, count)))[:, 0:1]
    scale = lax.rsqrt(column / width + EPS)
    hidden[...] = (jax.nn.silu(total[:, 0:units] * scale) * (total[:, units:] * scale)).astype(BF16)


def leave_kernel(capacity, h0, h1, h2, h3, w0, w1, w2, w3, out, wide):
    total = (dot(h0[...], w0[...]) + dot(h1[...], w1[...])) + (
        dot(h2[...], w2[...]) + dot(h3[...], w3[...])
    )
    for strided, near, cols in places(capacity, wide, total.shape[1]):
        wide[strided, :] = total[near, cols]
    out[...] = wide[...].astype(BF16)


def final_kernel(
    capacity, returned, w, share0, share1, resid, blend, own, came, last, out, wide, rows
):
    count, quarter = resid.shape
    wide[...] = returned[...].astype(F32)
    for strided, near, cols in places(capacity, wide, quarter):
        rows[near, cols] = wide[strided, :].astype(BF16)
    picked = dot(w[...], rows[...])
    lanes = wide.shape[1]
    for c in range(quarter // lanes):
        cols = slice(c * lanes, (c + 1) * lanes)
        moe = share0[...] * picked[0:count, cols] + share1[...] * picked[count:, cols]
        dense = (own[:, cols].astype(F32) + came[:, cols].astype(F32)) + last[:, cols].astype(F32)
        out[:, cols] = (resid[:, cols].astype(F32) + moe + blend[...] * dense).astype(BF16)


def call(kernel, outs, scratch=(), limit=4, in_specs=None, out_specs=None):
    out_specs = out_specs or [VMEM] * len(outs)
    kinds = {id(VMEM): pltpu.VMEM, id(OUT): pltpu.HBM}
    out_shape = [
        kinds.get(id(spec), jax.ShapeDtypeStruct)(s, d) for (s, d), spec in zip(outs, out_specs)
    ]

    def run(*args):
        specs = in_specs or [VMEM] * len(args)
        spaces = {id(VMEM): pltpu.VMEM, id(HBM): pltpu.HBM}
        fixed = [
            pltpu.with_memory_space_constraint(a, spaces.get(id(spec), pl.ANY))
            for a, spec in zip(args, specs)
        ]
        return pl.pallas_call(
            kernel,
            out_shape=tuple(out_shape),
            in_specs=specs,
            out_specs=tuple(out_specs),
            scratch_shapes=list(scratch),
            compiler_params=pltpu.CompilerParams(vmem_limit_bytes=limit << 20),
        )(*fixed)

    return run


def per_device(
    tokens,
    norm_gain,
    in_weight,
    sequence_state_real,
    sequence_state_imaginary,
    eigen_decay_real,
    log_step,
    input_matrix_real,
    input_matrix_imaginary,
    output_matrix_real,
    output_matrix_imaginary,
    channel_skip_scale,
    out_weight,
    ffn_gain,
    routes,
    group_weight,
    expert_logit,
    expert_gate,
    expert_up,
    expert_down,
    dense_gate,
    dense_up,
    dense_down,
    blend_weight,
):
    rows, width = tokens.shape
    tp = lax.axis_size("tp")
    ep = lax.axis_size("ep")
    quarter = width // tp
    lanes = 128
    blocks = quarter // lanes
    capacity = max(2, 2 * rows * routes.shape[1] // (ep * expert_gate.shape[0]))
    slots = ep * capacity
    groups, entries, channels = input_matrix_real.shape
    hid = expert_gate.shape[2]
    gate = expert_gate.reshape(width, hid)
    up = expert_up.reshape(width, hid)
    down = expert_down.reshape(hid, width)
    piece = ((rows, quarter), BF16)

    def by_channel(matrix):
        return jnp.swapaxes(matrix, 1, 2).reshape(groups * channels, entries)

    states = ((rows, groups * entries), F32)
    state_inputs = (
        log_step,
        eigen_decay_real,
        channel_skip_scale,
        by_channel(input_matrix_real),
        by_channel(input_matrix_imaginary),
        output_matrix_real.reshape(groups * channels, entries),
        output_matrix_imaginary.reshape(groups * channels, entries),
        tokens,
        norm_gain,
        in_weight,
        sequence_state_real,
        sequence_state_imaginary,
        out_weight,
    )
    own, beside, new_re, new_im = call(
        state_kernel,
        [((rows, 2 * quarter), BF16)] * 2 + [states] * 2,
        [pltpu.SMEM(log_step.shape, F32)]
        + [pltpu.VMEM(x.shape, x.dtype) for x in state_inputs[1:]]
        + [pltpu.VMEM((4, groups * channels, groups * entries), BF16)]
        + [pltpu.SemaphoreType.DMA((13,))],
        20,
        [HBM] * 13,
        [VMEM] * 4,
    )(*state_inputs)
    came_mix = exchanged(beside, 1)
    (onward,) = call(half_kernel, [piece])(own, came_mix)
    last_mix = exchanged(onward, 2)
    reshard = call(reshard_kernel, [((quarter, 2 * hid), BF16)] * 4 + [((hid, quarter), BF16)] * 4)
    pieces = reshard(gate, up, down)
    wide2 = exchanged(pieces[2], 2)
    wide3 = exchanged(pieces[3], 3)
    wide1 = exchanged(pieces[1], 1)
    moved = [pieces[0], wide1, wide2, wide3]
    downs = [pieces[4]] + [exchanged(pieces[4 + m], m) for m in (1, 2, 3)]
    z, w, share0, share1 = call(
        functools.partial(route_kernel, ep),
        [((slots, lanes), BF16), ((2 * rows, slots), BF16)] + [((rows, lanes), F32)] * 2,
        [pltpu.VMEM((8, lanes), jnp.int32)],
    )(routes.T, group_weight.reshape(1, rows), expert_logit.T)
    wide = pltpu.VMEM((slots * blocks, lanes), F32)
    resid16, packed = call(
        functools.partial(pack_kernel, capacity),
        [piece, ((slots * blocks, lanes), BF16)],
        [wide],
        8,
        out_specs=[VMEM, FREE],
    )(tokens, own, came_mix, last_mix, z)
    across = exchanged(resid16, 2)
    arrived = lax.all_to_all(
        packed.reshape(ep, capacity * blocks, lanes), "ep", 0, 0, tiled=True
    ).reshape(slots * blocks, lanes)
    near = [resid16, exchanged(resid16, 1), across, exchanged(across, 1)]
    gains = ffn_gain.reshape(1, width)
    send, x_rows, squares = call(
        functools.partial(enter_kernel, capacity),
        [((slots + 8, 4 * hid), BF16), ((slots, quarter), BF16), ((8, slots), F32)],
        [wide, pltpu.VMEM((slots, lanes), F32)],
        8,
    )(arrived, gains, moved[1], moved[3])
    came = exchanged(send, 1)
    (keep,) = call(stay_kernel, [((slots + 8, 4 * hid), F32)])(x_rows, squares, moved[0], moved[2])
    (onward,) = call(relay_kernel, [((slots + 16, 2 * hid), BF16)])(keep, came)
    last = exchanged(onward, 2)
    dense_own, dense_beside, blend = call(
        dense_kernel,
        [((rows, 2 * quarter), BF16)] * 2 + [((rows, lanes), F32)],
        [pltpu.VMEM((rows, width), BF16)]
        + [pltpu.VMEM(x.shape, BF16) for x in (dense_gate, dense_up, dense_down)]
        + [pltpu.SemaphoreType.DMA((3,))],
        12,
        [VMEM] * 6 + [HBM] * 3,
        [OUT] * 3,
    )(gains, *near, blend_weight.reshape(1, width), dense_gate, dense_up, dense_down)
    dense_came = exchanged(dense_beside, 1)
    (dense_onward,) = call(half_kernel, [piece], out_specs=[OUT])(dense_own, dense_came)
    dense_last = exchanged(dense_onward, 2)
    (hidden,) = call(
        functools.partial(hidden_kernel, float(width)), [((slots, hid), BF16)]
    )(keep, came, last)
    hidden = gathered(hidden)
    (sent,) = call(
        functools.partial(leave_kernel, capacity),
        [((slots * blocks, lanes), BF16)],
        [wide],
        8,
        out_specs=[FREE],
    )(*hidden, *downs)
    returned = lax.all_to_all(
        sent.reshape(ep, capacity * blocks, lanes), "ep", 0, 0, tiled=True
    ).reshape(slots * blocks, lanes)
    (new_tokens,) = call(
        functools.partial(final_kernel, capacity),
        [piece],
        [wide, pltpu.VMEM((slots, quarter), BF16)],
        8,
        out_specs=[FREE],
    )(returned, w, share0, share1, resid16, blend, dense_own, dense_came, dense_last)
    return (new_tokens, new_re, new_im)


def solution(mesh):
    in_specs = (
        P("ep", None),
        P(),
        P(None, "tp"),
        P("ep", "tp"),
        P("ep", "tp"),
        P("tp", None),
        P("tp"),
        P("tp", None, None),
        P("tp", None, None),
        P("tp", None, None),
        P("tp", None, None),
        P("tp", None),
        P("tp", None),
        P(),
        P("ep", None),
        P("ep"),
        P("ep", None),
        P("ep", None, "tp"),
        P("ep", None, "tp"),
        P("ep", "tp", None),
        P(None, "tp"),
        P(None, "tp"),
        P("tp", None),
        P(),
    )
    out_specs = (P("ep", "tp"), P("ep", "tp"), P("ep", "tp"))

    return jax.shard_map(
        per_device, mesh=mesh, in_specs=in_specs, out_specs=out_specs, check_vma=False
    )
```

```python
import functools
import math

import jax
import jax.numpy as jnp
from jax import lax
from jax.experimental import pallas as pl
from jax.experimental.pallas import tpu as pltpu
from jax.sharding import PartitionSpec as P


EPS = 1e-06
F32 = jnp.float32
BF16 = jnp.bfloat16
HIGHEST = lax.Precision.HIGHEST
VMEM = pl.BlockSpec(memory_space=pltpu.VMEM)
SMEM = pl.BlockSpec(memory_space=pltpu.SMEM)
ANY = pl.BlockSpec(memory_space=pl.ANY)
HBM = pl.BlockSpec(memory_space=pltpu.HBM)
FREE = pl.BlockSpec(memory_space=pltpu.VMEM)
OUT = pl.BlockSpec()


def iota(shape, dim):
    return lax.broadcasted_iota(jnp.int32, shape, dim)


def nt_dot(a, b, precision=None):
    return lax.dot_general(
        a, b, (((1,), (1,)), ((), ())), precision=precision, preferred_element_type=F32
    )


def dot(a, b, precision=None):
    return jnp.dot(a, b, precision=precision, preferred_element_type=F32)


def cols_of(index, size):
    return pl.ds(pl.multiple_of(index * size, size), size)


def exchanged(value, mask):
    return lax.ppermute(value, "tp", [(i, i ^ mask) for i in range(4)])


def spread_blocks(out, small, channels):
    rows, entries = small.shape
    width = 2 * entries
    tiler = (iota((entries, width), 1) % entries == iota((entries, width), 0)).astype(BF16)
    tiled = dot(small.astype(BF16), tiler)
    mine = iota((rows, width), 0) // channels % 2 == iota((rows, width), 1) // entries
    tiled = jnp.where(mine, tiled, 0.0).astype(BF16)
    out[...] = jnp.zeros(out.shape, BF16)
    for pair in range(rows // (2 * channels)):
        near = slice(2 * channels * pair, 2 * channels * (pair + 1))
        out[near, width * pair : width * (pair + 1)] = tiled[near, :]


def row_of(small):
    groups, n = small.shape
    width = groups * n
    tiler = (iota((n, width), 1) % n == iota((n, width), 0)).astype(F32)
    tiled = dot(small, tiler, HIGHEST)
    mine = iota((groups, width), 0) == iota((groups, width), 1) // n
    return jnp.sum(jnp.where(mine, tiled, 0.0), axis=0, keepdims=True)


def state_kernel(*refs):
    inputs, (own, beside, new_re, new_im), held = refs[0:13], refs[13:17], refs[17:30]
    blocks_v, sems = refs[30:]
    t = lax.axis_index("tp")
    loads = [
        pltpu.make_async_copy(a, b, sems.at[i]) for i, (a, b) in enumerate(zip(inputs, held))
    ]
    for load in loads:
        load.start()
    log_step, decay, skip, tokens_v, gain, b_re, b_im, in_v, re_v, im_v, c_re, c_im, out_v = held
    groups, entries = decay.shape
    channels = skip.shape[1]
    width = groups * entries
    of_group = iota((1, width), 1) // entries
    for load in loads[0:3]:
        load.wait()
    logs = jnp.zeros((1, width), F32)
    for g in range(groups):
        logs = jnp.where(of_group == g, log_step[g], logs)
    step = jnp.exp(logs)
    eigen = row_of(decay[...])
    direct = row_of(skip[...])
    freq = math.pi * (iota((1, width), 1) % entries).astype(F32)
    magnitude = jnp.exp(eigen * step)
    turned = freq * step
    lam_re = magnitude * jnp.cos(turned)
    lam_im = magnitude * jnp.sin(turned)
    denom = eigen * eigen + freq * freq
    fac_re = ((lam_re - 1.0) * eigen + lam_im * freq) / denom
    fac_im = (lam_im * eigen - (lam_re - 1.0) * freq) / denom
    for load in loads[3:5]:
        load.wait()
    x = tokens_v[...].astype(F32)
    scale = lax.rsqrt(jnp.mean(x * x, axis=-1, keepdims=True) + EPS)
    normed = (x * scale * gain[...].astype(F32).reshape(1, -1)).astype(BF16)
    for load in loads[5:7]:
        load.wait()
    spread_blocks(blocks_v.at[0], b_re[...], channels)
    spread_blocks(blocks_v.at[1], b_im[...], channels)
    loads[7].wait()
    drive = dot(normed, in_v[...]).astype(BF16)
    in_re = dot(drive, blocks_v[0])
    in_im = dot(drive, blocks_v[1])
    for load in loads[8:12]:
        load.wait()
    spread_blocks(blocks_v.at[2], c_re[...], channels)
    spread_blocks(blocks_v.at[3], c_im[...], channels)
    was_re, was_im = re_v[...], im_v[...]
    fresh_re = lam_re * was_re - lam_im * was_im + (fac_re * in_re - fac_im * in_im)
    fresh_im = lam_re * was_im + lam_im * was_re + (fac_re * in_im + fac_im * in_re)
    new_re[...] = fresh_re
    new_im[...] = fresh_im
    mixed = (
        nt_dot(fresh_re.astype(BF16), blocks_v[2])
        - nt_dot(fresh_im.astype(BF16), blocks_v[3])
        + direct * drive.astype(F32)
    )
    act = jax.nn.gelu(mixed).astype(BF16)
    loads[12].wait()
    quarter = own.shape[1] // 2
    for m, pair in ((1, beside), (3, beside), (0, own), (2, own)):
        near = pl.ds((m // 2) * quarter, quarter)
        pair[:, near] = dot(act, out_v[:, cols_of(t ^ m, quarter)]).astype(BF16)


def half_kernel(own, came, onward):
    quarter = onward.shape[1]
    onward[...] = (own[:, quarter:].astype(F32) + came[:, quarter:].astype(F32)).astype(BF16)


def reshard_kernel(gate, up, down, *pieces):
    t = lax.axis_index("tp")
    hid = gate.shape[1]
    for m, (wide, deep) in enumerate(zip(pieces[:4], pieces[4:])):
        part = cols_of(t ^ m, wide.shape[0])
        wide[:, 0:hid] = gate[part, :]
        wide[:, hid:] = up[part, :]
        deep[...] = down[:, cols_of(t ^ m, deep.shape[1])]


def route_kernel(experts, routes, group_weight, logits, z, w, share0, share1, padded):
    rows = routes.shape[1]
    slots, lanes = z.shape
    padded[...] = jnp.full(padded.shape, -1, jnp.int32)
    padded[0:2, 0:rows] = routes[...]
    named = [padded[k : k + 1, :] for k in range(2)]
    hot = [(iota((experts, lanes), 0) == r).astype(F32) for r in named]
    earlier = (iota((lanes, lanes), 0) < iota((lanes, lanes), 1)).astype(BF16)
    before = dot((hot[0] + hot[1]).astype(BF16), earlier)
    place = [jnp.sum(before * h, axis=0, keepdims=True).astype(jnp.int32) for h in hot]
    slot = [jnp.where(r >= 0, p * experts + r, -1) for r, p in zip(named, place)]
    at = iota((slots, lanes), 0)
    z[...] = jnp.logical_or(at == slot[0], at == slot[1]).astype(F32).astype(BF16)
    eye = iota((lanes, lanes), 0) == iota((lanes, lanes), 1)
    at = iota((rows, slots), 1)
    for k in range(2):
        column = jnp.sum(jnp.where(eye, slot[k], 0), axis=1, keepdims=True)[0:rows]
        w[k * rows : (k + 1) * rows, :] = (at == column).astype(F32).astype(BF16)
    expo = jnp.exp(logits[...])
    share = group_weight[...] * expo / (expo[0:1] + expo[1:2])
    small_eye = iota((rows, rows), 0) == iota((rows, rows), 1)
    for k, out in enumerate((share0, share1)):
        column = jnp.sum(jnp.where(small_eye, share[k : k + 1], 0.0), axis=1, keepdims=True)
        out[...] = jnp.broadcast_to(column, out.shape)


def places(capacity, wide, quarter):
    blocks = quarter // wide.shape[1]
    peers = wide.shape[0] // (capacity * blocks)
    for s in range(capacity):
        for c in range(blocks):
            yield (
                pl.ds(c * capacity + s, peers, stride=capacity * blocks),
                slice(s * peers, (s + 1) * peers),
                slice(c * wide.shape[1], (c + 1) * wide.shape[1]),
            )


def three_terms(row, size):
    if row.shape[1] < size:
        row = jnp.concatenate([row, jnp.zeros((1, size - row.shape[1]), F32)], axis=1)
    high = row.astype(BF16).astype(F32)
    middle = (row - high).astype(BF16).astype(F32)
    low = row - high - middle
    at = iota((8, size), 0)
    block = jnp.where(at == 0, high, jnp.where(at == 1, middle, jnp.where(at == 2, low, 0.0)))
    return block.astype(BF16)


def sum_terms(block):
    return jnp.sum(block.astype(F32), axis=0, keepdims=True)


def pack_kernel(capacity, tokens, own, came, last, z, resid16, packed, wide):
    t = lax.axis_index("tp")
    quarter = last.shape[1]
    total = tokens[:, cols_of(t, quarter)].astype(F32) + (
        (own[:, 0:quarter].astype(F32) + came[:, 0:quarter].astype(F32)) + last[...].astype(F32)
    )
    short = total.astype(BF16)
    resid16[...] = short
    gap = jnp.zeros((z.shape[1] - short.shape[0], quarter), BF16)
    spread = dot(z[...], jnp.concatenate([short, gap], axis=0))
    for strided, near, cols in places(capacity, wide, quarter):
        wide[strided, :] = spread[near, cols]
    packed[...] = wide[...].astype(BF16)


def dense_kernel(
    gains, a0, a1, a2, a3, blend_weight, gate, up, down, own, beside, blend,
    full, gate_v, up_v, down_v, sems,
):
    t = lax.axis_index("tp")
    loads = [
        pltpu.make_async_copy(a, b, sems.at[i])
        for i, (a, b) in enumerate(((gate, gate_v), (up, up_v), (down, down_v)))
    ]
    for load in loads:
        load.start()
    quarter = a0.shape[1]
    for m, a in enumerate((a0, a1, a2, a3)):
        full[:, cols_of(t ^ m, quarter)] = a[...]
    x = full[...].astype(F32)
    scale = lax.rsqrt(jnp.mean(x * x, axis=-1, keepdims=True) + EPS)
    normed = (x * scale * gains[...].astype(F32)).astype(BF16)
    score = jnp.sum(
        normed.astype(F32) * blend_weight[...].astype(F32), axis=-1, keepdims=True
    )
    blend[...] = jnp.broadcast_to(jax.nn.sigmoid(score), blend.shape)
    loads[0].wait()
    pre_gate = dot(normed, gate_v[...])
    loads[1].wait()
    pre_up = dot(normed, up_v[...])
    hidden = (jax.nn.silu(pre_gate) * pre_up).astype(BF16)
    loads[2].wait()
    for m, pair in ((1, beside), (3, beside), (0, own), (2, own)):
        near = pl.ds((m // 2) * quarter, quarter)
        pair[:, near] = dot(hidden, down_v[:, cols_of(t ^ m, quarter)]).astype(BF16)


def enter_kernel(capacity, arrived, gains, w1, w3, send, rows, squares, wide, sums):
    t = lax.axis_index("tp")
    lanes = arrived.shape[1]
    count, quarter = rows.shape
    wide[...] = arrived[...].astype(F32)
    gain = gains[:, cols_of(t, quarter)].astype(F32)
    for strided, near, cols in places(capacity, wide, quarter):
        x = wide[strided, :]
        sums[near, :] = x * x if cols.start == 0 else sums[near, :] + x * x
        rows[near, cols] = (x * gain[:, cols]).astype(BF16)
    total = nt_dot(jnp.ones((8, lanes), F32), sums[...], HIGHEST)
    squares[...] = total
    send[count:, :] = three_terms(total[0:1], send.shape[1])
    pair = w1.shape[1]
    x = rows[...]
    send[0:count, 0:pair] = dot(x, w1[...]).astype(BF16)
    send[0:count, pair:] = dot(x, w3[...]).astype(BF16)


def stay_kernel(rows, squares, w0, w2, keep):
    count = rows.shape[0]
    gap = jnp.zeros((8, keep.shape[1] - count), F32)
    keep[count:, :] = jnp.concatenate([squares[...], gap], axis=1)
    pair = w0.shape[1]
    x = rows[...]
    keep[0:count, 0:pair] = dot(x, w0[...])
    keep[0:count, pair:] = dot(x, w2[...])


def relay_kernel(keep, came, onward):
    pair = onward.shape[1]
    count = keep.shape[0] - 8
    onward[0:count, :] = (keep[0:count, pair:] + came[0:count, pair:].astype(F32)).astype(BF16)
    squares = keep[count : count + 1, :] + sum_terms(came[count:, :])
    onward[count : count + 8, :] = three_terms(squares[:, 0:pair], pair)
    onward[count + 8 :, :] = three_terms(squares[:, pair:], pair)


def hidden_kernel(width, keep, came, last, hidden):
    count, units = hidden.shape
    pair = 2 * units
    total = (
        keep[0:count, 0:pair] + came[0:count, 0:pair].astype(F32) + last[0:count, :].astype(F32)
    )
    squares = keep[count : count + 1, :] + sum_terms(came[count:, :])
    squares = squares + jnp.concatenate(
        [sum_terms(last[count : count + 8, :]), sum_terms(last[count + 8 :, :])], axis=1
    )
    column = jnp.transpose(jnp.broadcast_to(squares[:, 0:count], (8, count)))[:, 0:1]
    scale = lax.rsqrt(column / width + EPS)
    hidden[...] = (jax.nn.silu(total[:, 0:units] * scale) * (total[:, units:] * scale)).astype(BF16)


def leave_kernel(capacity, h0, h1, h2, h3, w0, w1, w2, w3, out, wide):
    total = (dot(h0[...], w0[...]) + dot(h1[...], w1[...])) + (
        dot(h2[...], w2[...]) + dot(h3[...], w3[...])
    )
    for strided, near, cols in places(capacity, wide, total.shape[1]):
        wide[strided, :] = total[near, cols]
    out[...] = wide[...].astype(BF16)


def final_kernel(
    capacity, returned, w, share0, share1, resid, blend, own, came, last, out, wide, rows
):
    count, quarter = resid.shape
    wide[...] = returned[...].astype(F32)
    for strided, near, cols in places(capacity, wide, quarter):
        rows[near, cols] = wide[strided, :].astype(BF16)
    picked = dot(w[...], rows[...])
    lanes = wide.shape[1]
    for c in range(quarter // lanes):
        cols = slice(c * lanes, (c + 1) * lanes)
        moe = share0[...] * picked[0:count, cols] + share1[...] * picked[count:, cols]
        dense = (own[:, cols].astype(F32) + came[:, cols].astype(F32)) + last[:, cols].astype(F32)
        out[:, cols] = (resid[:, cols].astype(F32) + moe + blend[...] * dense).astype(BF16)


def call(kernel, outs, scratch=(), limit=4, in_specs=None, out_specs=None):
    out_specs = out_specs or [VMEM] * len(outs)
    kinds = {id(VMEM): pltpu.VMEM, id(OUT): pltpu.HBM}
    out_shape = [
        kinds.get(id(spec), jax.ShapeDtypeStruct)(s, d) for (s, d), spec in zip(outs, out_specs)
    ]

    def run(*args):
        specs = in_specs or [VMEM] * len(args)
        spaces = {id(VMEM): pltpu.VMEM, id(HBM): pltpu.HBM}
        fixed = [
            pltpu.with_memory_space_constraint(a, spaces.get(id(spec), pl.ANY))
            for a, spec in zip(args, specs)
        ]
        return pl.pallas_call(
            kernel,
            out_shape=tuple(out_shape),
            in_specs=specs,
            out_specs=tuple(out_specs),
            scratch_shapes=list(scratch),
            compiler_params=pltpu.CompilerParams(vmem_limit_bytes=limit << 20),
        )(*fixed)

    return run


def per_device(
    tokens,
    norm_gain,
    in_weight,
    sequence_state_real,
    sequence_state_imaginary,
    eigen_decay_real,
    log_step,
    input_matrix_real,
    input_matrix_imaginary,
    output_matrix_real,
    output_matrix_imaginary,
    channel_skip_scale,
    out_weight,
    ffn_gain,
    routes,
    group_weight,
    expert_logit,
    expert_gate,
    expert_up,
    expert_down,
    dense_gate,
    dense_up,
    dense_down,
    blend_weight,
):
    rows, width = tokens.shape
    tp = lax.axis_size("tp")
    ep = lax.axis_size("ep")
    quarter = width // tp
    lanes = 128
    blocks = quarter // lanes
    capacity = max(2, 2 * rows * routes.shape[1] // (ep * expert_gate.shape[0]))
    slots = ep * capacity
    groups, entries, channels = input_matrix_real.shape
    hid = expert_gate.shape[2]
    gate = expert_gate.reshape(width, hid)
    up = expert_up.reshape(width, hid)
    down = expert_down.reshape(hid, width)
    piece = ((rows, quarter), BF16)

    def by_channel(matrix):
        return jnp.swapaxes(matrix, 1, 2).reshape(groups * channels, entries)

    states = ((rows, groups * entries), F32)
    state_inputs = (
        log_step,
        eigen_decay_real,
        channel_skip_scale,
        tokens,
        norm_gain,
        by_channel(input_matrix_real),
        by_channel(input_matrix_imaginary),
        in_weight,
        sequence_state_real,
        sequence_state_imaginary,
        output_matrix_real.reshape(groups * channels, entries),
        output_matrix_imaginary.reshape(groups * channels, entries),
        out_weight,
    )
    own, beside, new_re, new_im = call(
        state_kernel,
        [((rows, 2 * quarter), BF16)] * 2 + [states] * 2,
        [pltpu.SMEM(log_step.shape, F32)]
        + [pltpu.VMEM(x.shape, x.dtype) for x in state_inputs[1:]]
        + [pltpu.VMEM((4, groups * channels, groups * entries), BF16)]
        + [pltpu.SemaphoreType.DMA((13,))],
        20,
        [HBM] * 13,
        [VMEM] * 4,
    )(*state_inputs)
    came_mix = exchanged(beside, 1)
    z, w, share0, share1 = call(
        functools.partial(route_kernel, ep),
        [((slots, lanes), BF16), ((2 * rows, slots), BF16)] + [((rows, lanes), F32)] * 2,
        [pltpu.VMEM((8, lanes), jnp.int32)],
    )(routes.T, group_weight.reshape(1, rows), expert_logit.T)
    wide = pltpu.VMEM((slots * blocks, lanes), F32)
    (onward,) = call(half_kernel, [piece])(own, came_mix)
    last_mix = exchanged(onward, 2)
    reshard = call(reshard_kernel, [((quarter, 2 * hid), BF16)] * 4 + [((hid, quarter), BF16)] * 4)
    pieces = reshard(gate, up, down)
    wide2 = exchanged(pieces[2], 2)
    wide3 = exchanged(pieces[3], 3)
    wide1 = exchanged(pieces[1], 1)
    moved = [pieces[0], wide1, wide2, wide3]
    downs = [pieces[4]] + [exchanged(pieces[4 + m], m) for m in (1, 2, 3)]
    resid16, packed = call(
        functools.partial(pack_kernel, capacity),
        [piece, ((slots * blocks, lanes), BF16)],
        [wide],
        8,
        out_specs=[VMEM, FREE],
    )(tokens, own, came_mix, last_mix, z)
    across = exchanged(resid16, 2)
    arrived = lax.all_to_all(
        packed.reshape(ep, capacity * blocks, lanes), "ep", 0, 0, tiled=True
    ).reshape(slots * blocks, lanes)
    near = [resid16, exchanged(resid16, 1), across, exchanged(across, 1)]
    gains = ffn_gain.reshape(1, width)
    send, x_rows, squares = call(
        functools.partial(enter_kernel, capacity),
        [((slots + 8, 4 * hid), BF16), ((slots, quarter), BF16), ((8, slots), F32)],
        [wide, pltpu.VMEM((slots, lanes), F32)],
        8,
    )(arrived, gains, moved[1], moved[3])
    came = exchanged(send, 1)
    (keep,) = call(stay_kernel, [((slots + 8, 4 * hid), F32)])(x_rows, squares, moved[0], moved[2])
    (onward,) = call(relay_kernel, [((slots + 16, 2 * hid), BF16)])(keep, came)
    last = exchanged(onward, 2)
    dense_own, dense_beside, blend = call(
        dense_kernel,
        [((rows, 2 * quarter), BF16)] * 2 + [((rows, lanes), F32)],
        [pltpu.VMEM((rows, width), BF16)]
        + [pltpu.VMEM(x.shape, BF16) for x in (dense_gate, dense_up, dense_down)]
        + [pltpu.SemaphoreType.DMA((3,))],
        12,
        [VMEM] * 6 + [HBM] * 3,
        [OUT] * 3,
    )(gains, *near, blend_weight.reshape(1, width), dense_gate, dense_up, dense_down)
    dense_came = exchanged(dense_beside, 1)
    (dense_onward,) = call(half_kernel, [piece])(dense_own, dense_came)
    dense_last = exchanged(dense_onward, 2)
    (hidden,) = call(
        functools.partial(hidden_kernel, float(width)), [((slots, hid), BF16)]
    )(keep, came, last)
    unit_across, unit_beside = exchanged(hidden, 2), exchanged(hidden, 1)
    hidden = [hidden, unit_beside, unit_across, exchanged(unit_across, 1)]
    (sent,) = call(
        functools.partial(leave_kernel, capacity),
        [((slots * blocks, lanes), BF16)],
        [wide],
        8,
        out_specs=[FREE],
    )(*hidden, *downs)
    returned = lax.all_to_all(
        sent.reshape(ep, capacity * blocks, lanes), "ep", 0, 0, tiled=True
    ).reshape(slots * blocks, lanes)
    (new_tokens,) = call(
        functools.partial(final_kernel, capacity),
        [piece],
        [wide, pltpu.VMEM((slots, quarter), BF16)],
        8,
        out_specs=[FREE],
    )(returned, w, share0, share1, resid16, blend, dense_own, dense_came, dense_last)
    return (new_tokens, new_re, new_im)


def solution(mesh):
    in_specs = (
        P("ep", None),
        P(),
        P(None, "tp"),
        P("ep", "tp"),
        P("ep", "tp"),
        P("tp", None),
        P("tp"),
        P("tp", None, None),
        P("tp", None, None),
        P("tp", None, None),
        P("tp", None, None),
        P("tp", None),
        P("tp", None),
        P(),
        P("ep", None),
        P("ep"),
        P("ep", None),
        P("ep", None, "tp"),
        P("ep", None, "tp"),
        P("ep", "tp", None),
        P(None, "tp"),
        P(None, "tp"),
        P("tp", None),
        P(),
    )
    out_specs = (P("ep", "tp"), P("ep", "tp"), P("ep", "tp"))

    return jax.shard_map(
        per_device, mesh=mesh, in_specs=in_specs, out_specs=out_specs, check_vma=False
    )
```

```python
import functools
import math

import jax
import jax.numpy as jnp
from jax import lax
from jax.experimental import pallas as pl
from jax.experimental.pallas import tpu as pltpu
from jax.sharding import PartitionSpec as P


EPS = 1e-06
F32 = jnp.float32
BF16 = jnp.bfloat16
HIGHEST = lax.Precision.HIGHEST
VMEM = pl.BlockSpec(memory_space=pltpu.VMEM)
SMEM = pl.BlockSpec(memory_space=pltpu.SMEM)
ANY = pl.BlockSpec(memory_space=pl.ANY)
HBM = pl.BlockSpec(memory_space=pltpu.HBM)
FREE = pl.BlockSpec(memory_space=pltpu.VMEM)
OUT = pl.BlockSpec()


def iota(shape, dim):
    return lax.broadcasted_iota(jnp.int32, shape, dim)


def nt_dot(a, b, precision=None):
    return lax.dot_general(
        a, b, (((1,), (1,)), ((), ())), precision=precision, preferred_element_type=F32
    )


def dot(a, b, precision=None):
    return jnp.dot(a, b, precision=precision, preferred_element_type=F32)


def cols_of(index, size):
    return pl.ds(pl.multiple_of(index * size, size), size)


def exchanged(value, mask):
    return lax.ppermute(value, "tp", [(i, i ^ mask) for i in range(4)])


def gathered(value):
    across = exchanged(value, 2)
    return [value, exchanged(value, 1), across, exchanged(across, 1)]


def spread_blocks(out, small, channels):
    rows, entries = small.shape
    width = 2 * entries
    tiler = (iota((entries, width), 1) % entries == iota((entries, width), 0)).astype(BF16)
    tiled = dot(small.astype(BF16), tiler)
    mine = iota((rows, width), 0) // channels % 2 == iota((rows, width), 1) // entries
    tiled = jnp.where(mine, tiled, 0.0).astype(BF16)
    out[...] = jnp.zeros(out.shape, BF16)
    for pair in range(rows // (2 * channels)):
        near = slice(2 * channels * pair, 2 * channels * (pair + 1))
        out[near, width * pair : width * (pair + 1)] = tiled[near, :]


def row_of(small):
    groups, n = small.shape
    width = groups * n
    tiler = (iota((n, width), 1) % n == iota((n, width), 0)).astype(F32)
    tiled = dot(small, tiler, HIGHEST)
    mine = iota((groups, width), 0) == iota((groups, width), 1) // n
    return jnp.sum(jnp.where(mine, tiled, 0.0), axis=0, keepdims=True)


def state_kernel(*refs):
    inputs, (own, beside, new_re, new_im), held = refs[0:13], refs[13:17], refs[17:30]
    blocks_v, sems = refs[30:]
    t = lax.axis_index("tp")
    loads = [
        pltpu.make_async_copy(a, b, sems.at[i]) for i, (a, b) in enumerate(zip(inputs, held))
    ]
    for load in loads:
        load.start()
    log_step, decay, skip, tokens_v, gain, b_re, b_im, in_v, re_v, im_v, c_re, c_im, out_v = held
    groups, entries = decay.shape
    channels = skip.shape[1]
    width = groups * entries
    of_group = iota((1, width), 1) // entries
    for load in loads[0:3]:
        load.wait()
    logs = jnp.zeros((1, width), F32)
    for g in range(groups):
        logs = jnp.where(of_group == g, log_step[g], logs)
    step = jnp.exp(logs)
    eigen = row_of(decay[...])
    direct = row_of(skip[...])
    freq = math.pi * (iota((1, width), 1) % entries).astype(F32)
    magnitude = jnp.exp(eigen * step)
    turned = freq * step
    lam_re = magnitude * jnp.cos(turned)
    lam_im = magnitude * jnp.sin(turned)
    denom = eigen * eigen + freq * freq
    fac_re = ((lam_re - 1.0) * eigen + lam_im * freq) / denom
    fac_im = (lam_im * eigen - (lam_re - 1.0) * freq) / denom
    for load in loads[3:5]:
        load.wait()
    x = tokens_v[...].astype(F32)
    scale = lax.rsqrt(jnp.mean(x * x, axis=-1, keepdims=True) + EPS)
    normed = (x * scale * gain[...].astype(F32).reshape(1, -1)).astype(BF16)
    for load in loads[5:7]:
        load.wait()
    spread_blocks(blocks_v.at[0], b_re[...], channels)
    spread_blocks(blocks_v.at[1], b_im[...], channels)
    loads[7].wait()
    drive = dot(normed, in_v[...]).astype(BF16)
    in_re = dot(drive, blocks_v[0])
    in_im = dot(drive, blocks_v[1])
    for load in loads[8:12]:
        load.wait()
    spread_blocks(blocks_v.at[2], c_re[...], channels)
    spread_blocks(blocks_v.at[3], c_im[...], channels)
    was_re, was_im = re_v[...], im_v[...]
    fresh_re = lam_re * was_re - lam_im * was_im + (fac_re * in_re - fac_im * in_im)
    fresh_im = lam_re * was_im + lam_im * was_re + (fac_re * in_im + fac_im * in_re)
    new_re[...] = fresh_re
    new_im[...] = fresh_im
    mixed = (
        nt_dot(fresh_re.astype(BF16), blocks_v[2])
        - nt_dot(fresh_im.astype(BF16), blocks_v[3])
        + direct * drive.astype(F32)
    )
    act = jax.nn.gelu(mixed).astype(BF16)
    loads[12].wait()
    quarter = own.shape[1] // 2
    for m, pair in ((1, beside), (3, beside), (0, own), (2, own)):
        near = pl.ds((m // 2) * quarter, quarter)
        pair[:, near] = dot(act, out_v[:, cols_of(t ^ m, quarter)]).astype(BF16)


def half_kernel(own, came, onward):
    quarter = onward.shape[1]
    onward[...] = (own[:, quarter:].astype(F32) + came[:, quarter:].astype(F32)).astype(BF16)


def reshard_kernel(gate, up, down, *pieces):
    t = lax.axis_index("tp")
    hid = gate.shape[1]
    for m, (wide, deep) in enumerate(zip(pieces[:4], pieces[4:])):
        part = cols_of(t ^ m, wide.shape[0])
        wide[:, 0:hid] = gate[part, :]
        wide[:, hid:] = up[part, :]
        deep[...] = down[:, cols_of(t ^ m, deep.shape[1])]


def route_kernel(experts, routes, group_weight, logits, z, w, share0, share1, padded):
    rows = routes.shape[1]
    slots, lanes = z.shape
    padded[...] = jnp.full(padded.shape, -1, jnp.int32)
    padded[0:2, 0:rows] = routes[...]
    named = [padded[k : k + 1, :] for k in range(2)]
    hot = [(iota((experts, lanes), 0) == r).astype(F32) for r in named]
    earlier = (iota((lanes, lanes), 0) < iota((lanes, lanes), 1)).astype(BF16)
    before = dot((hot[0] + hot[1]).astype(BF16), earlier)
    place = [jnp.sum(before * h, axis=0, keepdims=True).astype(jnp.int32) for h in hot]
    slot = [jnp.where(r >= 0, p * experts + r, -1) for r, p in zip(named, place)]
    at = iota((slots, lanes), 0)
    z[...] = jnp.logical_or(at == slot[0], at == slot[1]).astype(F32).astype(BF16)
    eye = iota((lanes, lanes), 0) == iota((lanes, lanes), 1)
    at = iota((rows, slots), 1)
    for k in range(2):
        column = jnp.sum(jnp.where(eye, slot[k], 0), axis=1, keepdims=True)[0:rows]
        w[k * rows : (k + 1) * rows, :] = (at == column).astype(F32).astype(BF16)
    expo = jnp.exp(logits[...])
    share = group_weight[...] * expo / (expo[0:1] + expo[1:2])
    small_eye = iota((rows, rows), 0) == iota((rows, rows), 1)
    for k, out in enumerate((share0, share1)):
        column = jnp.sum(jnp.where(small_eye, share[k : k + 1], 0.0), axis=1, keepdims=True)
        out[...] = jnp.broadcast_to(column, out.shape)


def places(capacity, wide, quarter):
    blocks = quarter // wide.shape[1]
    peers = wide.shape[0] // (capacity * blocks)
    for s in range(capacity):
        for c in range(blocks):
            yield (
                pl.ds(c * capacity + s, peers, stride=capacity * blocks),
                slice(s * peers, (s + 1) * peers),
                slice(c * wide.shape[1], (c + 1) * wide.shape[1]),
            )


def three_terms(row, size):
    if row.shape[1] < size:
        row = jnp.concatenate([row, jnp.zeros((1, size - row.shape[1]), F32)], axis=1)
    high = row.astype(BF16).astype(F32)
    middle = (row - high).astype(BF16).astype(F32)
    low = row - high - middle
    at = iota((8, size), 0)
    block = jnp.where(at == 0, high, jnp.where(at == 1, middle, jnp.where(at == 2, low, 0.0)))
    return block.astype(BF16)


def sum_terms(block):
    return jnp.sum(block.astype(F32), axis=0, keepdims=True)


def pack_kernel(capacity, tokens, own, came, last, z, resid16, packed, wide):
    t = lax.axis_index("tp")
    quarter = last.shape[1]
    total = tokens[:, cols_of(t, quarter)].astype(F32) + (
        (own[:, 0:quarter].astype(F32) + came[:, 0:quarter].astype(F32)) + last[...].astype(F32)
    )
    short = total.astype(BF16)
    resid16[...] = short
    gap = jnp.zeros((z.shape[1] - short.shape[0], quarter), BF16)
    spread = dot(z[...], jnp.concatenate([short, gap], axis=0))
    for strided, near, cols in places(capacity, wide, quarter):
        wide[strided, :] = spread[near, cols]
    packed[...] = wide[...].astype(BF16)


def dense_kernel(
    gains, a0, a1, a2, a3, blend_weight, gate, up, down, own, beside, blend,
    full, gate_v, up_v, down_v, sems,
):
    t = lax.axis_index("tp")
    loads = [
        pltpu.make_async_copy(a, b, sems.at[i])
        for i, (a, b) in enumerate(((gate, gate_v), (up, up_v), (down, down_v)))
    ]
    for load in loads:
        load.start()
    quarter = a0.shape[1]
    for m, a in enumerate((a0, a1, a2, a3)):
        full[:, cols_of(t ^ m, quarter)] = a[...]
    x = full[...].astype(F32)
    scale = lax.rsqrt(jnp.mean(x * x, axis=-1, keepdims=True) + EPS)
    normed = (x * scale * gains[...].astype(F32)).astype(BF16)
    score = jnp.sum(
        normed.astype(F32) * blend_weight[...].astype(F32), axis=-1, keepdims=True
    )
    blend[...] = jnp.broadcast_to(jax.nn.sigmoid(score), blend.shape)
    loads[0].wait()
    pre_gate = dot(normed, gate_v[...])
    loads[1].wait()
    pre_up = dot(normed, up_v[...])
    hidden = (jax.nn.silu(pre_gate) * pre_up).astype(BF16)
    loads[2].wait()
    for m, pair in ((1, beside), (3, beside), (0, own), (2, own)):
        near = pl.ds((m // 2) * quarter, quarter)
        pair[:, near] = dot(hidden, down_v[:, cols_of(t ^ m, quarter)]).astype(BF16)


def enter_kernel(capacity, arrived, gains, w1, w3, send, rows, squares, wide, sums):
    t = lax.axis_index("tp")
    lanes = arrived.shape[1]
    count, quarter = rows.shape
    wide[...] = arrived[...].astype(F32)
    gain = gains[:, cols_of(t, quarter)].astype(F32)
    for strided, near, cols in places(capacity, wide, quarter):
        x = wide[strided, :]
        sums[near, :] = x * x if cols.start == 0 else sums[near, :] + x * x
        rows[near, cols] = (x * gain[:, cols]).astype(BF16)
    total = nt_dot(jnp.ones((8, lanes), F32), sums[...], HIGHEST)
    squares[...] = total
    send[count:, :] = three_terms(total[0:1], send.shape[1])
    pair = w1.shape[1]
    x = rows[...]
    send[0:count, 0:pair] = dot(x, w1[...]).astype(BF16)
    send[0:count, pair:] = dot(x, w3[...]).astype(BF16)


def stay_kernel(rows, squares, w0, w2, keep):
    count = rows.shape[0]
    gap = jnp.zeros((8, keep.shape[1] - count), F32)
    keep[count:, :] = jnp.concatenate([squares[...], gap], axis=1)
    pair = w0.shape[1]
    x = rows[...]
    keep[0:count, 0:pair] = dot(x, w0[...])
    keep[0:count, pair:] = dot(x, w2[...])


def relay_kernel(keep, came, onward):
    pair = onward.shape[1]
    count = keep.shape[0] - 8
    onward[0:count, :] = (keep[0:count, pair:] + came[0:count, pair:].astype(F32)).astype(BF16)
    squares = keep[count : count + 1, :] + sum_terms(came[count:, :])
    onward[count : count + 8, :] = three_terms(squares[:, 0:pair], pair)
    onward[count + 8 :, :] = three_terms(squares[:, pair:], pair)


def hidden_kernel(width, keep, came, last, hidden):
    count, units = hidden.shape
    pair = 2 * units
    total = (
        keep[0:count, 0:pair] + came[0:count, 0:pair].astype(F32) + last[0:count, :].astype(F32)
    )
    squares = keep[count : count + 1, :] + sum_terms(came[count:, :])
    squares = squares + jnp.concatenate(
        [sum_terms(last[count : count + 8, :]), sum_terms(last[count + 8 :, :])], axis=1
    )
    column = jnp.transpose(jnp.broadcast_to(squares[:, 0:count], (8, count)))[:, 0:1]
    scale = lax.rsqrt(column / width + EPS)
    hidden[...] = (jax.nn.silu(total[:, 0:units] * scale) * (total[:, units:] * scale)).astype(BF16)


def leave_kernel(capacity, h0, h1, h2, h3, w0, w1, w2, w3, out, wide):
    total = (dot(h0[...], w0[...]) + dot(h1[...], w1[...])) + (
        dot(h2[...], w2[...]) + dot(h3[...], w3[...])
    )
    for strided, near, cols in places(capacity, wide, total.shape[1]):
        wide[strided, :] = total[near, cols]
    out[...] = wide[...].astype(BF16)


def final_kernel(
    capacity, returned, w, share0, share1, resid, blend, own, came, last, out, wide, rows
):
    count, quarter = resid.shape
    wide[...] = returned[...].astype(F32)
    for strided, near, cols in places(capacity, wide, quarter):
        rows[near, cols] = wide[strided, :].astype(BF16)
    picked = dot(w[...], rows[...])
    lanes = wide.shape[1]
    for c in range(quarter // lanes):
        cols = slice(c * lanes, (c + 1) * lanes)
        moe = share0[...] * picked[0:count, cols] + share1[...] * picked[count:, cols]
        dense = (own[:, cols].astype(F32) + came[:, cols].astype(F32)) + last[:, cols].astype(F32)
        out[:, cols] = (resid[:, cols].astype(F32) + moe + blend[...] * dense).astype(BF16)


def call(kernel, outs, scratch=(), limit=4, in_specs=None, out_specs=None):
    out_specs = out_specs or [VMEM] * len(outs)
    kinds = {id(VMEM): pltpu.VMEM, id(OUT): pltpu.HBM}
    out_shape = [
        kinds.get(id(spec), jax.ShapeDtypeStruct)(s, d) for (s, d), spec in zip(outs, out_specs)
    ]

    def run(*args):
        specs = in_specs or [VMEM] * len(args)
        spaces = {id(VMEM): pltpu.VMEM, id(HBM): pltpu.HBM}
        fixed = [
            pltpu.with_memory_space_constraint(a, spaces.get(id(spec), pl.ANY))
            for a, spec in zip(args, specs)
        ]
        return pl.pallas_call(
            kernel,
            out_shape=tuple(out_shape),
            in_specs=specs,
            out_specs=tuple(out_specs),
            scratch_shapes=list(scratch),
            compiler_params=pltpu.CompilerParams(vmem_limit_bytes=limit << 20),
        )(*fixed)

    return run


def per_device(
    tokens,
    norm_gain,
    in_weight,
    sequence_state_real,
    sequence_state_imaginary,
    eigen_decay_real,
    log_step,
    input_matrix_real,
    input_matrix_imaginary,
    output_matrix_real,
    output_matrix_imaginary,
    channel_skip_scale,
    out_weight,
    ffn_gain,
    routes,
    group_weight,
    expert_logit,
    expert_gate,
    expert_up,
    expert_down,
    dense_gate,
    dense_up,
    dense_down,
    blend_weight,
):
    rows, width = tokens.shape
    tp = lax.axis_size("tp")
    ep = lax.axis_size("ep")
    quarter = width // tp
    lanes = 128
    blocks = quarter // lanes
    capacity = max(2, 2 * rows * routes.shape[1] // (ep * expert_gate.shape[0]))
    slots = ep * capacity
    groups, entries, channels = input_matrix_real.shape
    hid = expert_gate.shape[2]
    gate = expert_gate.reshape(width, hid)
    up = expert_up.reshape(width, hid)
    down = expert_down.reshape(hid, width)
    piece = ((rows, quarter), BF16)

    def by_channel(matrix):
        return jnp.swapaxes(matrix, 1, 2).reshape(groups * channels, entries)

    states = ((rows, groups * entries), F32)
    state_inputs = (
        log_step,
        eigen_decay_real,
        channel_skip_scale,
        tokens,
        norm_gain,
        by_channel(input_matrix_real),
        by_channel(input_matrix_imaginary),
        in_weight,
        sequence_state_real,
        sequence_state_imaginary,
        output_matrix_real.reshape(groups * channels, entries),
        output_matrix_imaginary.reshape(groups * channels, entries),
        out_weight,
    )
    own, beside, new_re, new_im = call(
        state_kernel,
        [((rows, 2 * quarter), BF16)] * 2 + [states] * 2,
        [pltpu.SMEM(log_step.shape, F32)]
        + [pltpu.VMEM(x.shape, x.dtype) for x in state_inputs[1:]]
        + [pltpu.VMEM((4, groups * channels, groups * entries), BF16)]
        + [pltpu.SemaphoreType.DMA((13,))],
        20,
        [HBM] * 13,
        [VMEM] * 4,
    )(*state_inputs)
    came_mix = exchanged(beside, 1)
    z, w, share0, share1 = call(
        functools.partial(route_kernel, ep),
        [((slots, lanes), BF16), ((2 * rows, slots), BF16)] + [((rows, lanes), F32)] * 2,
        [pltpu.VMEM((8, lanes), jnp.int32)],
    )(routes.T, group_weight.reshape(1, rows), expert_logit.T)
    wide = pltpu.VMEM((slots * blocks, lanes), F32)
    (onward,) = call(half_kernel, [piece])(own, came_mix)
    last_mix = exchanged(onward, 2)
    reshard = call(reshard_kernel, [((quarter, 2 * hid), BF16)] * 4 + [((hid, quarter), BF16)] * 4)
    pieces = reshard(gate, up, down)
    wide2 = exchanged(pieces[2], 2)
    wide3 = exchanged(pieces[3], 3)
    wide1 = exchanged(pieces[1], 1)
    moved = [pieces[0], wide1, wide2, wide3]
    downs = [pieces[4]] + [exchanged(pieces[4 + m], m) for m in (1, 2, 3)]
    resid16, packed = call(
        functools.partial(pack_kernel, capacity),
        [piece, ((slots * blocks, lanes), BF16)],
        [wide],
        8,
        out_specs=[VMEM, FREE],
    )(tokens, own, came_mix, last_mix, z)
    across = exchanged(resid16, 2)
    arrived = lax.all_to_all(
        packed.reshape(ep, capacity * blocks, lanes), "ep", 0, 0, tiled=True
    ).reshape(slots * blocks, lanes)
    near = [resid16, exchanged(resid16, 1), across, exchanged(across, 1)]
    gains = ffn_gain.reshape(1, width)
    send, x_rows, squares = call(
        functools.partial(enter_kernel, capacity),
        [((slots + 8, 4 * hid), BF16), ((slots, quarter), BF16), ((8, slots), F32)],
        [wide, pltpu.VMEM((slots, lanes), F32)],
        8,
    )(arrived, gains, moved[1], moved[3])
    came = exchanged(send, 1)
    (keep,) = call(stay_kernel, [((slots + 8, 4 * hid), F32)])(x_rows, squares, moved[0], moved[2])
    (onward,) = call(relay_kernel, [((slots + 16, 2 * hid), BF16)])(keep, came)
    last = exchanged(onward, 2)
    dense_own, dense_beside, blend = call(
        dense_kernel,
        [((rows, 2 * quarter), BF16)] * 2 + [((rows, lanes), F32)],
        [pltpu.VMEM((rows, width), BF16)]
        + [pltpu.VMEM(x.shape, BF16) for x in (dense_gate, dense_up, dense_down)]
        + [pltpu.SemaphoreType.DMA((3,))],
        12,
        [VMEM] * 6 + [HBM] * 3,
        [OUT] * 3,
    )(gains, *near, blend_weight.reshape(1, width), dense_gate, dense_up, dense_down)
    dense_came = exchanged(dense_beside, 1)
    (dense_onward,) = call(half_kernel, [piece])(dense_own, dense_came)
    dense_last = exchanged(dense_onward, 2)
    (hidden,) = call(
        functools.partial(hidden_kernel, float(width)), [((slots, hid), BF16)]
    )(keep, came, last)
    hidden = gathered(hidden)
    (sent,) = call(
        functools.partial(leave_kernel, capacity),
        [((slots * blocks, lanes), BF16)],
        [wide],
        8,
        out_specs=[FREE],
    )(*hidden, *downs)
    returned = lax.all_to_all(
        sent.reshape(ep, capacity * blocks, lanes), "ep", 0, 0, tiled=True
    ).reshape(slots * blocks, lanes)
    (new_tokens,) = call(
        functools.partial(final_kernel, capacity),
        [piece],
        [wide, pltpu.VMEM((slots, quarter), BF16)],
        8,
        out_specs=[FREE],
    )(returned, w, share0, share1, resid16, blend, dense_own, dense_came, dense_last)
    return (new_tokens, new_re, new_im)


def solution(mesh):
    in_specs = (
        P("ep", None),
        P(),
        P(None, "tp"),
        P("ep", "tp"),
        P("ep", "tp"),
        P("tp", None),
        P("tp"),
        P("tp", None, None),
        P("tp", None, None),
        P("tp", None, None),
        P("tp", None, None),
        P("tp", None),
        P("tp", None),
        P(),
        P("ep", None),
        P("ep"),
        P("ep", None),
        P("ep", None, "tp"),
        P("ep", None, "tp"),
        P("ep", "tp", None),
        P(None, "tp"),
        P(None, "tp"),
        P("tp", None),
        P(),
    )
    out_specs = (P("ep", "tp"), P("ep", "tp"), P("ep", "tp"))

    return jax.shard_map(
        per_device, mesh=mesh, in_specs=in_specs, out_specs=out_specs, check_vma=False
    )
```
